512 devices in a mesh: sp: 64 (over z, y), tp: 8 (over x, core).
Axes of the slice: x: 4, y: 8, z: 8, core: 2. Of those that a mesh axis runs over, the one named last changes fastest.
Arguments:
- query_one: bfloat16 [8192, 1024], P('sp', 'tp'), may hold values from -85 to 85
- key_one: bfloat16 [8192, 1024], P('sp', 'tp'), may hold values from -6.5 to 6.5
- query_two: bfloat16 [8192, 1024], P('sp', 'tp'), may hold values from -85 to 85
- key_two: bfloat16 [8192, 1024], P('sp', 'tp'), may hold values from -6.5 to 6.5
- values: bfloat16 [8192, 2048], P('sp', 'tp'), may hold values from -6 to 6
- mix_weight: float32 [8], P('tp'), may hold values from 0.3 to 0.8
- head_gain: float32 [256], replicated, may hold values from 0.1 to 1.9
- residual: bfloat16 [8192, 2048], P(('sp', 'tp')), may hold values from -6 to 6
- out_weight: bfloat16 [2048, 2048], P('tp'), may hold values from -0.125 to 0.125
- norm_gain: float32 [2048], replicated, may hold values from 0.1 to 1.9
- lift_weight: bfloat16 [2048, 5632], P('sp', 'tp'), may hold values from -0.125 to 0.125
- gate_weight: bfloat16 [2048, 5632], P('sp', 'tp'), may hold values from -0.125 to 0.125
- conv_taps: float32 [3, 5632], P(None, 'tp'), may hold values from -3 to 3
- down_weight: bfloat16 [5632, 2048], P('tp'), may hold values from -0.078125 to 0.078125
Outputs:
- layer_out: bfloat16 [8192, 2048], P(('sp', 'tp'))
The draws below stay inside these ranges and needn't reach their ends.
All inputs are finite; a program needn't handle non-finite values.
Results may differ from the reference program's by a relative error of at most 0.015.
Values may be sent and summed in bfloat16 or wider, within the bound.
No kernel may reach another device: no remote copies, remote signals or barrier semaphores. Data moves between devices by JAX's collectives and lax.ppermute only.
A program may use at most 64 MiB of HBM per device.

```python
import math
import jax
import jax.numpy as jnp
from jax import lax

D = 2048
HEADS = 8
HD = 128
VD = 256
FF = 5632
STRETCH = 64
WIDTH = 3
TOKENS = 8192
N_TP = 8


def drawn_pair(key, which):
    base = jax.random.fold_in(key, 71 + which)
    key_draw, query_draw = jax.random.split(base)
    keys = 1.3 * jnp.clip(jax.random.normal(key_draw, (TOKENS, HEADS * HD), jnp.float32), -5.0, 5.0)
    queries = 1.3 * jnp.clip(jax.random.normal(query_draw, (TOKENS, HEADS * HD), jnp.float32), -5.0, 5.0)
    return (queries, keys)


def draw_query_one(key, part):
    return drawn_pair(key, 0)[0].astype(jnp.bfloat16)


def draw_key_one(key, part):
    return drawn_pair(key, 0)[1].astype(jnp.bfloat16)


def draw_query_two(key, part):
    return drawn_pair(key, 1)[0].astype(jnp.bfloat16)


def draw_key_two(key, part):
    return drawn_pair(key, 1)[1].astype(jnp.bfloat16)


def levels(rng, extent, cuts, least, largest):
    def one(axis_at, parts):
        draws = jax.random.uniform(jax.random.fold_in(jax.random.fold_in(rng, 6), axis_at), (parts,), jnp.float32, least / len(cuts), largest / len(cuts))
        return jnp.repeat(jnp.exp(draws), extent[axis_at] // parts).reshape((-1,) + (1,) * (len(extent) - axis_at - 1))

    gain = one(*cuts[0])
    for cut in cuts[1:]:
        gain = gain * one(*cut)
    return gain


def centred(rng, dims, deviation, reach, cuts=(), kind=jnp.bfloat16):
    factor_of = levels(rng, dims, cuts, -0.22, 0.18) if cuts else 1.0
    drawn = jax.random.normal(rng, dims, jnp.float32) * deviation * factor_of
    return jnp.minimum(jnp.maximum(drawn, -reach), reach).astype(kind)


def setup_inputs(seed: int = 0) -> dict:
    key_list = jax.random.split(jax.random.key(seed), 15)
    return {
        "query_one": draw_query_one(jax.random.fold_in(key_list[14], 71), 0),
        "key_one": draw_key_one(jax.random.fold_in(key_list[14], 71), 0),
        "query_two": draw_query_two(jax.random.fold_in(key_list[14], 71), 0),
        "key_two": draw_key_two(jax.random.fold_in(key_list[14], 71), 0),
        "values": centred(key_list[4], (TOKENS, HEADS * VD), 1.0, 6.0, ((0, 64), (1, 8))),
        "mix_weight": jnp.clip(0.3 + 0.5 * jax.random.uniform(key_list[5], (HEADS,), jnp.float32) ** levels(key_list[5], (HEADS,), ((0, 8),), -0.2, 0.2), 0.3, 0.8),
        "head_gain": jnp.clip(1.0 + 0.18 * jax.random.normal(key_list[6], (VD,), jnp.float32), 0.1, 1.9),
        "residual": centred(key_list[7], (TOKENS, D), 1.0, 6.0, ((0, 512),)),
        "out_weight": centred(key_list[8], (HEADS * VD, D), (HEADS * VD) ** -0.5, 0.125, ((0, 8),)),
        "norm_gain": jnp.clip(1.0 + 0.18 * jax.random.normal(key_list[9], (D,), jnp.float32), 0.1, 1.9),
        "lift_weight": centred(key_list[10], (D, FF), D ** -0.5, 0.125, ((0, 64), (1, 8))),
        "gate_weight": centred(key_list[11], (D, FF), D ** -0.5, 0.125, ((0, 64), (1, 8))),
        "conv_taps": centred(key_list[12], (WIDTH, FF), 0.577, 3.0, ((1, 8),), jnp.float32),
        "down_weight": centred(key_list[13], (FF, D), FF ** -0.5, 0.078125, ((0, 8),)),
    }


epsilon = 1e-06
masked_score = -1e+30

def attend_block(first_q, first_k, second_q, second_k, vals, mix_weight, head_gain, start, block_rows):
    scale_factor = HD ** (-0.5)
    q_pos = start + lax.iota(jnp.int32, block_rows)
    k_pos = lax.iota(jnp.int32, TOKENS)
    visible = k_pos[None, :] // STRETCH <= q_pos[:, None] // STRETCH

    def one_map(queries, keys):
        scores = jnp.einsum('thd,shd->hts', queries, keys) * scale_factor
        scores = jnp.where(visible[None], scores, masked_score)
        peak = lax.optimization_barrier(jnp.max(scores, axis=-1, keepdims=True))
        weights = jnp.where(visible[None], jnp.exp(scores - peak), 0.0)
        total = lax.optimization_barrier(jnp.sum(weights, axis=-1))
        rounded = lax.optimization_barrier(weights.astype(jnp.bfloat16))
        acc = jnp.einsum('hts,she->hte', rounded.astype(jnp.float32), vals)
        return acc / total[..., None]
    mixed = one_map(first_q, first_k) - mix_weight[:, None, None] * one_map(second_q, second_k)
    normed = mixed * lax.rsqrt(lax.optimization_barrier(jnp.mean(mixed * mixed, axis=-1, keepdims=True)) + epsilon) * head_gain
    return jnp.transpose(normed.astype(jnp.bfloat16), (1, 0, 2))

def reference(query_one, key_one, query_two, key_two, values, mix_weight, head_gain, residual, out_weight, norm_gain, lift_weight, gate_weight, conv_taps, down_weight):
    val_width = 2 * HD
    block_rows = math.gcd(TOKENS, 512)
    blocks = TOKENS // block_rows
    q_one = query_one.astype(jnp.float32).reshape(TOKENS, HEADS, HD)
    q_two = query_two.astype(jnp.float32).reshape(TOKENS, HEADS, HD)
    k_one = key_one.astype(jnp.float32).reshape(TOKENS, HEADS, HD)
    k_two = key_two.astype(jnp.float32).reshape(TOKENS, HEADS, HD)
    vals = values.astype(jnp.float32).reshape(TOKENS, HEADS, val_width)

    def per_block(index):
        start = (index * block_rows).astype(jnp.int32)
        first_q = lax.dynamic_slice_in_dim(q_one, start, block_rows, 0)
        second_q = lax.dynamic_slice_in_dim(q_two, start, block_rows, 0)
        return attend_block(first_q, k_one, second_q, k_two, vals, mix_weight, head_gain, start, block_rows)
    head_out = lax.map(per_block, jnp.arange(blocks, dtype=jnp.int32))
    head_out = head_out.reshape(TOKENS, HEADS * val_width)
    group = HEADS * val_width // N_TP
    attended = jnp.zeros((TOKENS, D), jnp.float32)
    for index in range(N_TP):
        partial_sum = jnp.dot(head_out[:, index * group:(index + 1) * group], out_weight[index * group:(index + 1) * group], preferred_element_type=jnp.float32)
        attended = attended + partial_sum.astype(jnp.bfloat16).astype(jnp.float32)
    stream = residual.astype(jnp.float32) + attended
    normed = (stream * lax.rsqrt(lax.optimization_barrier(jnp.mean(stream * stream, axis=-1, keepdims=True)) + epsilon) * norm_gain).astype(jnp.bfloat16)
    lifted = jnp.dot(normed, lift_weight, preferred_element_type=jnp.float32).astype(jnp.bfloat16)
    gated = jnp.dot(normed, gate_weight, preferred_element_type=jnp.float32).astype(jnp.bfloat16)
    padded = jnp.concatenate([jnp.zeros((WIDTH - 1, FF), jnp.float32), gated.astype(jnp.float32)], axis=0)
    conv = jnp.zeros((TOKENS, FF), jnp.float32)
    for index in range(WIDTH):
        conv = conv + conv_taps[index] * padded[index:index + TOKENS]
    hidden = (jax.nn.silu(conv) * lifted.astype(jnp.float32)).astype(jnp.bfloat16)
    units = FF // N_TP
    mixer = jnp.zeros((TOKENS, D), jnp.float32)
    for index in range(N_TP):
        partial_sum = jnp.dot(hidden[:, index * units:(index + 1) * units], down_weight[index * units:(index + 1) * units], preferred_element_type=jnp.float32)
        mixer = mixer + partial_sum.astype(jnp.bfloat16).astype(jnp.float32)
    return (stream + mixer).astype(jnp.bfloat16)
```

```python
import jax
import jax.numpy as jnp
import numpy as np
from jax import lax
from jax.experimental import pallas as pl
from jax.experimental.pallas import tpu as pltpu
from jax.sharding import Mesh, PartitionSpec as P

HD = 128
VD = 256
STRETCH = 64
WIDTH = 3
SIDE = 8
BLOCK = 128
PACK = 4 * BLOCK + 16
epsilon = 1e-06
masked_score = -1e30
LOG2E = 1.4426950408889634
EXP2_SCALE = LOG2E * HD**-0.5
f32 = jnp.float32
bf16 = jnp.bfloat16
TP = ("x", "core")
ALL = ("z", "y", "x", "core")
PLACES = np.arange(SIDE * SIDE * 8).reshape(SIDE, SIDE, 4, 2)
ROWS = [[PLACES[i, :, x, c].tolist() for i in range(SIDE) for x in range(4)] for c in range(2)]
COLS = [[PLACES[:, i, x, c].tolist() for i in range(SIDE) for x in range(4)] for c in range(2)]
Q_GROUPS = ROWS[0] + COLS[1]
K_GROUPS = COLS[0] + ROWS[1]


def vmem():
    return pl.BlockSpec(memory_space=pltpu.VMEM)


def pack_kernel(q1, q2, k1, k2, v, qsend, ksend):
    for i in range(SIDE):
        qsend[i, 0:128, :] = q1[...]
        qsend[i, 128:256, :] = q2[...]
        ksend[i, 0:128, :] = k1[...]
        ksend[i, 128:256, :] = k2[...]
        ksend[i, 256:384, :] = v[:, 0:128]
        ksend[i, 384:512, :] = v[:, 128:256]


def attend_kernel(plan, qpool, kpool, out, scores):
    q_base, q_step, k_base, k_step = (plan[i] for i in range(4))
    first_chunk, pairs = plan[4], plan[5]
    row = lax.broadcasted_iota(jnp.int32, (256, 256), 0)
    col = lax.broadcasted_iota(jnp.int32, (256, 256), 1)
    at = lax.broadcasted_iota(jnp.int32, (16, 128), 0)

    def blank(c, carry):
        for h in range(2):
            out[2 * c + h, 0:512, :] = jnp.zeros((512, 128), bf16)
            level = jnp.where((at == 0) | (at == 3), masked_score, 0.0)
            out[2 * c + h, 512:528, :] = level.astype(bf16)
        return carry

    lax.fori_loop(0, first_chunk, blank, 0)

    def chunk(c, carry):
        queries = [
            jnp.concatenate(
                [qpool[2 * c, 128 * m : 128 * m + 128, :], qpool[2 * c + 1, 128 * m : 128 * m + 128, :]],
                axis=0,
            )
            for m in range(2)
        ]
        q_at = 2 * (q_base + q_step * (2 * c + row // 128)) + (row % 128) // STRETCH

        def scored(p, peaks):
            k_at = 2 * (k_base + k_step * (2 * p + col // 128)) + (col % 128) // STRETCH
            seen = k_at <= q_at
            new = []
            for m in range(2):
                k = jnp.concatenate(
                    [kpool[2 * p, 128 * m : 128 * m + 128, :], kpool[2 * p + 1, 128 * m : 128 * m + 128, :]],
                    axis=0,
                )
                s = lax.dot_general(
                    queries[m], k, (((1,), (1,)), ((), ())), preferred_element_type=f32
                )
                s = jnp.where(seen, s, masked_score)
                scores[2 * p + m] = s
                new.append(jnp.maximum(peaks[m], jnp.maximum(s[:, 0:128], s[:, 128:256])))
            return tuple(new)

        low = jnp.full((256, 128), masked_score, f32)
        peaks = lax.fori_loop(0, pairs, scored, (low, low))
        tops = [jnp.max(peak, axis=-1, keepdims=True) for peak in peaks]

        def weighed(p, carry):
            totals, acc = carry
            new, ws = [], []
            for m in range(2):
                w = jnp.exp2((scores[2 * p + m] - tops[m]) * EXP2_SCALE)
                new.append(totals[m] + (w[:, 0:128] + w[:, 128:256]))
                ws.append(w.astype(bf16))
            va = jnp.concatenate([kpool[2 * p, 256:384, :], kpool[2 * p, 384:512, :]], axis=1)
            vb = jnp.concatenate([kpool[2 * p + 1, 256:384, :], kpool[2 * p + 1, 384:512, :]], axis=1)
            vals = jnp.concatenate([va, vb], axis=0)
            acc = acc + jnp.dot(
                jnp.concatenate(ws, axis=0), vals, preferred_element_type=f32
            )
            return tuple(new), acc

        none = jnp.zeros((256, 128), f32)
        totals, acc = lax.fori_loop(
            0, pairs, weighed, ((none, none), jnp.zeros((512, VD), f32))
        )
        levels = []
        for m in range(2):
            total = jnp.sum(totals[m], axis=-1, keepdims=True)
            o = (acc[256 * m : 256 * m + 256] / total).astype(bf16)
            seen = tops[m] > 0.5 * masked_score
            levels.append(jnp.where(seen, tops[m] * EXP2_SCALE + jnp.log2(total), masked_score))
            for h in range(2):
                for e in range(2):
                    out[2 * c + h, 256 * m + 128 * e : 256 * m + 128 * e + 128, :] = o[
                        128 * h : 128 * h + 128, 128 * e : 128 * e + 128
                    ]
        for h in range(2):
            rows = jnp.zeros((16, 128), f32)
            for m in range(2):
                wide = jnp.transpose(
                    jnp.broadcast_to(levels[m][128 * h : 128 * h + 128], (128, 128))
                )[0:16]
                a = wide.astype(bf16).astype(f32)
                b = (wide - a).astype(bf16).astype(f32)
                d = wide - a - b
                for n, piece in enumerate((a, b, d)):
                    rows = jnp.where(at == 3 * m + n, piece, rows)
            out[2 * c + h, 512:528, :] = rows.astype(bf16)
        return carry

    lax.fori_loop(first_chunk, SIDE // 2, chunk, 0)


def join_kernel(mix, parts, gain, weight, out):
    tails = [parts[i, 512:528, :].astype(f32) for i in range(SIDE)]

    def joined(m):
        levels = jnp.concatenate(
            [jnp.sum(tail[3 * m : 3 * m + 3], axis=0, keepdims=True) for tail in tails], axis=0
        )
        top = jnp.max(levels, axis=0, keepdims=True)
        w = jnp.exp2(levels - top)
        w = w / jnp.sum(w, axis=0, keepdims=True)
        w = jnp.transpose(jnp.concatenate([w, jnp.zeros((120, 128), f32)], axis=0))
        acc = [jnp.zeros((128, 128), f32), jnp.zeros((128, 128), f32)]
        for i in range(SIDE):
            wi = w[:, i : i + 1]
            for e in range(2):
                at = 256 * m + 128 * e
                acc[e] = acc[e] + wi * parts[i, at : at + 128, :].astype(f32)
        return jnp.concatenate(acc, axis=1)

    mixed = joined(0) - mix[0] * joined(1)
    r = lax.rsqrt(jnp.mean(mixed * mixed, axis=-1, keepdims=True) + epsilon)
    head = (mixed * r * gain[...]).astype(bf16)
    out[...] = jnp.dot(head, weight[...], preferred_element_type=f32).astype(bf16)


def norm_kernel(parts, residual, gain, stream, normed):
    total = residual[...].astype(f32)
    att = parts[0].astype(f32)
    for i in range(1, 8):
        att = att + parts[i].astype(f32)
    total = total + att
    stream[...] = total
    r = lax.rsqrt(jnp.mean(total * total, axis=-1, keepdims=True) + epsilon)
    n = (total * r * gain[...]).astype(bf16)
    for i in range(8):
        normed[i] = n


def last_kernel(parts, stream, out):
    mixer = parts[0].astype(f32)
    for i in range(1, 8):
        mixer = mixer + parts[i].astype(f32)
    out[...] = (stream[...] + mixer).astype(bf16)


def swapped(a, axis, groups=None):
    return lax.all_to_all(a, axis, 0, 0, axis_index_groups=groups, tiled=True)


def on_device(
    query_one,
    key_one,
    query_two,
    key_two,
    values,
    mix_weight,
    head_gain,
    residual,
    out_weight,
    norm_gain,
    lift_weight,
    gate_weight,
    conv_taps,
    down_weight,
):
    tokens = query_one.shape[0]
    own = residual.shape[0]
    width = residual.shape[1]
    z = lax.axis_index("z")
    y = lax.axis_index("y")
    core = lax.axis_index("core")
    along_y = jnp.stack([z * SIDE, 1 + 0 * z, y, SIDE + 0 * z, 0 * z, z // 2 + 1])
    along_z = jnp.stack([y, SIDE + 0 * z, z * SIDE, 1 + 0 * z, z // 2, SIDE // 2 + 0 * z])
    plan = jnp.where(core == 0, along_y, along_z).astype(jnp.int32)
    qsend, ksend = pl.pallas_call(
        pack_kernel,
        out_shape=[
            jax.ShapeDtypeStruct((SIDE, 256, 128), bf16),
            jax.ShapeDtypeStruct((SIDE, 512, 128), bf16),
        ],
        in_specs=[vmem()] * 5,
        out_specs=[vmem()] * 2,
        name="pack",
    )(query_one, query_two, key_one, key_two, values)
    both = jnp.concatenate([lift_weight, gate_weight], axis=1)
    with jax.named_scope("kpool"):
        kpool = swapped(ksend, ALL, K_GROUPS)
    with jax.named_scope("qpool"):
        qpool = swapped(qsend, ALL, Q_GROUPS)
    weights = lax.all_gather(both, ("z", "y"), axis=0, tiled=True)
    out = pl.pallas_call(
        attend_kernel,
        out_shape=jax.ShapeDtypeStruct((SIDE, PACK, 128), bf16),
        in_specs=[pl.BlockSpec(memory_space=pltpu.SMEM), vmem(), vmem()],
        out_specs=vmem(),
        scratch_shapes=[pltpu.VMEM((8, 256, 256), f32)],
        name="attend",
    )(plan, qpool, kpool)
    back = swapped(out, ALL, Q_GROUPS)
    attended = pl.pallas_call(
        join_kernel,
        out_shape=jax.ShapeDtypeStruct((tokens, width), bf16),
        in_specs=[pl.BlockSpec(memory_space=pltpu.SMEM)] + [vmem()] * 3,
        out_specs=vmem(),
        name="join",
    )(mix_weight, back, head_gain.reshape(1, VD), out_weight)
    parts = swapped(attended.reshape(8, own, width), TP)
    stream, normed = pl.pallas_call(
        norm_kernel,
        out_shape=[
            jax.ShapeDtypeStruct((own, width), f32),
            jax.ShapeDtypeStruct((8, own, width), bf16),
        ],
        in_specs=[vmem()] * 3,
        out_specs=[vmem()] * 2,
        name="norm",
    )(parts, residual, norm_gain.reshape(1, width))
    rows = swapped(normed, TP).reshape(tokens, width)
    units = lift_weight.shape[1]
    lift_pre = jnp.dot(rows, weights[:, :units], preferred_element_type=f32)
    gate_pre = jnp.dot(rows, weights[:, units:], preferred_element_type=f32)
    lifted = lift_pre.astype(bf16)
    gated = gate_pre.astype(bf16)
    route = [(i, i + 1) for i in range(SIDE * SIDE - 1)]
    prior = lax.ppermute(gated[tokens - (WIDTH - 1) :], ("z", "y"), route)
    extended = jnp.concatenate([prior, gated], axis=0).astype(f32)
    conv = conv_taps[0] * extended[0:tokens]
    for index in range(1, WIDTH):
        conv = conv + conv_taps[index] * extended[index : index + tokens]
    hidden = (jax.nn.silu(conv) * lifted.astype(f32)).astype(bf16)
    down = jnp.dot(hidden, down_weight, preferred_element_type=f32).astype(bf16)
    mixer = swapped(down.reshape(8, own, width), TP)
    return pl.pallas_call(
        last_kernel,
        out_shape=jax.ShapeDtypeStruct((own, width), bf16),
        in_specs=[vmem()] * 2,
        out_specs=vmem(),
        name="last",
    )(mixer, stream)


def solution(mesh):
    fine = Mesh(mesh.devices.reshape(SIDE, SIDE, 4, 2), ("z", "y", "x", "core"))
    sp = ("z", "y")
    return jax.shard_map(
        on_device,
        mesh=fine,
        in_specs=(
            P(sp, TP),
            P(sp, TP),
            P(sp, TP),
            P(sp, TP),
            P(sp, TP),
            P(TP),
            P(),
            P(("z", "y", "x", "core"), None),
            P(TP, None),
            P(),
            P(sp, TP),
            P(sp, TP),
            P(None, TP),
            P(TP, None),
        ),
        out_specs=P(("z", "y", "x", "core"), None),
        check_vma=False,
    )
```

```python
import jax
import jax.numpy as jnp
import numpy as np
from jax import lax
from jax.experimental import pallas as pl
from jax.experimental.pallas import tpu as pltpu
from jax.sharding import Mesh, PartitionSpec as P

HD = 128
VD = 256
STRETCH = 64
WIDTH = 3
SIDE = 8
BLOCK = 128
PACK = 4 * BLOCK + 16
TILES = 5
MAIN = 128 * TILES
SENT = 512 + 352
epsilon = 1e-06
masked_score = -1e30
LOG2E = 1.4426950408889634
EXP2_SCALE = LOG2E * HD**-0.5
f32 = jnp.float32
bf16 = jnp.bfloat16
TP = ("x", "core")
ALL = ("z", "y", "x", "core")
PLACES = np.arange(SIDE * SIDE * 8).reshape(SIDE, SIDE, 4, 2)
ROWS = [[PLACES[i, :, x, c].tolist() for i in range(SIDE) for x in range(4)] for c in range(2)]
COLS = [[PLACES[:, i, x, c].tolist() for i in range(SIDE) for x in range(4)] for c in range(2)]
Q_GROUPS = ROWS[0] + COLS[1]
K_GROUPS = COLS[0] + ROWS[1]


def vmem():
    return pl.BlockSpec(memory_space=pltpu.VMEM)


def pack_kernel(q1, q2, k1, k2, v, lift, gate, qsend, ksend, vv, ll, gg, kk, sems):
    moves = [
        pltpu.make_async_copy(src, dst, sems.at[i])
        for i, (src, dst) in enumerate(
            (
                (k1, kk.at[0]),
                (k2, kk.at[1]),
                (v, vv),
                (lift, ll),
                (gate, gg),
                (q1, qsend.at[0:128]),
                (q2, qsend.at[128:256]),
            )
        )
    ]
    for move in moves:
        move.start()
    for move in moves:
        move.wait()
    tail = jnp.concatenate([ll[:, MAIN:], gg[:, MAIN:]], axis=1)
    for i in range(SIDE):
        ksend[i, 0:128, :] = kk[0]
        ksend[i, 128:256, :] = kk[1]
        ksend[i, 256:384, :] = vv[:, 0:128]
        ksend[i, 384:512, :] = vv[:, 128:256]
        for n in range(TILES):
            ksend[i, 512 + 32 * n : 544 + 32 * n, :] = gg[:, 128 * n : 128 * n + 128]
            ksend[i, 704 + 32 * n : 736 + 32 * n, :] = ll[:, 128 * n : 128 * n + 128]
        ksend[i, 672:704, :] = tail


def attend_kernel(plan, qpool, kpool, out, scores):
    q_base, q_step, k_base, k_step = (plan[i] for i in range(4))
    first_chunk, pairs = plan[4], plan[5]
    row = lax.broadcasted_iota(jnp.int32, (256, 256), 0)
    col = lax.broadcasted_iota(jnp.int32, (256, 256), 1)
    at = lax.broadcasted_iota(jnp.int32, (16, 128), 0)

    def blank(c, carry):
        for h in range(2):
            out[2 * c + h, 0:512, :] = jnp.zeros((512, 128), bf16)
            level = jnp.where((at == 0) | (at == 3), masked_score, 0.0)
            out[2 * c + h, 512:528, :] = level.astype(bf16)
        return carry

    lax.fori_loop(0, first_chunk, blank, 0)

    def chunk(c, carry):
        queries = [
            jnp.concatenate(
                [qpool[2 * c, 128 * m : 128 * m + 128, :], qpool[2 * c + 1, 128 * m : 128 * m + 128, :]],
                axis=0,
            )
            for m in range(2)
        ]
        q_at = 2 * (q_base + q_step * (2 * c + row // 128)) + (row % 128) // STRETCH

        def scored(p, peaks):
            k_at = 2 * (k_base + k_step * (2 * p + col // 128)) + (col % 128) // STRETCH
            seen = k_at <= q_at
            new = []
            for m in range(2):
                k = jnp.concatenate(
                    [kpool[2 * p, 128 * m : 128 * m + 128, :], kpool[2 * p + 1, 128 * m : 128 * m + 128, :]],
                    axis=0,
                )
                s = lax.dot_general(
                    queries[m], k, (((1,), (1,)), ((), ())), preferred_element_type=f32
                )
                s = jnp.where(seen, s, masked_score)
                scores[2 * p + m] = s
                new.append(jnp.maximum(peaks[m], jnp.maximum(s[:, 0:128], s[:, 128:256])))
            return tuple(new)

        low = jnp.full((256, 128), masked_score, f32)
        peaks = lax.fori_loop(0, pairs, scored, (low, low))
        tops = [jnp.max(peak, axis=-1, keepdims=True) for peak in peaks]

        def weighed(p, carry):
            totals, acc = carry
            new, ws = [], []
            for m in range(2):
                w = jnp.exp2((scores[2 * p + m] - tops[m]) * EXP2_SCALE)
                new.append(totals[m] + (w[:, 0:128] + w[:, 128:256]))
                ws.append(w.astype(bf16))
            va = jnp.concatenate([kpool[2 * p, 256:384, :], kpool[2 * p, 384:512, :]], axis=1)
            vb = jnp.concatenate([kpool[2 * p + 1, 256:384, :], kpool[2 * p + 1, 384:512, :]], axis=1)
            vals = jnp.concatenate([va, vb], axis=0)
            acc = acc + jnp.dot(
                jnp.concatenate(ws, axis=0), vals, preferred_element_type=f32
            )
            return tuple(new), acc

        none = jnp.zeros((256, 128), f32)
        totals, acc = lax.fori_loop(
            0, pairs, weighed, ((none, none), jnp.zeros((512, VD), f32))
        )
        levels = []
        for m in range(2):
            total = jnp.sum(totals[m], axis=-1, keepdims=True)
            o = (acc[256 * m : 256 * m + 256] / total).astype(bf16)
            seen = tops[m] > 0.5 * masked_score
            levels.append(jnp.where(seen, tops[m] * EXP2_SCALE + jnp.log2(total), masked_score))
            for h in range(2):
                for e in range(2):
                    out[2 * c + h, 256 * m + 128 * e : 256 * m + 128 * e + 128, :] = o[
                        128 * h : 128 * h + 128, 128 * e : 128 * e + 128
                    ]
        for h in range(2):
            rows = jnp.zeros((16, 128), f32)
            for m in range(2):
                wide = jnp.transpose(
                    jnp.broadcast_to(levels[m][128 * h : 128 * h + 128], (128, 128))
                )[0:16]
                a = wide.astype(bf16).astype(f32)
                b = (wide - a).astype(bf16).astype(f32)
                d = wide - a - b
                for n, piece in enumerate((a, b, d)):
                    rows = jnp.where(at == 3 * m + n, piece, rows)
            out[2 * c + h, 512:528, :] = rows.astype(bf16)
        return carry

    lax.fori_loop(first_chunk, SIDE // 2, chunk, 0)


def join_kernel(mix, parts, gain, weight, out):
    tails = [parts[i, 512:528, :].astype(f32) for i in range(SIDE)]

    def joined(m):
        levels = jnp.concatenate(
            [jnp.sum(tail[3 * m : 3 * m + 3], axis=0, keepdims=True) for tail in tails], axis=0
        )
        top = jnp.max(levels, axis=0, keepdims=True)
        w = jnp.exp2(levels - top)
        w = w / jnp.sum(w, axis=0, keepdims=True)
        w = jnp.transpose(jnp.concatenate([w, jnp.zeros((120, 128), f32)], axis=0))
        acc = [jnp.zeros((128, 128), f32), jnp.zeros((128, 128), f32)]
        for i in range(SIDE):
            wi = w[:, i : i + 1]
            for e in range(2):
                at = 256 * m + 128 * e
                acc[e] = acc[e] + wi * parts[i, at : at + 128, :].astype(f32)
        return jnp.concatenate(acc, axis=1)

    mixed = joined(0) - mix[0] * joined(1)
    r = lax.rsqrt(jnp.mean(mixed * mixed, axis=-1, keepdims=True) + epsilon)
    head = (mixed * r * gain[...]).astype(bf16)
    out[...] = jnp.dot(head, weight[...], preferred_element_type=f32).astype(bf16)


def norm_kernel(parts, residual, gain, stream, normed):
    att = parts[0].astype(f32)
    for i in range(1, 8):
        att = att + parts[i].astype(f32)
    total = residual[...].astype(f32) + att
    stream[...] = total
    r = lax.rsqrt(jnp.mean(total * total, axis=-1, keepdims=True) + epsilon)
    normed[...] = (total * r * gain[...]).astype(bf16)


def fetched(core, weights, buffer, sems, first):
    height = buffer.shape[2]
    for g in range(SIDE):
        rows = pl.ds(first, height)

        @pl.when(core == 0)
        def _():
            pltpu.make_async_copy(weights.at[:, g, rows, :], buffer.at[g], sems.at[g]).start()

        @pl.when(core != 0)
        def _():
            pltpu.make_async_copy(weights.at[g, :, rows, :], buffer.at[g], sems.at[g]).start()


def multiplied(rows, weights, buffer, sems, first):
    height = buffer.shape[2]
    count = height // 32
    acc = [None] * ((count + 1) // 2)
    for g in range(SIDE):
        pltpu.make_async_copy(
            weights.at[0, :, pl.ds(first, height), :], buffer.at[g], sems.at[g]
        ).wait()
        lhs = rows[:, 256 * g : 256 * g + 256]
        for n in range(0, count, 2):
            tiles = [
                buffer[g, :, 32 * m : 32 * m + 32, :].reshape(256, 128)
                for m in range(n, min(n + 2, count))
            ]
            rhs = jnp.concatenate(tiles, axis=1) if len(tiles) > 1 else tiles[0]
            d = jnp.dot(lhs, rhs, preferred_element_type=f32)
            acc[n // 2] = d if acc[n // 2] is None else acc[n // 2] + d
    return acc


def gate_kernel(core, rows, weights, gated, edge, buffer, sems):
    fetched(core[0], weights, buffer, sems, 0)
    for n, part in enumerate(multiplied(rows, weights, buffer, sems, 0)):
        part = part.astype(bf16)
        gated[:, 256 * n : 256 * n + 256] = part
        edge[:, 256 * n : 256 * n + 256] = part[112:128]


def lift_kernel(core, rows, weights, lifted, buffer, sems):
    fetched(core[0], weights, buffer, sems, 192)
    for n, part in enumerate(multiplied(rows, weights, buffer, sems, 192)):
        lifted[:, 256 * n : 256 * n + part.shape[1]] = part.astype(bf16)


def down_kernel(gated, lifted, prior, taps, weight, out):
    at = lax.broadcasted_iota(jnp.int32, (128, 1), 0)

    def activated(lo, hi):
        g = gated[:, lo:hi].astype(f32)
        p = prior[:, lo:hi].astype(f32)
        one = jnp.where(at == 0, p[15:16], pltpu.roll(g, 1, 0))
        two = jnp.where(at == 0, p[14:15], jnp.where(at == 1, p[15:16], pltpu.roll(g, 2, 0)))
        conv = taps[0:1, lo:hi] * two + taps[1:2, lo:hi] * one + taps[2:3, lo:hi] * g
        return g, conv * jax.nn.sigmoid(conv)

    acc = None
    for n in range(0, MAIN, 128):
        _, a = activated(n, n + 128)
        h = (a * lifted[:, n : n + 128].astype(f32)).astype(bf16)
        d = jnp.dot(h, weight[n : n + 128, :], preferred_element_type=f32)
        acc = d if acc is None else acc + d
    g, a = activated(MAIN, MAIN + 128)
    h = (pltpu.roll(a, 64, 1) * g).astype(bf16)
    acc = acc + jnp.dot(h[:, 0:64], weight[MAIN:, :], preferred_element_type=f32)
    out[...] = acc.astype(bf16)


def last_kernel(parts, stream, out):
    mixer = parts[0].astype(f32)
    for i in range(1, 8):
        mixer = mixer + parts[i].astype(f32)
    out[...] = (stream[...] + mixer).astype(bf16)


def swapped(a, axis, groups=None):
    return lax.all_to_all(a, axis, 0, 0, axis_index_groups=groups, tiled=True)


def gathered(a, axis, groups=None):
    return lax.all_gather(a, axis, axis_index_groups=groups, axis=0, tiled=True)


def in_hbm(a):
    return pltpu.with_memory_space_constraint(a, pltpu.HBM)


SMALL = pltpu.CompilerParams(vmem_limit_bytes=20 << 20)


def on_device(
    query_one,
    key_one,
    query_two,
    key_two,
    values,
    mix_weight,
    head_gain,
    residual,
    out_weight,
    norm_gain,
    lift_weight,
    gate_weight,
    conv_taps,
    down_weight,
):
    tokens = query_one.shape[0]
    own = residual.shape[0]
    width = residual.shape[1]
    z = lax.axis_index("z")
    y = lax.axis_index("y")
    core = lax.axis_index("core")
    along_y = jnp.stack([z * SIDE, 1 + 0 * z, y, SIDE + 0 * z, 0 * z, z // 2 + 1])
    along_z = jnp.stack([y, SIDE + 0 * z, z * SIDE, 1 + 0 * z, z // 2, SIDE // 2 + 0 * z])
    plan = jnp.where(core == 0, along_y, along_z).astype(jnp.int32)
    smem = pl.BlockSpec(memory_space=pltpu.SMEM)
    hbm = pl.BlockSpec(memory_space=pltpu.HBM)
    own_core = core.reshape(1).astype(jnp.int32)
    qsend, ksend = pl.pallas_call(
        pack_kernel,
        out_shape=[
            jax.ShapeDtypeStruct((256, 128), bf16),
            jax.ShapeDtypeStruct((SIDE, SENT, 128), bf16),
        ],
        in_specs=[hbm] * 7,
        out_specs=[vmem()] * 2,
        scratch_shapes=[
            pltpu.VMEM((128, 256), bf16),
            pltpu.VMEM((32, 704), bf16),
            pltpu.VMEM((32, 704), bf16),
            pltpu.VMEM((2, 128, 128), bf16),
            pltpu.SemaphoreType.DMA((7,)),
        ],
        compiler_params=SMALL,
        name="pack",
    )(*(in_hbm(a) for a in (query_one, query_two, key_one, key_two, values, lift_weight, gate_weight)))
    kpool = swapped(ksend, ALL, K_GROUPS)
    qpool = gathered(qsend, ALL, Q_GROUPS).reshape(SIDE, 256, 128)
    part = kpool[:, 512:, :].reshape(SIDE * 352, 128)
    weights = in_hbm(gathered(part, ALL, Q_GROUPS).reshape(SIDE, SIDE, 352, 128))
    out = pl.pallas_call(
        attend_kernel,
        grid=(1,),
        out_shape=jax.ShapeDtypeStruct((SIDE, PACK, 128), bf16),
        in_specs=[
            pl.BlockSpec(memory_space=pltpu.SMEM),
            vmem(),
            pl.BlockSpec((SIDE, 512, 128), lambda i: (0, 0, 0)),
        ],
        out_specs=vmem(),
        scratch_shapes=[pltpu.VMEM((8, 256, 256), f32)],
        compiler_params=SMALL,
        name="attend",
    )(plan, qpool, kpool)
    back = swapped(out, ALL, Q_GROUPS)
    attended = pl.pallas_call(
        join_kernel,
        out_shape=jax.ShapeDtypeStruct((tokens, width), bf16),
        in_specs=[pl.BlockSpec(memory_space=pltpu.SMEM)] + [vmem()] * 3,
        out_specs=vmem(),
        compiler_params=SMALL,
        name="join",
    )(mix_weight, back, head_gain.reshape(1, VD), out_weight)
    parts = swapped(attended.reshape(8, own, width), TP)
    stream, normed = pl.pallas_call(
        norm_kernel,
        out_shape=[
            jax.ShapeDtypeStruct((own, width), f32),
            jax.ShapeDtypeStruct((own, width), bf16),
        ],
        in_specs=[vmem()] * 3,
        out_specs=[vmem()] * 2,
        compiler_params=SMALL,
        name="norm",
    )(parts, residual, norm_gain.reshape(1, width))
    rows = gathered(normed, TP)
    gated, edge = pl.pallas_call(
        gate_kernel,
        out_shape=[
            jax.ShapeDtypeStruct((tokens, MAIN + 128), bf16),
            jax.ShapeDtypeStruct((16, MAIN + 128), bf16),
        ],
        in_specs=[smem, vmem(), hbm],
        out_specs=[vmem()] * 2,
        scratch_shapes=[
            pltpu.VMEM((SIDE, SIDE, 192, 128), bf16),
            pltpu.SemaphoreType.DMA((SIDE,)),
        ],
        compiler_params=SMALL,
        name="gate",
    )(own_core, rows, weights)
    route = [(i, i + 1) for i in range(SIDE * SIDE - 1)]
    prior = lax.ppermute(edge, ("z", "y"), route)
    lifted = pl.pallas_call(
        lift_kernel,
        out_shape=jax.ShapeDtypeStruct((tokens, MAIN), bf16),
        in_specs=[smem, vmem(), hbm],
        out_specs=vmem(),
        scratch_shapes=[
            pltpu.VMEM((SIDE, SIDE, 160, 128), bf16),
            pltpu.SemaphoreType.DMA((SIDE,)),
        ],
        compiler_params=SMALL,
        cost_estimate=pl.CostEstimate(
            flops=2 * 128 * 2048 * 640, bytes_accessed=3 << 20, transcendentals=0
        ),
        name="lift",
    )(own_core, rows, weights)
    gap = jnp.zeros((WIDTH, 64), f32)
    taps = jnp.concatenate([conv_taps[:, :MAIN], gap, conv_taps[:, MAIN:]], axis=1)
    down = pl.pallas_call(
        down_kernel,
        out_shape=jax.ShapeDtypeStruct((tokens, width), bf16),
        in_specs=[vmem()] * 5,
        out_specs=vmem(),
        compiler_params=SMALL,
        name="down",
    )(gated, lifted, prior, taps, down_weight)
    mixer = swapped(down.reshape(8, own, width), TP)
    return pl.pallas_call(
        last_kernel,
        out_shape=jax.ShapeDtypeStruct((own, width), bf16),
        in_specs=[vmem()] * 2,
        out_specs=vmem(),
        compiler_params=SMALL,
        name="last",
    )(mixer, stream)


def solution(mesh):
    fine = Mesh(mesh.devices.reshape(SIDE, SIDE, 4, 2), ("z", "y", "x", "core"))
    sp = ("z", "y")

    return jax.shard_map(
        on_device,
        mesh=fine,
        in_specs=(
            P(sp, TP),
            P(sp, TP),
            P(sp, TP),
            P(sp, TP),
            P(sp, TP),
            P(TP),
            P(),
            P(("z", "y", "x", "core"), None),
            P(TP, None),
            P(),
            P(sp, TP),
            P(sp, TP),
            P(None, TP),
            P(TP, None),
        ),
        out_specs=P(("z", "y", "x", "core"), None),
        check_vma=False,
    )
```

```python
import jax
import jax.numpy as jnp
import numpy as np
from jax import lax
from jax.experimental import pallas as pl
from jax.experimental.pallas import tpu as pltpu
from jax.sharding import Mesh, PartitionSpec as P

HD = 128
VD = 256
STRETCH = 64
WIDTH = 3
SIDE = 8
BLOCK = 128
PACK = 4 * BLOCK + 16
TILES = 5
MAIN = 128 * TILES
SENT = 512 + 352
SHIFTS = (0, 1, -1, 2, -2, 3, -3, 4)
epsilon = 1e-06
masked_score = -1e30
LOG2E = 1.4426950408889634
EXP2_SCALE = LOG2E * HD**-0.5
f32 = jnp.float32
bf16 = jnp.bfloat16
TP = ("x", "core")
ALL = ("z", "y", "x", "core")
PLACES = np.arange(SIDE * SIDE * 8).reshape(SIDE, SIDE, 4, 2)
ROWS = [[PLACES[i, :, x, c].tolist() for i in range(SIDE) for x in range(4)] for c in range(2)]
COLS = [[PLACES[:, i, x, c].tolist() for i in range(SIDE) for x in range(4)] for c in range(2)]
Q_GROUPS = ROWS[0] + COLS[1]
K_GROUPS = COLS[0] + ROWS[1]


def steps(by):
    moved = np.stack(
        [np.roll(PLACES, -by, axis=1)[..., 0], np.roll(PLACES, -by, axis=0)[..., 1]], axis=-1
    )
    return list(zip(PLACES.reshape(-1).tolist(), moved.reshape(-1).tolist()))


UP, DOWN = steps(1), steps(-1)


def vmem():
    return pl.BlockSpec(memory_space=pltpu.VMEM)


def pack_kernel(q1, q2, k1, k2, v, lift, gate, qsend, ksend, vv, ll, gg, kk, sems):
    moves = [
        pltpu.make_async_copy(src, dst, sems.at[i])
        for i, (src, dst) in enumerate(
            (
                (k1, kk.at[0]),
                (k2, kk.at[1]),
                (v, vv),
                (lift, ll),
                (gate, gg),
                (q1, qsend.at[0:128]),
                (q2, qsend.at[128:256]),
            )
        )
    ]
    for move in moves:
        move.start()
    for move in moves:
        move.wait()
    tail = jnp.concatenate([ll[:, MAIN:], gg[:, MAIN:]], axis=1)
    for i in range(SIDE):
        ksend[i, 0:128, :] = kk[0]
        ksend[i, 128:256, :] = kk[1]
        ksend[i, 256:384, :] = vv[:, 0:128]
        ksend[i, 384:512, :] = vv[:, 128:256]
        for n in range(TILES):
            ksend[i, 512 + 32 * n : 544 + 32 * n, :] = gg[:, 128 * n : 128 * n + 128]
            ksend[i, 704 + 32 * n : 736 + 32 * n, :] = ll[:, 128 * n : 128 * n + 128]
        ksend[i, 672:704, :] = tail


def attend_kernel(plan, qpool, kpool, out, scores):
    q_base, q_step, k_base, k_step = (plan[i] for i in range(4))
    first_chunk, pairs = plan[4], plan[5]
    row = lax.broadcasted_iota(jnp.int32, (256, 256), 0)
    col = lax.broadcasted_iota(jnp.int32, (256, 256), 1)
    at = lax.broadcasted_iota(jnp.int32, (16, 128), 0)

    def blank(c, carry):
        for h in range(2):
            out[2 * c + h, 0:512, :] = jnp.zeros((512, 128), bf16)
            level = jnp.where((at == 0) | (at == 3), masked_score, 0.0)
            out[2 * c + h, 512:528, :] = level.astype(bf16)
        return carry

    lax.fori_loop(0, first_chunk, blank, 0)

    def chunk(c, carry):
        queries = [
            jnp.concatenate(
                [qpool[2 * c, 128 * m : 128 * m + 128, :], qpool[2 * c + 1, 128 * m : 128 * m + 128, :]],
                axis=0,
            )
            for m in range(2)
        ]
        q_at = 2 * (q_base + q_step * (2 * c + row // 128)) + (row % 128) // STRETCH

        def scored(p, peaks):
            k_at = 2 * (k_base + k_step * (2 * p + col // 128)) + (col % 128) // STRETCH
            seen = k_at <= q_at
            new = []
            for m in range(2):
                k = jnp.concatenate(
                    [kpool[2 * p, 128 * m : 128 * m + 128, :], kpool[2 * p + 1, 128 * m : 128 * m + 128, :]],
                    axis=0,
                )
                s = lax.dot_general(
                    queries[m], k, (((1,), (1,)), ((), ())), preferred_element_type=f32
                )
                s = jnp.where(seen, s, masked_score)
                scores[2 * p + m] = s
                new.append(jnp.maximum(peaks[m], jnp.maximum(s[:, 0:128], s[:, 128:256])))
            return tuple(new)

        low = jnp.full((256, 128), masked_score, f32)
        peaks = lax.fori_loop(0, pairs, scored, (low, low))
        tops = [jnp.max(peak, axis=-1, keepdims=True) for peak in peaks]

        def weighed(p, carry):
            totals, acc = carry
            new, ws = [], []
            for m in range(2):
                w = jnp.exp2((scores[2 * p + m] - tops[m]) * EXP2_SCALE)
                new.append(totals[m] + (w[:, 0:128] + w[:, 128:256]))
                ws.append(w.astype(bf16))
            va = jnp.concatenate([kpool[2 * p, 256:384, :], kpool[2 * p, 384:512, :]], axis=1)
            vb = jnp.concatenate([kpool[2 * p + 1, 256:384, :], kpool[2 * p + 1, 384:512, :]], axis=1)
            vals = jnp.concatenate([va, vb], axis=0)
            acc = acc + jnp.dot(
                jnp.concatenate(ws, axis=0), vals, preferred_element_type=f32
            )
            return tuple(new), acc

        none = jnp.zeros((256, 128), f32)
        totals, acc = lax.fori_loop(
            0, pairs, weighed, ((none, none), jnp.zeros((512, VD), f32))
        )
        levels = []
        for m in range(2):
            total = jnp.sum(totals[m], axis=-1, keepdims=True)
            o = (acc[256 * m : 256 * m + 256] / total).astype(bf16)
            seen = tops[m] > 0.5 * masked_score
            levels.append(jnp.where(seen, tops[m] * EXP2_SCALE + jnp.log2(total), masked_score))
            for h in range(2):
                for e in range(2):
                    out[2 * c + h, 256 * m + 128 * e : 256 * m + 128 * e + 128, :] = o[
                        128 * h : 128 * h + 128, 128 * e : 128 * e + 128
                    ]
        for h in range(2):
            rows = jnp.zeros((16, 128), f32)
            for m in range(2):
                wide = jnp.transpose(
                    jnp.broadcast_to(levels[m][128 * h : 128 * h + 128], (128, 128))
                )[0:16]
                a = wide.astype(bf16).astype(f32)
                b = (wide - a).astype(bf16).astype(f32)
                d = wide - a - b
                for n, piece in enumerate((a, b, d)):
                    rows = jnp.where(at == 3 * m + n, piece, rows)
            out[2 * c + h, 512:528, :] = rows.astype(bf16)
        return carry

    lax.fori_loop(first_chunk, SIDE // 2, chunk, 0)


def join_kernel(mix, parts, gain, weight, out):
    tails = [parts[i, 512:528, :].astype(f32) for i in range(SIDE)]

    def joined(m):
        levels = jnp.concatenate(
            [jnp.sum(tail[3 * m : 3 * m + 3], axis=0, keepdims=True) for tail in tails], axis=0
        )
        top = jnp.max(levels, axis=0, keepdims=True)
        w = jnp.exp2(levels - top)
        w = w / jnp.sum(w, axis=0, keepdims=True)
        w = jnp.transpose(jnp.concatenate([w, jnp.zeros((120, 128), f32)], axis=0))
        acc = [jnp.zeros((128, 128), f32), jnp.zeros((128, 128), f32)]
        for i in range(SIDE):
            wi = w[:, i : i + 1]
            for e in range(2):
                at = 256 * m + 128 * e
                acc[e] = acc[e] + wi * parts[i, at : at + 128, :].astype(f32)
        return jnp.concatenate(acc, axis=1)

    mixed = joined(0) - mix[0] * joined(1)
    r = lax.rsqrt(jnp.mean(mixed * mixed, axis=-1, keepdims=True) + epsilon)
    head = (mixed * r * gain[...]).astype(bf16)
    out[...] = jnp.dot(head, weight[...], preferred_element_type=f32).astype(bf16)


def norm_kernel(parts, residual, gain, stream, normed):
    att = parts[0].astype(f32)
    for i in range(1, 8):
        att = att + parts[i].astype(f32)
    total = residual[...].astype(f32) + att
    stream[...] = total
    r = lax.rsqrt(jnp.mean(total * total, axis=-1, keepdims=True) + epsilon)
    n = (total * r * gain[...]).astype(bf16)
    for i in range(8):
        normed[i] = n


def fetched(place, pieces, buffer, sems, first):
    height = buffer.shape[2]
    core, me = place[0], place[1]
    rows = pl.ds(first, height)
    for n, (piece, shift) in enumerate(zip(pieces, SHIFTS)):
        at = lax.rem(me + SIDE - shift, SIDE)

        @pl.when(core == 0)
        def _():
            pltpu.make_async_copy(piece.at[:, rows, :], buffer.at[:, at], sems.at[n]).start()

        @pl.when(core != 0)
        def _():
            pltpu.make_async_copy(piece.at[:, rows, :], buffer.at[at], sems.at[n]).start()


def multiplied(rows, pieces, buffer, sems, first):
    height = buffer.shape[2]
    count = height // 32
    acc = [None] * ((count + 1) // 2)
    for n in range(SIDE):
        pltpu.make_async_copy(
            pieces[0].at[:, pl.ds(first, height), :], buffer.at[n], sems.at[n]
        ).wait()
    for g in range(SIDE):
        lhs = rows[:, 256 * g : 256 * g + 256]
        for n in range(0, count, 2):
            tiles = [
                buffer[g, :, 32 * m : 32 * m + 32, :].reshape(256, 128)
                for m in range(n, min(n + 2, count))
            ]
            rhs = jnp.concatenate(tiles, axis=1) if len(tiles) > 1 else tiles[0]
            d = jnp.dot(lhs, rhs, preferred_element_type=f32)
            acc[n // 2] = d if acc[n // 2] is None else acc[n // 2] + d
    return acc


def gate_kernel(place, rows, *refs):
    pieces, (gated, edge, buffer, sems) = refs[:SIDE], refs[SIDE:]
    fetched(place, pieces, buffer, sems, 0)
    for n, part in enumerate(multiplied(rows, pieces, buffer, sems, 0)):
        part = part.astype(bf16)
        gated[:, 256 * n : 256 * n + 256] = part
        edge[:, 256 * n : 256 * n + 256] = part[112:128]


def lift_kernel(place, rows, *refs):
    pieces, (lifted, buffer, sems) = refs[:SIDE], refs[SIDE:]
    fetched(place, pieces, buffer, sems, 192)
    for n, part in enumerate(multiplied(rows, pieces, buffer, sems, 192)):
        lifted[:, 256 * n : 256 * n + part.shape[1]] = part.astype(bf16)


def down_kernel(gated, lifted, prior, taps, weight, out):
    at = lax.broadcasted_iota(jnp.int32, (128, 1), 0)

    def activated(lo, hi):
        g = gated[:, lo:hi].astype(f32)
        p = prior[:, lo:hi].astype(f32)
        one = jnp.where(at == 0, p[15:16], pltpu.roll(g, 1, 0))
        two = jnp.where(at == 0, p[14:15], jnp.where(at == 1, p[15:16], pltpu.roll(g, 2, 0)))
        conv = taps[0:1, lo:hi] * two + taps[1:2, lo:hi] * one + taps[2:3, lo:hi] * g
        return g, conv * jax.nn.sigmoid(conv)

    acc = None
    for n in range(0, MAIN, 128):
        _, a = activated(n, n + 128)
        h = (a * lifted[:, n : n + 128].astype(f32)).astype(bf16)
        d = jnp.dot(h, weight[n : n + 128, :], preferred_element_type=f32)
        acc = d if acc is None else acc + d
    g, a = activated(MAIN, MAIN + 128)
    h = (pltpu.roll(a, 64, 1) * g).astype(bf16)
    acc = acc + jnp.dot(h[:, 0:64], weight[MAIN:, :], preferred_element_type=f32)
    out[...] = acc.astype(bf16)


def last_kernel(parts, stream, out):
    mixer = parts[0].astype(f32)
    for i in range(1, 8):
        mixer = mixer + parts[i].astype(f32)
    out[...] = (stream[...] + mixer).astype(bf16)


def swapped(a, axis, groups=None):
    return lax.all_to_all(a, axis, 0, 0, axis_index_groups=groups, tiled=True)


def gathered(a, axis, groups=None):
    return lax.all_gather(a, axis, axis_index_groups=groups, axis=0, tiled=True)


def in_hbm(a):
    return pltpu.with_memory_space_constraint(a, pltpu.HBM)


SMALL = pltpu.CompilerParams(vmem_limit_bytes=20 << 20)


def on_device(
    query_one,
    key_one,
    query_two,
    key_two,
    values,
    mix_weight,
    head_gain,
    residual,
    out_weight,
    norm_gain,
    lift_weight,
    gate_weight,
    conv_taps,
    down_weight,
):
    tokens = query_one.shape[0]
    own = residual.shape[0]
    width = residual.shape[1]
    z = lax.axis_index("z")
    y = lax.axis_index("y")
    core = lax.axis_index("core")
    along_y = jnp.stack([z * SIDE, 1 + 0 * z, y, SIDE + 0 * z, 0 * z, z // 2 + 1])
    along_z = jnp.stack([y, SIDE + 0 * z, z * SIDE, 1 + 0 * z, z // 2, SIDE // 2 + 0 * z])
    plan = jnp.where(core == 0, along_y, along_z).astype(jnp.int32)
    smem = pl.BlockSpec(memory_space=pltpu.SMEM)
    hbm = pl.BlockSpec(memory_space=pltpu.HBM)
    place = jnp.stack([core, jnp.where(core == 0, y, z)]).astype(jnp.int32)
    qsend, ksend = pl.pallas_call(
        pack_kernel,
        out_shape=[
            jax.ShapeDtypeStruct((256, 128), bf16),
            jax.ShapeDtypeStruct((SIDE, SENT, 128), bf16),
        ],
        in_specs=[hbm] * 7,
        out_specs=[vmem()] * 2,
        scratch_shapes=[
            pltpu.VMEM((128, 256), bf16),
            pltpu.VMEM((32, 704), bf16),
            pltpu.VMEM((32, 704), bf16),
            pltpu.VMEM((2, 128, 128), bf16),
            pltpu.SemaphoreType.DMA((7,)),
        ],
        compiler_params=SMALL,
        name="pack",
    )(*(in_hbm(a) for a in (query_one, query_two, key_one, key_two, values, lift_weight, gate_weight)))
    kpool = swapped(ksend, ALL, K_GROUPS)
    qpool = gathered(qsend, ALL, Q_GROUPS).reshape(SIDE, 256, 128)
    out = pl.pallas_call(
        attend_kernel,
        grid=(1,),
        out_shape=pltpu.HBM((SIDE, PACK, 128), bf16),
        in_specs=[
            pl.BlockSpec(memory_space=pltpu.SMEM),
            vmem(),
            pl.BlockSpec((SIDE, 512, 128), lambda i: (0, 0, 0)),
        ],
        out_specs=vmem(),
        scratch_shapes=[pltpu.VMEM((8, 256, 256), f32)],
        compiler_params=SMALL,
        name="attend",
    )(plan, qpool, kpool)
    kpool, out = lax.optimization_barrier((kpool, out))
    back = swapped(out, ALL, Q_GROUPS)
    piece = kpool[:, 512:, :].reshape(SIDE * 352, 128)
    above, below = lax.ppermute(piece, ALL, UP), lax.ppermute(piece, ALL, DOWN)
    above_two, below_two = lax.ppermute(above, ALL, UP), lax.ppermute(below, ALL, DOWN)
    attended = pl.pallas_call(
        join_kernel,
        out_shape=jax.ShapeDtypeStruct((tokens, width), bf16),
        in_specs=[pl.BlockSpec(memory_space=pltpu.SMEM)] + [vmem()] * 3,
        out_specs=vmem(),
        compiler_params=SMALL,
        name="join",
    )(mix_weight, back, head_gain.reshape(1, VD), out_weight)
    attended, above_two, below_two = lax.optimization_barrier((attended, above_two, below_two))
    parts = swapped(attended.reshape(8, own, width), TP)
    above_three = lax.ppermute(above_two, ALL, UP)
    below_three = lax.ppermute(below_two, ALL, DOWN)
    stream, normed = pl.pallas_call(
        norm_kernel,
        out_shape=[
            jax.ShapeDtypeStruct((own, width), f32),
            jax.ShapeDtypeStruct((8, own, width), bf16),
        ],
        in_specs=[vmem()] * 3,
        out_specs=[vmem()] * 2,
        compiler_params=SMALL,
        name="norm",
    )(parts, residual, norm_gain.reshape(1, width))
    normed, above_three = lax.optimization_barrier((normed, above_three))
    rows = swapped(normed, TP).reshape(tokens, width)
    above_four = lax.ppermute(above_three, ALL, UP)
    pieces = [piece, above, below, above_two, below_two, above_three, below_three, above_four]
    pieces = [p.reshape(SIDE, 352, 128) for p in pieces]
    gated, edge = pl.pallas_call(
        gate_kernel,
        out_shape=[
            jax.ShapeDtypeStruct((tokens, MAIN + 128), bf16),
            jax.ShapeDtypeStruct((16, MAIN + 128), bf16),
        ],
        in_specs=[smem, vmem()] + [pl.BlockSpec(memory_space=pl.ANY)] * SIDE,
        out_specs=[vmem()] * 2,
        scratch_shapes=[
            pltpu.VMEM((SIDE, SIDE, 192, 128), bf16),
            pltpu.SemaphoreType.DMA((SIDE,)),
        ],
        compiler_params=SMALL,
        name="gate",
    )(place, rows, *pieces)
    route = [(i, i + 1) for i in range(SIDE * SIDE - 1)]
    prior = lax.ppermute(edge, ("z", "y"), route)
    lifted = pl.pallas_call(
        lift_kernel,
        out_shape=jax.ShapeDtypeStruct((tokens, MAIN), bf16),
        in_specs=[smem, vmem()] + [pl.BlockSpec(memory_space=pl.ANY)] * SIDE,
        out_specs=vmem(),
        scratch_shapes=[
            pltpu.VMEM((SIDE, SIDE, 160, 128), bf16),
            pltpu.SemaphoreType.DMA((SIDE,)),
        ],
        compiler_params=SMALL,
        cost_estimate=pl.CostEstimate(
            flops=2 * 128 * 2048 * 640, bytes_accessed=3 << 20, transcendentals=0
        ),
        name="lift",
    )(place, rows, *pieces)
    gap = jnp.zeros((WIDTH, 64), f32)
    taps = jnp.concatenate([conv_taps[:, :MAIN], gap, conv_taps[:, MAIN:]], axis=1)
    down = pl.pallas_call(
        down_kernel,
        out_shape=jax.ShapeDtypeStruct((tokens, width), bf16),
        in_specs=[vmem()] * 5,
        out_specs=vmem(),
        compiler_params=SMALL,
        name="down",
    )(gated, lifted, prior, taps, down_weight)
    mixer = swapped(down.reshape(8, own, width), TP)
    return pl.pallas_call(
        last_kernel,
        out_shape=jax.ShapeDtypeStruct((own, width), bf16),
        in_specs=[vmem()] * 2,
        out_specs=vmem(),
        compiler_params=SMALL,
        name="last",
    )(mixer, stream)


def solution(mesh):
    fine = Mesh(mesh.devices.reshape(SIDE, SIDE, 4, 2), ("z", "y", "x", "core"))
    sp = ("z", "y")

    return jax.shard_map(
        on_device,
        mesh=fine,
        in_specs=(
            P(sp, TP),
            P(sp, TP),
            P(sp, TP),
            P(sp, TP),
            P(sp, TP),
            P(TP),
            P(),
            P(("z", "y", "x", "core"), None),
            P(TP, None),
            P(),
            P(sp, TP),
            P(sp, TP),
            P(None, TP),
            P(TP, None),
        ),
        out_specs=P(("z", "y", "x", "core"), None),
        check_vma=False,
    )
```

```python
import jax
import jax.numpy as jnp
import numpy as np
from jax import lax
from jax.experimental import pallas as pl
from jax.experimental.pallas import tpu as pltpu
from jax.sharding import Mesh, PartitionSpec as P

HD = 128
VD = 256
STRETCH = 64
WIDTH = 3
SIDE = 8
BLOCK = 128
PACK = 4 * BLOCK + 16
TILES = 5
MAIN = 128 * TILES
SENT = 512 + 352
SHIFTS = (0, 1, -1, 2)
epsilon = 1e-06
masked_score = -1e30
LOG2E = 1.4426950408889634
EXP2_SCALE = LOG2E * HD**-0.5
f32 = jnp.float32
bf16 = jnp.bfloat16
TP = ("x", "core")
ALL = ("z", "y", "x", "core")
PLACES = np.arange(SIDE * SIDE * 8).reshape(SIDE, SIDE, 4, 2)
ROWS = [[PLACES[i, :, x, c].tolist() for i in range(SIDE) for x in range(4)] for c in range(2)]
COLS = [[PLACES[:, i, x, c].tolist() for i in range(SIDE) for x in range(4)] for c in range(2)]
Q_GROUPS = ROWS[0] + COLS[1]
K_GROUPS = COLS[0] + ROWS[1]


def vmem():
    return pl.BlockSpec(memory_space=pltpu.VMEM)


def pack_kernel(q1, q2, k1, k2, v, lift, gate, qsend, ksend, vv, ll, gg, rows, sems, sent):
    moves = [
        pltpu.make_async_copy(src, dst, sems.at[i])
        for i, (src, dst) in enumerate(
            (
                (k1, rows.at[0:128]),
                (k2, rows.at[128:256]),
                (v, vv),
                (lift, ll),
                (gate, gg),
                (q1, qsend.at[0:128]),
                (q2, qsend.at[128:256]),
            )
        )
    ]
    for move in moves:
        move.start()
    for move in moves:
        move.wait()
    rows[256:384, :] = vv[:, 0:128]
    rows[384:512, :] = vv[:, 128:256]
    for n in range(TILES):
        rows[512 + 32 * n : 544 + 32 * n, :] = gg[:, 128 * n : 128 * n + 128]
        rows[704 + 32 * n : 736 + 32 * n, :] = ll[:, 128 * n : 128 * n + 128]
    rows[672:704, :] = jnp.concatenate([ll[:, MAIN:], gg[:, MAIN:]], axis=1)
    copies = [pltpu.make_async_copy(rows, ksend.at[i], sent.at[i]) for i in range(SIDE)]
    for copy in copies:
        copy.start()
    for copy in copies:
        copy.wait()


def attend_kernel(plan, qpool, kpool, out, scores):
    q_base, q_step, k_base, k_step = (plan[i] for i in range(4))
    first_chunk, pairs = plan[4], plan[5]
    row = lax.broadcasted_iota(jnp.int32, (256, 256), 0)
    col = lax.broadcasted_iota(jnp.int32, (256, 256), 1)
    at = lax.broadcasted_iota(jnp.int32, (16, 128), 0)

    def blank(c, carry):
        for h in range(2):
            out[2 * c + h, 0:512, :] = jnp.zeros((512, 128), bf16)
            level = jnp.where((at == 0) | (at == 3), masked_score, 0.0)
            out[2 * c + h, 512:528, :] = level.astype(bf16)
        return carry

    lax.fori_loop(0, first_chunk, blank, 0)

    def chunk(c, carry):
        queries = [
            jnp.concatenate(
                [qpool[2 * c, 128 * m : 128 * m + 128, :], qpool[2 * c + 1, 128 * m : 128 * m + 128, :]],
                axis=0,
            )
            for m in range(2)
        ]
        q_at = 2 * (q_base + q_step * (2 * c + row // 128)) + (row % 128) // STRETCH

        def scored(p, peaks):
            k_at = 2 * (k_base + k_step * (2 * p + col // 128)) + (col % 128) // STRETCH
            seen = k_at <= q_at
            new = []
            for m in range(2):
                k = jnp.concatenate(
                    [kpool[2 * p, 128 * m : 128 * m + 128, :], kpool[2 * p + 1, 128 * m : 128 * m + 128, :]],
                    axis=0,
                )
                s = lax.dot_general(
                    queries[m], k, (((1,), (1,)), ((), ())), preferred_element_type=f32
                )
                s = jnp.where(seen, s, masked_score)
                scores[2 * p + m] = s
                new.append(jnp.maximum(peaks[m], jnp.maximum(s[:, 0:128], s[:, 128:256])))
            return tuple(new)

        low = jnp.full((256, 128), masked_score, f32)
        peaks = lax.fori_loop(0, pairs, scored, (low, low))
        tops = [jnp.max(peak, axis=-1, keepdims=True) for peak in peaks]

        def weighed(p, carry):
            totals, acc = carry
            new, ws = [], []
            for m in range(2):
                w = jnp.exp2((scores[2 * p + m] - tops[m]) * EXP2_SCALE)
                new.append(totals[m] + (w[:, 0:128] + w[:, 128:256]))
                ws.append(w.astype(bf16))
            va = jnp.concatenate([kpool[2 * p, 256:384, :], kpool[2 * p, 384:512, :]], axis=1)
            vb = jnp.concatenate([kpool[2 * p + 1, 256:384, :], kpool[2 * p + 1, 384:512, :]], axis=1)
            vals = jnp.concatenate([va, vb], axis=0)
            acc = acc + jnp.dot(
                jnp.concatenate(ws, axis=0), vals, preferred_element_type=f32
            )
            return tuple(new), acc

        none = jnp.zeros((256, 128), f32)
        totals, acc = lax.fori_loop(
            0, pairs, weighed, ((none, none), jnp.zeros((512, VD), f32))
        )
        levels = []
        for m in range(2):
            total = jnp.sum(totals[m], axis=-1, keepdims=True)
            o = (acc[256 * m : 256 * m + 256] / total).astype(bf16)
            seen = tops[m] > 0.5 * masked_score
            levels.append(jnp.where(seen, tops[m] * EXP2_SCALE + jnp.log2(total), masked_score))
            for h in range(2):
                for e in range(2):
                    out[2 * c + h, 256 * m + 128 * e : 256 * m + 128 * e + 128, :] = o[
                        128 * h : 128 * h + 128, 128 * e : 128 * e + 128
                    ]
        for h in range(2):
            rows = jnp.zeros((16, 128), f32)
            for m in range(2):
                wide = jnp.transpose(
                    jnp.broadcast_to(levels[m][128 * h : 128 * h + 128], (128, 128))
                )[0:16]
                a = wide.astype(bf16).astype(f32)
                b = (wide - a).astype(bf16).astype(f32)
                d = wide - a - b
                for n, piece in enumerate((a, b, d)):
                    rows = jnp.where(at == 3 * m + n, piece, rows)
            out[2 * c + h, 512:528, :] = rows.astype(bf16)
        return carry

    lax.fori_loop(first_chunk, SIDE // 2, chunk, 0)


def join_kernel(mix, parts, gain, out):
    tails = [parts[i, 512:528, :].astype(f32) for i in range(SIDE)]

    def joined(m):
        levels = jnp.concatenate(
            [jnp.sum(tail[3 * m : 3 * m + 3], axis=0, keepdims=True) for tail in tails], axis=0
        )
        top = jnp.max(levels, axis=0, keepdims=True)
        w = jnp.exp2(levels - top)
        w = w / jnp.sum(w, axis=0, keepdims=True)
        w = jnp.transpose(jnp.concatenate([w, jnp.zeros((120, 128), f32)], axis=0))
        acc = [jnp.zeros((128, 128), f32), jnp.zeros((128, 128), f32)]
        for i in range(SIDE):
            wi = w[:, i : i + 1]
            for e in range(2):
                at = 256 * m + 128 * e
                acc[e] = acc[e] + wi * parts[i, at : at + 128, :].astype(f32)
        return jnp.concatenate(acc, axis=1)

    mixed = joined(0) - mix[0] * joined(1)
    r = lax.rsqrt(jnp.mean(mixed * mixed, axis=-1, keepdims=True) + epsilon)
    head = (mixed * r * gain[...]).astype(bf16)
    for i in range(4):
        out[i] = head


def project_kernel(place, heads, *refs):
    weights, (half, sent, buffer, sems) = refs[:4], refs[4:]
    x = place[1]
    moves = [
        pltpu.make_async_copy(weight, buffer.at[i], sems.at[i]) for i, weight in enumerate(weights)
    ]
    for move in moves:
        move.start()
    for i, shift in enumerate(SHIFTS):
        moves[i].wait()
        head = heads[lax.rem(x + 4 - shift, 4)]
        for n in range(0, 2048, 256):
            d = jnp.dot(head, buffer[i, :, n : n + 256], preferred_element_type=f32)
            if i > 0:
                d = d + half[:, n : n + 256]
            half[:, n : n + 256] = d
            if i == 3:
                sent[:, n : n + 256] = d.astype(bf16)


def fetched(core, weights, buffer, sems, first):
    height = buffer.shape[2]
    for g in range(SIDE):
        rows = pl.ds(first, height)

        @pl.when(core == 0)
        def _():
            pltpu.make_async_copy(weights.at[:, g, rows, :], buffer.at[g], sems.at[g]).start()

        @pl.when(core != 0)
        def _():
            pltpu.make_async_copy(weights.at[g, :, rows, :], buffer.at[g], sems.at[g]).start()


def multiplied(rows, weights, buffer, sems, first):
    height = buffer.shape[2]
    count = height // 32
    acc = [None] * ((count + 1) // 2)
    for g in range(SIDE):
        pltpu.make_async_copy(
            weights.at[0, :, pl.ds(first, height), :], buffer.at[g], sems.at[g]
        ).wait()
        lhs = rows[:, 256 * g : 256 * g + 256]
        for n in range(0, count, 2):
            tiles = [
                buffer[g, :, 32 * m : 32 * m + 32, :].reshape(256, 128)
                for m in range(n, min(n + 2, count))
            ]
            rhs = jnp.concatenate(tiles, axis=1) if len(tiles) > 1 else tiles[0]
            d = jnp.dot(lhs, rhs, preferred_element_type=f32)
            acc[n // 2] = d if acc[n // 2] is None else acc[n // 2] + d
    return acc


def gate_kernel(place, half, other, residual, gain, weights, gated, edge, rows, stream, buffer, sems):
    fetched(place[0], weights, buffer, sems, 0)
    for n in range(0, 128, 32):
        total = residual[n : n + 32].astype(f32) + (
            half[n : n + 32] + other[n : n + 32].astype(f32)
        )
        r = lax.rsqrt(jnp.mean(total * total, axis=-1, keepdims=True) + epsilon)
        rows[n : n + 32] = (total * r * gain[...]).astype(bf16)
    own = pl.ds(pl.multiple_of(place[2] * 16, 16), 16)
    stream[...] = residual[own].astype(f32) + (half[own] + other[own].astype(f32))
    for n, part in enumerate(multiplied(rows, weights, buffer, sems, 0)):
        part = part.astype(bf16)
        gated[:, 256 * n : 256 * n + 256] = part
        edge[:, 256 * n : 256 * n + 256] = part[112:128]


def lift_kernel(core, rows, weights, lifted, buffer, sems):
    fetched(core[0], weights, buffer, sems, 192)
    for n, part in enumerate(multiplied(rows, weights, buffer, sems, 192)):
        lifted[:, 256 * n : 256 * n + part.shape[1]] = part.astype(bf16)


def down_kernel(gated, lifted, prior, taps, weight, out):
    at = lax.broadcasted_iota(jnp.int32, (128, 1), 0)

    def activated(lo, hi):
        g = gated[:, lo:hi].astype(f32)
        p = prior[:, lo:hi].astype(f32)
        one = jnp.where(at == 0, p[15:16], pltpu.roll(g, 1, 0))
        two = jnp.where(at == 0, p[14:15], jnp.where(at == 1, p[15:16], pltpu.roll(g, 2, 0)))
        conv = taps[0:1, lo:hi] * two + taps[1:2, lo:hi] * one + taps[2:3, lo:hi] * g
        return g, conv * jax.nn.sigmoid(conv)

    acc = None
    for n in range(0, MAIN, 128):
        _, a = activated(n, n + 128)
        h = (a * lifted[:, n : n + 128].astype(f32)).astype(bf16)
        d = jnp.dot(h, weight[n : n + 128, :], preferred_element_type=f32)
        acc = d if acc is None else acc + d
    g, a = activated(MAIN, MAIN + 128)
    h = (pltpu.roll(a, 64, 1) * g).astype(bf16)
    acc = acc + jnp.dot(h[:, 0:64], weight[MAIN:, :], preferred_element_type=f32)
    out[...] = acc.astype(bf16)


def last_kernel(parts, stream, out):
    mixer = parts[0].astype(f32)
    for i in range(1, 8):
        mixer = mixer + parts[i].astype(f32)
    out[...] = (stream[...] + mixer).astype(bf16)


def swapped(a, axis, groups=None):
    return lax.all_to_all(a, axis, 0, 0, axis_index_groups=groups, tiled=True)


def gathered(a, axis, groups=None):
    return lax.all_gather(a, axis, axis_index_groups=groups, axis=0, tiled=True)


def in_hbm(a):
    return pltpu.with_memory_space_constraint(a, pltpu.HBM)


SMALL = pltpu.CompilerParams(vmem_limit_bytes=20 << 20)


def on_device(
    query_one,
    key_one,
    query_two,
    key_two,
    values,
    mix_weight,
    head_gain,
    residual,
    out_weight,
    norm_gain,
    lift_weight,
    gate_weight,
    conv_taps,
    down_weight,
):
    tokens = query_one.shape[0]
    own = residual.shape[0]
    width = residual.shape[1]
    z = lax.axis_index("z")
    y = lax.axis_index("y")
    core = lax.axis_index("core")
    along_y = jnp.stack([z * SIDE, 1 + 0 * z, y, SIDE + 0 * z, 0 * z, z // 2 + 1])
    along_z = jnp.stack([y, SIDE + 0 * z, z * SIDE, 1 + 0 * z, z // 2, SIDE // 2 + 0 * z])
    plan = jnp.where(core == 0, along_y, along_z).astype(jnp.int32)
    smem = pl.BlockSpec(memory_space=pltpu.SMEM)
    hbm = pl.BlockSpec(memory_space=pltpu.HBM)
    x = lax.axis_index("x")
    place = jnp.stack([core, x, 2 * x + core]).astype(jnp.int32)
    above = lax.ppermute(out_weight, "x", [(i, (i + 1) % 4) for i in range(4)])
    below = lax.ppermute(out_weight, "x", [(i, (i + 3) % 4) for i in range(4)])
    qsend, ksend = pl.pallas_call(
        pack_kernel,
        out_shape=[
            jax.ShapeDtypeStruct((256, 128), bf16),
            jax.ShapeDtypeStruct((SIDE, SENT, 128), bf16),
        ],
        in_specs=[hbm] * 7,
        out_specs=[vmem(), hbm],
        scratch_shapes=[
            pltpu.VMEM((128, 256), bf16),
            pltpu.VMEM((32, 704), bf16),
            pltpu.VMEM((32, 704), bf16),
            pltpu.VMEM((SENT, 128), bf16),
            pltpu.SemaphoreType.DMA((7,)),
            pltpu.SemaphoreType.DMA((SIDE,)),
        ],
        compiler_params=SMALL,
        name="pack",
    )(*(in_hbm(a) for a in (query_one, query_two, key_one, key_two, values, lift_weight, gate_weight)))
    kpool = swapped(ksend, ALL, K_GROUPS)
    qpool = gathered(qsend, ALL, Q_GROUPS).reshape(SIDE, 256, 128)
    part = kpool[:, 512:, :].reshape(SIDE * 352, 128)
    weights = in_hbm(gathered(part, ALL, Q_GROUPS).reshape(SIDE, SIDE, 352, 128))
    out = pl.pallas_call(
        attend_kernel,
        grid=(1,),
        out_shape=jax.ShapeDtypeStruct((SIDE, PACK, 128), bf16),
        in_specs=[
            pl.BlockSpec(memory_space=pltpu.SMEM),
            vmem(),
            pl.BlockSpec((SIDE, 512, 128), lambda i: (0, 0, 0)),
        ],
        out_specs=vmem(),
        scratch_shapes=[pltpu.VMEM((8, 256, 256), f32)],
        compiler_params=SMALL,
        name="attend",
    )(plan, qpool, kpool)
    back = swapped(out, ALL, Q_GROUPS)
    before = gathered(residual, TP)
    across = lax.ppermute(above, "x", [(i, (i + 1) % 4) for i in range(4)])
    heads = pl.pallas_call(
        join_kernel,
        out_shape=jax.ShapeDtypeStruct((4, tokens, VD), bf16),
        in_specs=[pl.BlockSpec(memory_space=pltpu.SMEM)] + [vmem()] * 2,
        out_specs=vmem(),
        compiler_params=SMALL,
        name="join",
    )(mix_weight, back, head_gain.reshape(1, VD))
    heads = swapped(heads, "x")
    half, sent = pl.pallas_call(
        project_kernel,
        out_shape=[
            jax.ShapeDtypeStruct((tokens, width), f32),
            jax.ShapeDtypeStruct((tokens, width), bf16),
        ],
        in_specs=[smem, vmem()] + [pl.BlockSpec(memory_space=pl.ANY)] * 4,
        out_specs=[vmem()] * 2,
        scratch_shapes=[pltpu.VMEM((4, VD, 2048), bf16), pltpu.SemaphoreType.DMA((4,))],
        compiler_params=SMALL,
        name="project",
    )(place, heads, out_weight, above, below, across)
    other = lax.ppermute(sent, "core", [(0, 1), (1, 0)])
    gated, edge, rows, stream = pl.pallas_call(
        gate_kernel,
        out_shape=[
            jax.ShapeDtypeStruct((tokens, MAIN + 128), bf16),
            jax.ShapeDtypeStruct((16, MAIN + 128), bf16),
            jax.ShapeDtypeStruct((tokens, width), bf16),
            jax.ShapeDtypeStruct((own, width), f32),
        ],
        in_specs=[smem] + [vmem()] * 4 + [hbm],
        out_specs=[vmem()] * 4,
        scratch_shapes=[
            pltpu.VMEM((SIDE, SIDE, 192, 128), bf16),
            pltpu.SemaphoreType.DMA((SIDE,)),
        ],
        compiler_params=SMALL,
        name="gate",
    )(place, half, other, before, norm_gain.reshape(1, width), weights)
    route = [(i, i + 1) for i in range(SIDE * SIDE - 1)]
    prior = lax.ppermute(edge, ("z", "y"), route)
    lifted = pl.pallas_call(
        lift_kernel,
        out_shape=jax.ShapeDtypeStruct((tokens, MAIN), bf16),
        in_specs=[smem, vmem(), hbm],
        out_specs=vmem(),
        scratch_shapes=[
            pltpu.VMEM((SIDE, SIDE, 160, 128), bf16),
            pltpu.SemaphoreType.DMA((SIDE,)),
        ],
        compiler_params=SMALL,
        cost_estimate=pl.CostEstimate(
            flops=2 * 128 * 2048 * 640, bytes_accessed=3 << 20, transcendentals=0
        ),
        name="lift",
    )(place, rows, weights)
    gap = jnp.zeros((WIDTH, 64), f32)
    taps = jnp.concatenate([conv_taps[:, :MAIN], gap, conv_taps[:, MAIN:]], axis=1)
    down = pl.pallas_call(
        down_kernel,
        out_shape=jax.ShapeDtypeStruct((tokens, width), bf16),
        in_specs=[vmem()] * 5,
        out_specs=vmem(),
        compiler_params=SMALL,
        name="down",
    )(gated, lifted, prior, taps, down_weight)
    mixer = swapped(down.reshape(8, own, width), TP)
    return pl.pallas_call(
        last_kernel,
        out_shape=jax.ShapeDtypeStruct((own, width), bf16),
        in_specs=[vmem()] * 2,
        out_specs=vmem(),
        compiler_params=SMALL,
        name="last",
    )(mixer, stream)


def solution(mesh):
    fine = Mesh(mesh.devices.reshape(SIDE, SIDE, 4, 2), ("z", "y", "x", "core"))
    sp = ("z", "y")

    return jax.shard_map(
        on_device,
        mesh=fine,
        in_specs=(
            P(sp, TP),
            P(sp, TP),
            P(sp, TP),
            P(sp, TP),
            P(sp, TP),
            P(TP),
            P(),
            P(("z", "y", "x", "core"), None),
            P(TP, None),
            P(),
            P(sp, TP),
            P(sp, TP),
            P(None, TP),
            P(TP, None),
        ),
        out_specs=P(("z", "y", "x", "core"), None),
        check_vma=False,
    )
```

```python
import jax
import jax.numpy as jnp
import numpy as np
from jax import lax
from jax.experimental import pallas as pl
from jax.experimental.pallas import tpu as pltpu
from jax.sharding import Mesh, PartitionSpec as P

HD = 128
VD = 256
STRETCH = 64
WIDTH = 3
SIDE = 8
BLOCK = 128
PACK = 4 * BLOCK + 16
TILES = 5
MAIN = 128 * TILES
SENT = 512 + 352
SHIFTS = (0, 1, -1, 2)
epsilon = 1e-06
masked_score = -1e30
LOG2E = 1.4426950408889634
EXP2_SCALE = LOG2E * HD**-0.5
f32 = jnp.float32
bf16 = jnp.bfloat16
TP = ("x", "core")
ALL = ("z", "y", "x", "core")
PLACES = np.arange(SIDE * SIDE * 8).reshape(SIDE, SIDE, 4, 2)
ROWS = [[PLACES[i, :, x, c].tolist() for i in range(SIDE) for x in range(4)] for c in range(2)]
COLS = [[PLACES[:, i, x, c].tolist() for i in range(SIDE) for x in range(4)] for c in range(2)]
Q_GROUPS = ROWS[0] + COLS[1]
K_GROUPS = COLS[0] + ROWS[1]


def vmem():
    return pl.BlockSpec(memory_space=pltpu.VMEM)


def pack_kernel(q1, q2, k1, k2, v, lift, gate, qsend, ksend, vv, ll, gg, rows, sems, sent):
    moves = [
        pltpu.make_async_copy(src, dst, sems.at[i])
        for i, (src, dst) in enumerate(
            (
                (k1, rows.at[0:128]),
                (k2, rows.at[128:256]),
                (v, vv),
                (lift, ll),
                (gate, gg),
                (q1, qsend.at[0:128]),
                (q2, qsend.at[128:256]),
            )
        )
    ]
    for move in moves:
        move.start()
    for move in moves:
        move.wait()
    rows[256:384, :] = vv[:, 0:128]
    rows[384:512, :] = vv[:, 128:256]
    for n in range(TILES):
        rows[512 + 32 * n : 544 + 32 * n, :] = gg[:, 128 * n : 128 * n + 128]
        rows[704 + 32 * n : 736 + 32 * n, :] = ll[:, 128 * n : 128 * n + 128]
    rows[672:704, :] = jnp.concatenate([ll[:, MAIN:], gg[:, MAIN:]], axis=1)
    copies = [pltpu.make_async_copy(rows, ksend.at[i], sent.at[i]) for i in range(SIDE)]
    for copy in copies:
        copy.start()
    for copy in copies:
        copy.wait()


def attend_kernel(plan, qpool, kpool, out, scores):
    q_base, q_step, k_base, k_step = (plan[i] for i in range(4))
    first_chunk, pairs = plan[4], plan[5]
    row = lax.broadcasted_iota(jnp.int32, (256, 256), 0)
    col = lax.broadcasted_iota(jnp.int32, (256, 256), 1)
    at = lax.broadcasted_iota(jnp.int32, (16, 128), 0)

    def blank(c, carry):
        for h in range(2):
            out[2 * c + h, 0:512, :] = jnp.zeros((512, 128), bf16)
            level = jnp.where((at == 0) | (at == 3), masked_score, 0.0)
            out[2 * c + h, 512:528, :] = level.astype(bf16)
        return carry

    lax.fori_loop(0, first_chunk, blank, 0)

    def chunk(c, carry):
        queries = [
            jnp.concatenate(
                [qpool[2 * c, 128 * m : 128 * m + 128, :], qpool[2 * c + 1, 128 * m : 128 * m + 128, :]],
                axis=0,
            )
            for m in range(2)
        ]
        q_at = 2 * (q_base + q_step * (2 * c + row // 128)) + (row % 128) // STRETCH

        def scored(p, peaks):
            k_at = 2 * (k_base + k_step * (2 * p + col // 128)) + (col % 128) // STRETCH
            seen = k_at <= q_at
            new = []
            for m in range(2):
                k = jnp.concatenate(
                    [kpool[2 * p, 128 * m : 128 * m + 128, :], kpool[2 * p + 1, 128 * m : 128 * m + 128, :]],
                    axis=0,
                )
                s = lax.dot_general(
                    queries[m], k, (((1,), (1,)), ((), ())), preferred_element_type=f32
                )
                s = jnp.where(seen, s, masked_score)
                scores[2 * p + m] = s
                new.append(jnp.maximum(peaks[m], jnp.maximum(s[:, 0:128], s[:, 128:256])))
            return tuple(new)

        low = jnp.full((256, 128), masked_score, f32)
        peaks = lax.fori_loop(0, pairs, scored, (low, low))
        tops = [jnp.max(peak, axis=-1, keepdims=True) for peak in peaks]

        def weighed(p, carry):
            totals, acc = carry
            new, ws = [], []
            for m in range(2):
                w = jnp.exp2((scores[2 * p + m] - tops[m]) * EXP2_SCALE)
                new.append(totals[m] + (w[:, 0:128] + w[:, 128:256]))
                ws.append(w.astype(bf16))
            va = jnp.concatenate([kpool[2 * p, 256:384, :], kpool[2 * p, 384:512, :]], axis=1)
            vb = jnp.concatenate([kpool[2 * p + 1, 256:384, :], kpool[2 * p + 1, 384:512, :]], axis=1)
            vals = jnp.concatenate([va, vb], axis=0)
            acc = acc + jnp.dot(
                jnp.concatenate(ws, axis=0), vals, preferred_element_type=f32
            )
            return tuple(new), acc

        none = jnp.zeros((256, 128), f32)
        totals, acc = lax.fori_loop(
            0, pairs, weighed, ((none, none), jnp.zeros((512, VD), f32))
        )
        levels = []
        for m in range(2):
            total = jnp.sum(totals[m], axis=-1, keepdims=True)
            o = (acc[256 * m : 256 * m + 256] / total).astype(bf16)
            seen = tops[m] > 0.5 * masked_score
            levels.append(jnp.where(seen, tops[m] * EXP2_SCALE + jnp.log2(total), masked_score))
            for h in range(2):
                for e in range(2):
                    out[2 * c + h, 256 * m + 128 * e : 256 * m + 128 * e + 128, :] = o[
                        128 * h : 128 * h + 128, 128 * e : 128 * e + 128
                    ]
        for h in range(2):
            rows = jnp.zeros((16, 128), f32)
            for m in range(2):
                wide = jnp.transpose(
                    jnp.broadcast_to(levels[m][128 * h : 128 * h + 128], (128, 128))
                )[0:16]
                a = wide.astype(bf16).astype(f32)
                b = (wide - a).astype(bf16).astype(f32)
                d = wide - a - b
                for n, piece in enumerate((a, b, d)):
                    rows = jnp.where(at == 3 * m + n, piece, rows)
            out[2 * c + h, 512:528, :] = rows.astype(bf16)
        return carry

    lax.fori_loop(first_chunk, SIDE // 2, chunk, 0)


def join_kernel(mix, parts, gain, out):
    tails = [parts[i, 512:528, :].astype(f32) for i in range(SIDE)]

    def joined(m):
        levels = jnp.concatenate(
            [jnp.sum(tail[3 * m : 3 * m + 3], axis=0, keepdims=True) for tail in tails], axis=0
        )
        top = jnp.max(levels, axis=0, keepdims=True)
        w = jnp.exp2(levels - top)
        w = w / jnp.sum(w, axis=0, keepdims=True)
        w = jnp.transpose(jnp.concatenate([w, jnp.zeros((120, 128), f32)], axis=0))
        acc = [jnp.zeros((128, 128), f32), jnp.zeros((128, 128), f32)]
        for i in range(SIDE):
            wi = w[:, i : i + 1]
            for e in range(2):
                at = 256 * m + 128 * e
                acc[e] = acc[e] + wi * parts[i, at : at + 128, :].astype(f32)
        return jnp.concatenate(acc, axis=1)

    mixed = joined(0) - mix[0] * joined(1)
    r = lax.rsqrt(jnp.mean(mixed * mixed, axis=-1, keepdims=True) + epsilon)
    head = (mixed * r * gain[...]).astype(bf16)
    for i in range(4):
        out[i] = head


def project_kernel(place, heads, *refs):
    weights, (half, sent, buffer, sems) = refs[:5], refs[5:]
    x = place[1]
    slots = [buffer.at[0], buffer.at[1], buffer.at[2], buffer.at[3, 0:128], buffer.at[3, 128:256]]
    moves = [
        pltpu.make_async_copy(weight, slot, sems.at[i])
        for i, (weight, slot) in enumerate(zip(weights, slots))
    ]
    for move in moves:
        move.start()
    for i, shift in enumerate(SHIFTS):
        moves[i].wait()
        if i == 3:
            moves[4].wait()
        head = heads[lax.rem(x + 4 - shift, 4)]
        for n in range(0, 2048, 256):
            d = jnp.dot(head, buffer[i, :, n : n + 256], preferred_element_type=f32)
            if i > 0:
                d = d + half[:, n : n + 256]
            half[:, n : n + 256] = d
            if i == 3:
                sent[:, n : n + 256] = d.astype(bf16)


def fetched(core, weights, buffer, sems, first):
    height = buffer.shape[2]
    for g in range(SIDE):
        rows = pl.ds(first, height)

        @pl.when(core == 0)
        def _():
            pltpu.make_async_copy(weights.at[:, g, rows, :], buffer.at[g], sems.at[g]).start()

        @pl.when(core != 0)
        def _():
            pltpu.make_async_copy(weights.at[g, :, rows, :], buffer.at[g], sems.at[g]).start()


def multiplied(rows, weights, buffer, sems, first):
    height = buffer.shape[2]
    count = height // 32
    acc = [None] * ((count + 1) // 2)
    for g in range(SIDE):
        pltpu.make_async_copy(
            weights.at[0, :, pl.ds(first, height), :], buffer.at[g], sems.at[g]
        ).wait()
        lhs = rows[:, 256 * g : 256 * g + 256]
        for n in range(0, count, 2):
            tiles = [
                buffer[g, :, 32 * m : 32 * m + 32, :].reshape(256, 128)
                for m in range(n, min(n + 2, count))
            ]
            rhs = jnp.concatenate(tiles, axis=1) if len(tiles) > 1 else tiles[0]
            d = jnp.dot(lhs, rhs, preferred_element_type=f32)
            acc[n // 2] = d if acc[n // 2] is None else acc[n // 2] + d
    return acc


def gate_kernel(place, half, other, residual, gain, weights, gated, edge, rows, stream, buffer, sems):
    fetched(place[0], weights, buffer, sems, 0)
    for n in range(0, 128, 32):
        total = residual[n : n + 32].astype(f32) + (
            half[n : n + 32] + other[n : n + 32].astype(f32)
        )
        r = lax.rsqrt(jnp.mean(total * total, axis=-1, keepdims=True) + epsilon)
        rows[n : n + 32] = (total * r * gain[...]).astype(bf16)
    own = pl.ds(pl.multiple_of(place[2] * 16, 16), 16)
    stream[...] = residual[own].astype(f32) + (half[own] + other[own].astype(f32))
    for n, part in enumerate(multiplied(rows, weights, buffer, sems, 0)):
        part = part.astype(bf16)
        gated[:, 256 * n : 256 * n + 256] = part
        edge[:, 256 * n : 256 * n + 256] = part[112:128]


def lift_kernel(core, rows, weights, lifted, buffer, sems):
    fetched(core[0], weights, buffer, sems, 192)
    for n, part in enumerate(multiplied(rows, weights, buffer, sems, 192)):
        lifted[:, 256 * n : 256 * n + part.shape[1]] = part.astype(bf16)


def down_kernel(gated, lifted, prior, taps, weight, out):
    at = lax.broadcasted_iota(jnp.int32, (128, 1), 0)

    def activated(lo, hi):
        g = gated[:, lo:hi].astype(f32)
        p = prior[:, lo:hi].astype(f32)
        one = jnp.where(at == 0, p[15:16], pltpu.roll(g, 1, 0))
        two = jnp.where(at == 0, p[14:15], jnp.where(at == 1, p[15:16], pltpu.roll(g, 2, 0)))
        conv = taps[0:1, lo:hi] * two + taps[1:2, lo:hi] * one + taps[2:3, lo:hi] * g
        return g, conv * jax.nn.sigmoid(conv)

    acc = None
    for n in range(0, MAIN, 128):
        _, a = activated(n, n + 128)
        h = (a * lifted[:, n : n + 128].astype(f32)).astype(bf16)
        d = jnp.dot(h, weight[n : n + 128, :], preferred_element_type=f32)
        acc = d if acc is None else acc + d
    g, a = activated(MAIN, MAIN + 128)
    h = (pltpu.roll(a, 64, 1) * g).astype(bf16)
    acc = acc + jnp.dot(h[:, 0:64], weight[MAIN:, :], preferred_element_type=f32)
    out[...] = acc.astype(bf16)


def last_kernel(parts, stream, out):
    mixer = parts[0].astype(f32)
    for i in range(1, 8):
        mixer = mixer + parts[i].astype(f32)
    out[...] = (stream[...] + mixer).astype(bf16)


def swapped(a, axis, groups=None):
    return lax.all_to_all(a, axis, 0, 0, axis_index_groups=groups, tiled=True)


def gathered(a, axis, groups=None):
    return lax.all_gather(a, axis, axis_index_groups=groups, axis=0, tiled=True)


def in_hbm(a):
    return pltpu.with_memory_space_constraint(a, pltpu.HBM)


SMALL = pltpu.CompilerParams(vmem_limit_bytes=20 << 20)


def on_device(
    query_one,
    key_one,
    query_two,
    key_two,
    values,
    mix_weight,
    head_gain,
    residual,
    out_weight,
    norm_gain,
    lift_weight,
    gate_weight,
    conv_taps,
    down_weight,
):
    tokens = query_one.shape[0]
    own = residual.shape[0]
    width = residual.shape[1]
    z = lax.axis_index("z")
    y = lax.axis_index("y")
    core = lax.axis_index("core")
    along_y = jnp.stack([z * SIDE, 1 + 0 * z, y, SIDE + 0 * z, 0 * z, z // 2 + 1])
    along_z = jnp.stack([y, SIDE + 0 * z, z * SIDE, 1 + 0 * z, z // 2, SIDE // 2 + 0 * z])
    plan = jnp.where(core == 0, along_y, along_z).astype(jnp.int32)
    smem = pl.BlockSpec(memory_space=pltpu.SMEM)
    hbm = pl.BlockSpec(memory_space=pltpu.HBM)
    x = lax.axis_index("x")
    place = jnp.stack([core, x, 2 * x + core]).astype(jnp.int32)
    above = lax.ppermute(out_weight, "x", [(i, (i + 1) % 4) for i in range(4)])
    below = lax.ppermute(out_weight, "x", [(i, (i + 3) % 4) for i in range(4)])
    qsend, ksend = pl.pallas_call(
        pack_kernel,
        out_shape=[
            jax.ShapeDtypeStruct((256, 128), bf16),
            jax.ShapeDtypeStruct((SIDE, SENT, 128), bf16),
        ],
        in_specs=[hbm] * 7,
        out_specs=[vmem(), hbm],
        scratch_shapes=[
            pltpu.VMEM((128, 256), bf16),
            pltpu.VMEM((32, 704), bf16),
            pltpu.VMEM((32, 704), bf16),
            pltpu.VMEM((SENT, 128), bf16),
            pltpu.SemaphoreType.DMA((7,)),
            pltpu.SemaphoreType.DMA((SIDE,)),
        ],
        compiler_params=SMALL,
        name="pack",
    )(*(in_hbm(a) for a in (query_one, query_two, key_one, key_two, values, lift_weight, gate_weight)))
    kpool = swapped(ksend, ALL, K_GROUPS)
    qpool = gathered(qsend, ALL, Q_GROUPS).reshape(SIDE, 256, 128)
    part = kpool[:, 512:, :].reshape(SIDE * 352, 128)
    weights = in_hbm(gathered(part, ALL, Q_GROUPS).reshape(SIDE, SIDE, 352, 128))
    out = pl.pallas_call(
        attend_kernel,
        grid=(1,),
        out_shape=jax.ShapeDtypeStruct((SIDE, PACK, 128), bf16),
        in_specs=[
            pl.BlockSpec(memory_space=pltpu.SMEM),
            vmem(),
            pl.BlockSpec((SIDE, 512, 128), lambda i: (0, 0, 0)),
        ],
        out_specs=vmem(),
        scratch_shapes=[pltpu.VMEM((8, 256, 256), f32)],
        compiler_params=SMALL,
        name="attend",
    )(plan, qpool, kpool)
    back = swapped(out, ALL, Q_GROUPS)
    before = gathered(residual, TP)
    above, below, before = lax.optimization_barrier((above, below, before))
    across = (
        lax.ppermute(above[0:128], "x", [(i, (i + 1) % 4) for i in range(4)]),
        lax.ppermute(below[128:256], "x", [(i, (i + 3) % 4) for i in range(4)]),
    )
    heads = pl.pallas_call(
        join_kernel,
        out_shape=jax.ShapeDtypeStruct((4, tokens, VD), bf16),
        in_specs=[pl.BlockSpec(memory_space=pltpu.SMEM)] + [vmem()] * 2,
        out_specs=vmem(),
        compiler_params=SMALL,
        name="join",
    )(mix_weight, back, head_gain.reshape(1, VD))
    heads = swapped(heads, "x")
    half, sent = pl.pallas_call(
        project_kernel,
        out_shape=[
            jax.ShapeDtypeStruct((tokens, width), f32),
            jax.ShapeDtypeStruct((tokens, width), bf16),
        ],
        in_specs=[smem, vmem()] + [pl.BlockSpec(memory_space=pl.ANY)] * 5,
        out_specs=[vmem()] * 2,
        scratch_shapes=[pltpu.VMEM((4, VD, 2048), bf16), pltpu.SemaphoreType.DMA((5,))],
        compiler_params=SMALL,
        name="project",
    )(place, heads, in_hbm(out_weight), above, below, *across)
    other = lax.ppermute(sent, "core", [(0, 1), (1, 0)])
    gated, edge, rows, stream = pl.pallas_call(
        gate_kernel,
        out_shape=[
            jax.ShapeDtypeStruct((tokens, MAIN + 128), bf16),
            jax.ShapeDtypeStruct((16, MAIN + 128), bf16),
            jax.ShapeDtypeStruct((tokens, width), bf16),
            jax.ShapeDtypeStruct((own, width), f32),
        ],
        in_specs=[smem] + [vmem()] * 4 + [hbm],
        out_specs=[vmem()] * 4,
        scratch_shapes=[
            pltpu.VMEM((SIDE, SIDE, 192, 128), bf16),
            pltpu.SemaphoreType.DMA((SIDE,)),
        ],
        compiler_params=SMALL,
        name="gate",
    )(place, half, other, before, norm_gain.reshape(1, width), weights)
    route = [(i, i + 1) for i in range(SIDE * SIDE - 1)]
    prior = lax.ppermute(edge, ("z", "y"), route)
    lifted = pl.pallas_call(
        lift_kernel,
        out_shape=jax.ShapeDtypeStruct((tokens, MAIN), bf16),
        in_specs=[smem, vmem(), hbm],
        out_specs=vmem(),
        scratch_shapes=[
            pltpu.VMEM((SIDE, SIDE, 160, 128), bf16),
            pltpu.SemaphoreType.DMA((SIDE,)),
        ],
        compiler_params=SMALL,
        cost_estimate=pl.CostEstimate(
            flops=2 * 128 * 2048 * 640, bytes_accessed=3 << 20, transcendentals=0
        ),
        name="lift",
    )(place, rows, weights)
    gap = jnp.zeros((WIDTH, 64), f32)
    taps = jnp.concatenate([conv_taps[:, :MAIN], gap, conv_taps[:, MAIN:]], axis=1)
    down = pl.pallas_call(
        down_kernel,
        out_shape=jax.ShapeDtypeStruct((tokens, width), bf16),
        in_specs=[vmem()] * 5,
        out_specs=vmem(),
        compiler_params=SMALL,
        name="down",
    )(gated, lifted, prior, taps, down_weight)
    mixer = swapped(down.reshape(8, own, width), TP)
    return pl.pallas_call(
        last_kernel,
        out_shape=jax.ShapeDtypeStruct((own, width), bf16),
        in_specs=[vmem()] * 2,
        out_specs=vmem(),
        compiler_params=SMALL,
        name="last",
    )(mixer, stream)


def solution(mesh):
    fine = Mesh(mesh.devices.reshape(SIDE, SIDE, 4, 2), ("z", "y", "x", "core"))
    sp = ("z", "y")

    return jax.shard_map(
        on_device,
        mesh=fine,
        in_specs=(
            P(sp, TP),
            P(sp, TP),
            P(sp, TP),
            P(sp, TP),
            P(sp, TP),
            P(TP),
            P(),
            P(("z", "y", "x", "core"), None),
            P(TP, None),
            P(),
            P(sp, TP),
            P(sp, TP),
            P(None, TP),
            P(TP, None),
        ),
        out_specs=P(("z", "y", "x", "core"), None),
        check_vma=False,
    )
```

```python
import jax
import jax.numpy as jnp
import numpy as np
from jax import lax
from jax.experimental import pallas as pl
from jax.experimental.pallas import tpu as pltpu
from jax.sharding import Mesh, PartitionSpec as P

HD = 128
VD = 256
STRETCH = 64
WIDTH = 3
SIDE = 8
BLOCK = 128
PACK = 4 * BLOCK + 16
TILES = 5
MAIN = 128 * TILES
SENT = 512 + 352
SHIFTS = (0, 1, -1, 2)
epsilon = 1e-06
masked_score = -1e30
LOG2E = 1.4426950408889634
EXP2_SCALE = LOG2E * HD**-0.5
f32 = jnp.float32
bf16 = jnp.bfloat16
TP = ("x", "core")
ALL = ("z", "y", "x", "core")
PLACES = np.arange(SIDE * SIDE * 8).reshape(SIDE, SIDE, 4, 2)
ROWS = [[PLACES[i, :, x, c].tolist() for i in range(SIDE) for x in range(4)] for c in range(2)]
COLS = [[PLACES[:, i, x, c].tolist() for i in range(SIDE) for x in range(4)] for c in range(2)]
Q_GROUPS = ROWS[0] + COLS[1]
K_GROUPS = COLS[0] + ROWS[1]


def vmem():
    return pl.BlockSpec(memory_space=pltpu.VMEM)


def pack_kernel(q1, q2, k1, k2, v, lift, gate, qsend, ksend, vv, ll, gg, rows, sems, sent):
    moves = [
        pltpu.make_async_copy(src, dst, sems.at[i])
        for i, (src, dst) in enumerate(
            (
                (k1, rows.at[0:128]),
                (k2, rows.at[128:256]),
                (v, vv),
                (lift, ll),
                (gate, gg),
                (q1, qsend.at[0:128]),
                (q2, qsend.at[128:256]),
            )
        )
    ]
    for move in moves:
        move.start()
    for move in moves:
        move.wait()
    rows[256:384, :] = vv[:, 0:128]
    rows[384:512, :] = vv[:, 128:256]
    for n in range(TILES):
        rows[512 + 32 * n : 544 + 32 * n, :] = gg[:, 128 * n : 128 * n + 128]
        rows[704 + 32 * n : 736 + 32 * n, :] = ll[:, 128 * n : 128 * n + 128]
    rows[672:704, :] = jnp.concatenate([ll[:, MAIN:], gg[:, MAIN:]], axis=1)
    copies = [pltpu.make_async_copy(rows, ksend.at[i], sent.at[i]) for i in range(SIDE)]
    for copy in copies:
        copy.start()
    for copy in copies:
        copy.wait()


def attend_kernel(plan, qpool, kpool, out, scores):
    q_base, q_step, k_base, k_step = (plan[i] for i in range(4))
    first_chunk, pairs = plan[4], plan[5]
    row = lax.broadcasted_iota(jnp.int32, (256, 256), 0)
    col = lax.broadcasted_iota(jnp.int32, (256, 256), 1)
    at = lax.broadcasted_iota(jnp.int32, (16, 128), 0)

    def blank(c, carry):
        for h in range(2):
            out[2 * c + h, 0:512, :] = jnp.zeros((512, 128), bf16)
            level = jnp.where((at == 0) | (at == 3), masked_score, 0.0)
            out[2 * c + h, 512:528, :] = level.astype(bf16)
        return carry

    lax.fori_loop(0, first_chunk, blank, 0)

    def chunk(c, carry):
        queries = [
            jnp.concatenate(
                [qpool[2 * c, 128 * m : 128 * m + 128, :], qpool[2 * c + 1, 128 * m : 128 * m + 128, :]],
                axis=0,
            )
            for m in range(2)
        ]
        q_at = 2 * (q_base + q_step * (2 * c + row // 128)) + (row % 128) // STRETCH

        def scored(p, peaks):
            k_at = 2 * (k_base + k_step * (2 * p + col // 128)) + (col % 128) // STRETCH
            seen = k_at <= q_at
            new = []
            for m in range(2):
                k = jnp.concatenate(
                    [kpool[2 * p, 128 * m : 128 * m + 128, :], kpool[2 * p + 1, 128 * m : 128 * m + 128, :]],
                    axis=0,
                )
                s = lax.dot_general(
                    queries[m], k, (((1,), (1,)), ((), ())), preferred_element_type=f32
                )
                s = jnp.where(seen, s, masked_score)
                scores[2 * p + m] = s
                new.append(jnp.maximum(peaks[m], jnp.maximum(s[:, 0:128], s[:, 128:256])))
            return tuple(new)

        low = jnp.full((256, 128), masked_score, f32)
        peaks = lax.fori_loop(0, pairs, scored, (low, low))
        tops = [jnp.max(peak, axis=-1, keepdims=True) for peak in peaks]

        def weighed(p, carry):
            totals, acc = carry
            new, ws = [], []
            for m in range(2):
                w = jnp.exp2((scores[2 * p + m] - tops[m]) * EXP2_SCALE)
                new.append(totals[m] + (w[:, 0:128] + w[:, 128:256]))
                ws.append(w.astype(bf16))
            va = jnp.concatenate([kpool[2 * p, 256:384, :], kpool[2 * p, 384:512, :]], axis=1)
            vb = jnp.concatenate([kpool[2 * p + 1, 256:384, :], kpool[2 * p + 1, 384:512, :]], axis=1)
            vals = jnp.concatenate([va, vb], axis=0)
            acc = acc + jnp.dot(
                jnp.concatenate(ws, axis=0), vals, preferred_element_type=f32
            )
            return tuple(new), acc

        none = jnp.zeros((256, 128), f32)
        totals, acc = lax.fori_loop(
            0, pairs, weighed, ((none, none), jnp.zeros((512, VD), f32))
        )
        levels = []
        for m in range(2):
            total = jnp.sum(totals[m], axis=-1, keepdims=True)
            o = (acc[256 * m : 256 * m + 256] / total).astype(bf16)
            seen = tops[m] > 0.5 * masked_score
            levels.append(jnp.where(seen, tops[m] * EXP2_SCALE + jnp.log2(total), masked_score))
            for h in range(2):
                for e in range(2):
                    out[2 * c + h, 256 * m + 128 * e : 256 * m + 128 * e + 128, :] = o[
                        128 * h : 128 * h + 128, 128 * e : 128 * e + 128
                    ]
        for h in range(2):
            rows = jnp.zeros((16, 128), f32)
            for m in range(2):
                wide = jnp.transpose(
                    jnp.broadcast_to(levels[m][128 * h : 128 * h + 128], (128, 128))
                )[0:16]
                a = wide.astype(bf16).astype(f32)
                b = (wide - a).astype(bf16).astype(f32)
                d = wide - a - b
                for n, piece in enumerate((a, b, d)):
                    rows = jnp.where(at == 3 * m + n, piece, rows)
            out[2 * c + h, 512:528, :] = rows.astype(bf16)
        return carry

    lax.fori_loop(first_chunk, SIDE // 2, chunk, 0)


def join_kernel(mix, parts, gain, residual, out):
    tails = [parts[i, 512:528, :].astype(f32) for i in range(SIDE)]

    def joined(m):
        levels = jnp.concatenate(
            [jnp.sum(tail[3 * m : 3 * m + 3], axis=0, keepdims=True) for tail in tails], axis=0
        )
        top = jnp.max(levels, axis=0, keepdims=True)
        w = jnp.exp2(levels - top)
        w = w / jnp.sum(w, axis=0, keepdims=True)
        w = jnp.transpose(jnp.concatenate([w, jnp.zeros((120, 128), f32)], axis=0))
        acc = [jnp.zeros((128, 128), f32), jnp.zeros((128, 128), f32)]
        for i in range(SIDE):
            wi = w[:, i : i + 1]
            for e in range(2):
                at = 256 * m + 128 * e
                acc[e] = acc[e] + wi * parts[i, at : at + 128, :].astype(f32)
        return jnp.concatenate(acc, axis=1)

    mixed = joined(0) - mix[0] * joined(1)
    r = lax.rsqrt(jnp.mean(mixed * mixed, axis=-1, keepdims=True) + epsilon)
    head = (mixed * r * gain[...]).astype(bf16)
    for i in range(4):
        out[i, 0:128] = head
        for j in range(8):
            out[i, 128 + 16 * j : 144 + 16 * j, :] = residual[:, 256 * j : 256 * j + 256]


def own_rows(place, i):
    return pl.ds(pl.multiple_of(32 * i + 16 * place[0], 16), 16)


def other_rows(place, i):
    return pl.ds(pl.multiple_of(32 * i + 16 - 16 * place[0], 16), 16)


def project_kernel(place, heads, *refs):
    weights, (half, sent, buffer, sems) = refs[:5], refs[5:]
    x = place[1]
    slots = [buffer.at[0], buffer.at[1], buffer.at[2], buffer.at[3, 0:128], buffer.at[3, 128:256]]
    moves = [
        pltpu.make_async_copy(weight, slot, sems.at[i])
        for i, (weight, slot) in enumerate(zip(weights, slots))
    ]
    for move in moves:
        move.start()
    for i, shift in enumerate(SHIFTS):
        moves[i].wait()
        if i == 3:
            moves[4].wait()
        head = heads[lax.rem(x + 4 - shift, 4), 0:128]
        for n in range(0, 2048, 256):
            d = jnp.dot(head, buffer[i, :, n : n + 256], preferred_element_type=f32)
            if i > 0:
                d = d + half[:, n : n + 256]
            half[:, n : n + 256] = d
    for i in range(4):
        rows = own_rows(place, i)
        for j in range(8):
            r = heads[i, 128 + 16 * j : 144 + 16 * j, :].astype(f32)
            half[rows, 256 * j : 256 * j + 256] = half[rows, 256 * j : 256 * j + 256] + r
    sent[...] = half[...].astype(bf16)


def fetched(core, weights, buffer, sems, first):
    height = buffer.shape[2]
    for g in range(SIDE):
        rows = pl.ds(first, height)

        @pl.when(core == 0)
        def _():
            pltpu.make_async_copy(weights.at[:, g, rows, :], buffer.at[g], sems.at[g]).start()

        @pl.when(core != 0)
        def _():
            pltpu.make_async_copy(weights.at[g, :, rows, :], buffer.at[g], sems.at[g]).start()


def multiplied(rows, weights, buffer, sems, first):
    height = buffer.shape[2]
    count = height // 32
    acc = [None] * ((count + 1) // 2)
    for g in range(SIDE):
        pltpu.make_async_copy(
            weights.at[0, :, pl.ds(first, height), :], buffer.at[g], sems.at[g]
        ).wait()
        lhs = rows[:, 256 * g : 256 * g + 256]
        for n in range(0, count, 2):
            tiles = [
                buffer[g, :, 32 * m : 32 * m + 32, :].reshape(256, 128)
                for m in range(n, min(n + 2, count))
            ]
            rhs = jnp.concatenate(tiles, axis=1) if len(tiles) > 1 else tiles[0]
            d = jnp.dot(lhs, rhs, preferred_element_type=f32)
            acc[n // 2] = d if acc[n // 2] is None else acc[n // 2] + d
    return acc


def gate_kernel(place, half, other, gain, weights, gated, edge, rows, stream, buffer, sems):
    fetched(place[0], weights, buffer, sems, 0)
    for n in range(0, 128, 32):
        total = half[n : n + 32] + other[n : n + 32].astype(f32)
        r = lax.rsqrt(jnp.mean(total * total, axis=-1, keepdims=True) + epsilon)
        rows[n : n + 32] = (total * r * gain[...]).astype(bf16)
    own = pl.ds(pl.multiple_of(place[2] * 16, 16), 16)
    stream[...] = half[own] + other[own].astype(f32)
    for n, part in enumerate(multiplied(rows, weights, buffer, sems, 0)):
        part = part.astype(bf16)
        gated[:, 256 * n : 256 * n + 256] = part
        edge[:, 256 * n : 256 * n + 256] = part[112:128]


def lift_kernel(core, rows, weights, lifted, buffer, sems):
    fetched(core[0], weights, buffer, sems, 192)
    for n, part in enumerate(multiplied(rows, weights, buffer, sems, 192)):
        lifted[:, 256 * n : 256 * n + part.shape[1]] = part.astype(bf16)


def down_kernel(place, gated, lifted, prior, taps, weight, keep, give, whole):
    at = lax.broadcasted_iota(jnp.int32, (128, 1), 0)

    def activated(lo, hi):
        g = gated[:, lo:hi].astype(f32)
        p = prior[:, lo:hi].astype(f32)
        one = jnp.where(at == 0, p[15:16], pltpu.roll(g, 1, 0))
        two = jnp.where(at == 0, p[14:15], jnp.where(at == 1, p[15:16], pltpu.roll(g, 2, 0)))
        conv = taps[0:1, lo:hi] * two + taps[1:2, lo:hi] * one + taps[2:3, lo:hi] * g
        return g, conv * jax.nn.sigmoid(conv)

    acc = None
    for n in range(0, MAIN, 128):
        _, a = activated(n, n + 128)
        h = (a * lifted[:, n : n + 128].astype(f32)).astype(bf16)
        d = jnp.dot(h, weight[n : n + 128, :], preferred_element_type=f32)
        acc = d if acc is None else acc + d
    g, a = activated(MAIN, MAIN + 128)
    h = (pltpu.roll(a, 64, 1) * g).astype(bf16)
    whole[...] = acc + jnp.dot(h[:, 0:64], weight[MAIN:, :], preferred_element_type=f32)
    for i in range(4):
        keep[16 * i : 16 * i + 16] = whole[own_rows(place, i)]
        give[16 * i : 16 * i + 16] = whole[other_rows(place, i)].astype(bf16)


def pair_kernel(keep, other, out):
    for i in range(4):
        rows = slice(16 * i, 16 * i + 16)
        out[i] = (keep[rows] + other[rows].astype(f32)).astype(bf16)


def last_kernel(parts, stream, out):
    mixer = parts[0].astype(f32)
    for i in range(1, 4):
        mixer = mixer + parts[i].astype(f32)
    out[...] = (stream[...] + mixer).astype(bf16)


def swapped(a, axis, groups=None):
    return lax.all_to_all(a, axis, 0, 0, axis_index_groups=groups, tiled=True)


def gathered(a, axis, groups=None):
    return lax.all_gather(a, axis, axis_index_groups=groups, axis=0, tiled=True)


def in_hbm(a):
    return pltpu.with_memory_space_constraint(a, pltpu.HBM)


SMALL = pltpu.CompilerParams(vmem_limit_bytes=20 << 20)


def on_device(
    query_one,
    key_one,
    query_two,
    key_two,
    values,
    mix_weight,
    head_gain,
    residual,
    out_weight,
    norm_gain,
    lift_weight,
    gate_weight,
    conv_taps,
    down_weight,
):
    tokens = query_one.shape[0]
    own = residual.shape[0]
    width = residual.shape[1]
    z = lax.axis_index("z")
    y = lax.axis_index("y")
    core = lax.axis_index("core")
    along_y = jnp.stack([z * SIDE, 1 + 0 * z, y, SIDE + 0 * z, 0 * z, z // 2 + 1])
    along_z = jnp.stack([y, SIDE + 0 * z, z * SIDE, 1 + 0 * z, z // 2, SIDE // 2 + 0 * z])
    plan = jnp.where(core == 0, along_y, along_z).astype(jnp.int32)
    smem = pl.BlockSpec(memory_space=pltpu.SMEM)
    hbm = pl.BlockSpec(memory_space=pltpu.HBM)
    x = lax.axis_index("x")
    place = jnp.stack([core, x, 2 * x + core]).astype(jnp.int32)
    qsend, ksend = pl.pallas_call(
        pack_kernel,
        out_shape=[
            jax.ShapeDtypeStruct((256, 128), bf16),
            jax.ShapeDtypeStruct((SIDE, SENT, 128), bf16),
        ],
        in_specs=[hbm] * 7,
        out_specs=[vmem(), hbm],
        scratch_shapes=[
            pltpu.VMEM((128, 256), bf16),
            pltpu.VMEM((32, 704), bf16),
            pltpu.VMEM((32, 704), bf16),
            pltpu.VMEM((SENT, 128), bf16),
            pltpu.SemaphoreType.DMA((7,)),
            pltpu.SemaphoreType.DMA((SIDE,)),
        ],
        compiler_params=SMALL,
        name="pack",
    )(*(in_hbm(a) for a in (query_one, query_two, key_one, key_two, values, lift_weight, gate_weight)))
    kpool = swapped(ksend, ALL, K_GROUPS)
    qpool = gathered(qsend, ALL, Q_GROUPS).reshape(SIDE, 256, 128)
    part = kpool[:, 512:, :].reshape(SIDE * 352, 128)
    own_rows_sent, qpool, part = lax.optimization_barrier((out_weight, qpool, part))
    weights = in_hbm(gathered(part, ALL, Q_GROUPS).reshape(SIDE, SIDE, 352, 128))
    above = lax.ppermute(own_rows_sent, "x", [(i, (i + 1) % 4) for i in range(4)])
    below = lax.ppermute(own_rows_sent, "x", [(i, (i + 3) % 4) for i in range(4)])
    run = pl.pallas_call(
    attend_kernel,
    grid=(1,),
    out_shape=jax.ShapeDtypeStruct((SIDE, PACK, 128), bf16),
    in_specs=[
        pl.BlockSpec(memory_space=pltpu.SMEM),
        vmem(),
        pl.BlockSpec((SIDE, 512, 128), lambda i: (0, 0, 0)),
    ],
    out_specs=vmem(),
    scratch_shapes=[pltpu.VMEM((8, 256, 256), f32)],
    compiler_params=SMALL,
    name="attend",
    )
    out = run(plan, qpool, kpool)
    back = swapped(out, ALL, Q_GROUPS)
    across = (
        lax.ppermute(above[0:128], "x", [(i, (i + 1) % 4) for i in range(4)]),
        lax.ppermute(below[128:256], "x", [(i, (i + 3) % 4) for i in range(4)]),
    )
    heads = pl.pallas_call(
        join_kernel,
        out_shape=jax.ShapeDtypeStruct((4, 2 * tokens, VD), bf16),
        in_specs=[pl.BlockSpec(memory_space=pltpu.SMEM)] + [vmem()] * 3,
        out_specs=vmem(),
        compiler_params=SMALL,
        name="join",
    )(mix_weight, back, head_gain.reshape(1, VD), residual)
    heads = swapped(heads, "x")
    half, sent = pl.pallas_call(
        project_kernel,
        out_shape=[
            jax.ShapeDtypeStruct((tokens, width), f32),
            jax.ShapeDtypeStruct((tokens, width), bf16),
        ],
        in_specs=[smem, vmem()] + [pl.BlockSpec(memory_space=pl.ANY)] * 5,
        out_specs=[vmem()] * 2,
        scratch_shapes=[pltpu.VMEM((4, VD, 2048), bf16), pltpu.SemaphoreType.DMA((5,))],
        compiler_params=SMALL,
        name="project",
    )(place, heads, in_hbm(out_weight), above, below, *(in_hbm(a) for a in across))
    other = lax.ppermute(sent, "core", [(0, 1), (1, 0)])
    gated, edge, rows, stream = pl.pallas_call(
        gate_kernel,
        out_shape=[
            jax.ShapeDtypeStruct((tokens, MAIN + 128), bf16),
            jax.ShapeDtypeStruct((16, MAIN + 128), bf16),
            jax.ShapeDtypeStruct((tokens, width), bf16),
            jax.ShapeDtypeStruct((own, width), f32),
        ],
        in_specs=[smem] + [vmem()] * 3 + [hbm],
        out_specs=[vmem()] * 4,
        scratch_shapes=[
            pltpu.VMEM((SIDE, SIDE, 192, 128), bf16),
            pltpu.SemaphoreType.DMA((SIDE,)),
        ],
        compiler_params=SMALL,
        name="gate",
    )(place, half, other, norm_gain.reshape(1, width), weights)
    route = [(i, i + 1) for i in range(SIDE * SIDE - 1)]
    prior = lax.ppermute(edge, ("z", "y"), route)
    lifted = pl.pallas_call(
        lift_kernel,
        out_shape=jax.ShapeDtypeStruct((tokens, MAIN), bf16),
        in_specs=[smem, vmem(), hbm],
        out_specs=vmem(),
        scratch_shapes=[
            pltpu.VMEM((SIDE, SIDE, 160, 128), bf16),
            pltpu.SemaphoreType.DMA((SIDE,)),
        ],
        compiler_params=SMALL,
        cost_estimate=pl.CostEstimate(
            flops=2 * 128 * 2048 * 640, bytes_accessed=3 << 20, transcendentals=0
        ),
        name="lift",
    )(place, rows, weights)
    gap = jnp.zeros((WIDTH, 64), f32)
    taps = jnp.concatenate([conv_taps[:, :MAIN], gap, conv_taps[:, MAIN:]], axis=1)
    keep, give = pl.pallas_call(
        down_kernel,
        out_shape=[
            jax.ShapeDtypeStruct((tokens // 2, width), f32),
            jax.ShapeDtypeStruct((tokens // 2, width), bf16),
        ],
        in_specs=[smem] + [vmem()] * 5,
        out_specs=[vmem()] * 2,
        scratch_shapes=[pltpu.VMEM((128, 2048), f32)],
        compiler_params=SMALL,
        name="down",
    )(place, gated, lifted, prior, taps, down_weight)
    taken = lax.ppermute(give, "core", [(0, 1), (1, 0)])
    pair = pl.pallas_call(
        pair_kernel,
        out_shape=jax.ShapeDtypeStruct((4, own, width), bf16),
        in_specs=[vmem()] * 2,
        out_specs=vmem(),
        compiler_params=SMALL,
        name="pair",
    )(keep, taken)
    mixer = swapped(pair, "x")
    return pl.pallas_call(
        last_kernel,
        out_shape=jax.ShapeDtypeStruct((own, width), bf16),
        in_specs=[vmem()] * 2,
        out_specs=vmem(),
        compiler_params=SMALL,
        name="last",
    )(mixer, stream)


def solution(mesh):
    fine = Mesh(mesh.devices.reshape(SIDE, SIDE, 4, 2), ("z", "y", "x", "core"))
    sp = ("z", "y")

    return jax.shard_map(
        on_device,
        mesh=fine,
        in_specs=(
            P(sp, TP),
            P(sp, TP),
            P(sp, TP),
            P(sp, TP),
            P(sp, TP),
            P(TP),
            P(),
            P(("z", "y", "x", "core"), None),
            P(TP, None),
            P(),
            P(sp, TP),
            P(sp, TP),
            P(None, TP),
            P(TP, None),
        ),
        out_specs=P(("z", "y", "x", "core"), None),
        check_vma=False,
    )
```

```python
import jax
import jax.numpy as jnp
import numpy as np
from jax import lax
from jax.experimental import pallas as pl
from jax.experimental.pallas import tpu as pltpu
from jax.sharding import Mesh, PartitionSpec as P

HD = 128
VD = 256
STRETCH = 64
WIDTH = 3
SIDE = 8
BLOCK = 128
PACK = 4 * BLOCK + 16
TILES = 5
MAIN = 128 * TILES
SENT = 512 + 352
SHIFTS = (0, 1, -1, 2)
epsilon = 1e-06
masked_score = -1e30
LOG2E = 1.4426950408889634
EXP2_SCALE = LOG2E * HD**-0.5
f32 = jnp.float32
bf16 = jnp.bfloat16
TP = ("x", "core")
ALL = ("z", "y", "x", "core")
PLACES = np.arange(SIDE * SIDE * 8).reshape(SIDE, SIDE, 4, 2)
ROWS = [[PLACES[i, :, x, c].tolist() for i in range(SIDE) for x in range(4)] for c in range(2)]
COLS = [[PLACES[:, i, x, c].tolist() for i in range(SIDE) for x in range(4)] for c in range(2)]
Q_GROUPS = ROWS[0] + COLS[1]
K_GROUPS = COLS[0] + ROWS[1]


def vmem():
    return pl.BlockSpec(memory_space=pltpu.VMEM)


def pack_kernel(q1, q2, k1, k2, v, lift, gate, qsend, ksend, vv, ll, gg, rows, sems, sent):
    moves = [
        pltpu.make_async_copy(src, dst, sems.at[i])
        for i, (src, dst) in enumerate(
            (
                (k1, rows.at[0:128]),
                (k2, rows.at[128:256]),
                (v, vv),
                (lift, ll),
                (gate, gg),
                (q1, qsend.at[0:128]),
                (q2, qsend.at[128:256]),
            )
        )
    ]
    for move in moves:
        move.start()
    for move in moves:
        move.wait()
    rows[256:384, :] = vv[:, 0:128]
    rows[384:512, :] = vv[:, 128:256]
    for n in range(TILES):
        rows[512 + 32 * n : 544 + 32 * n, :] = gg[:, 128 * n : 128 * n + 128]
        rows[704 + 32 * n : 736 + 32 * n, :] = ll[:, 128 * n : 128 * n + 128]
    rows[672:704, :] = jnp.concatenate([ll[:, MAIN:], gg[:, MAIN:]], axis=1)
    copies = [pltpu.make_async_copy(rows, ksend.at[i], sent.at[i]) for i in range(SIDE)]
    for copy in copies:
        copy.start()
    for copy in copies:
        copy.wait()


def attend_kernel(plan, qpool, kpool, out):
    q_base, q_step, k_base, k_step = (plan[i] for i in range(4))
    at = lax.broadcasted_iota(jnp.int32, (16, 128), 0)
    row = lax.broadcasted_iota(jnp.int32, (256, 1), 0)
    col = lax.broadcasted_iota(jnp.int32, (1, 1024), 1)
    k_at = 2 * (k_base + k_step * (col // 128)) + (col % 128) // STRETCH
    vals = jnp.concatenate(
        [kpool[:, 256:384, :].reshape(1024, 128), kpool[:, 384:512, :].reshape(1024, 128)], axis=1
    )
    for c in range(SIDE // 2):
        q_at = 2 * (q_base + q_step * (2 * c + row // 128)) + (row % 128) // STRETCH
        seen = k_at <= q_at
        levels = []
        for m in range(2):
            lo = slice(128 * m, 128 * m + 128)
            q = jnp.concatenate([qpool[2 * c, lo, :], qpool[2 * c + 1, lo, :]], axis=0)
            k = kpool[:, lo, :].reshape(1024, 128)
            s = lax.dot_general(q, k, (((1,), (1,)), ((), ())), preferred_element_type=f32)
            s = jnp.where(seen, s, masked_score)
            top = jnp.max(s, axis=-1, keepdims=True)
            w = jnp.exp2((s - top) * EXP2_SCALE)
            total = jnp.sum(w, axis=-1, keepdims=True)
            o = (jnp.dot(w.astype(bf16), vals, preferred_element_type=f32) / total).astype(bf16)
            level = top * EXP2_SCALE + jnp.log2(total)
            levels.append(jnp.where(top > 0.5 * masked_score, level, masked_score))
            for h in range(2):
                for e in range(2):
                    out[2 * c + h, 256 * m + 128 * e : 256 * m + 128 * e + 128, :] = o[
                        128 * h : 128 * h + 128, 128 * e : 128 * e + 128
                    ]
        for h in range(2):
            rows = jnp.zeros((16, 128), f32)
            for m in range(2):
                wide = jnp.transpose(
                    jnp.broadcast_to(levels[m][128 * h : 128 * h + 128], (128, 128))
                )[0:16]
                a = wide.astype(bf16).astype(f32)
                b = (wide - a).astype(bf16).astype(f32)
                d = wide - a - b
                for n, piece in enumerate((a, b, d)):
                    rows = jnp.where(at == 3 * m + n, piece, rows)
            out[2 * c + h, 512:528, :] = rows.astype(bf16)


def join_kernel(mix, parts, gain, out):
    tails = [parts[i, 512:528, :].astype(f32) for i in range(SIDE)]

    def joined(m):
        levels = jnp.concatenate(
            [jnp.sum(tail[3 * m : 3 * m + 3], axis=0, keepdims=True) for tail in tails], axis=0
        )
        top = jnp.max(levels, axis=0, keepdims=True)
        w = jnp.exp2(levels - top)
        w = w / jnp.sum(w, axis=0, keepdims=True)
        w = jnp.transpose(jnp.concatenate([w, jnp.zeros((120, 128), f32)], axis=0))
        acc = [jnp.zeros((128, 128), f32), jnp.zeros((128, 128), f32)]
        for i in range(SIDE):
            wi = w[:, i : i + 1]
            for e in range(2):
                at = 256 * m + 128 * e
                acc[e] = acc[e] + wi * parts[i, at : at + 128, :].astype(f32)
        return jnp.concatenate(acc, axis=1)

    mixed = joined(0) - mix[0] * joined(1)
    r = lax.rsqrt(jnp.mean(mixed * mixed, axis=-1, keepdims=True) + epsilon)
    head = (mixed * r * gain[...]).astype(bf16)
    for i in range(4):
        out[i] = head


def project_kernel(place, heads, *refs):
    weights, (half, sent, buffer, sems) = refs[:5], refs[5:]
    x = place[1]
    slots = [buffer.at[0], buffer.at[1], buffer.at[2], buffer.at[3, 0:128], buffer.at[3, 128:256]]
    moves = [
        pltpu.make_async_copy(weight, slot, sems.at[i])
        for i, (weight, slot) in enumerate(zip(weights, slots))
    ]
    for move in moves:
        move.start()
    for i, shift in enumerate(SHIFTS):
        moves[i].wait()
        if i == 3:
            moves[4].wait()
        head = heads[lax.rem(x + 4 - shift, 4)]
        for n in range(0, 2048, 256):
            d = jnp.dot(head, buffer[i, :, n : n + 256], preferred_element_type=f32)
            if i > 0:
                d = d + half[:, n : n + 256]
            half[:, n : n + 256] = d
            if i == 3:
                sent[:, n : n + 256] = d.astype(bf16)


def fetched(core, weights, buffer, sems, first):
    height = buffer.shape[2]
    for g in range(SIDE):
        rows = pl.ds(first, height)

        @pl.when(core == 0)
        def _():
            pltpu.make_async_copy(weights.at[:, g, rows, :], buffer.at[g], sems.at[g]).start()

        @pl.when(core != 0)
        def _():
            pltpu.make_async_copy(weights.at[g, :, rows, :], buffer.at[g], sems.at[g]).start()


def multiplied(rows, weights, buffer, sems, first):
    height = buffer.shape[2]
    count = height // 32
    acc = [None] * ((count + 1) // 2)
    for g in range(SIDE):
        pltpu.make_async_copy(
            weights.at[0, :, pl.ds(first, height), :], buffer.at[g], sems.at[g]
        ).wait()
        lhs = rows[:, 256 * g : 256 * g + 256]
        for n in range(0, count, 2):
            tiles = [
                buffer[g, :, 32 * m : 32 * m + 32, :].reshape(256, 128)
                for m in range(n, min(n + 2, count))
            ]
            rhs = jnp.concatenate(tiles, axis=1) if len(tiles) > 1 else tiles[0]
            d = jnp.dot(lhs, rhs, preferred_element_type=f32)
            acc[n // 2] = d if acc[n // 2] is None else acc[n // 2] + d
    return acc


def gate_kernel(place, half, other, residual, gain, weights, gated, edge, rows, stream, buffer, sems):
    fetched(place[0], weights, buffer, sems, 0)
    for n in range(0, 128, 32):
        total = residual[n : n + 32].astype(f32) + (
            half[n : n + 32] + other[n : n + 32].astype(f32)
        )
        r = lax.rsqrt(jnp.mean(total * total, axis=-1, keepdims=True) + epsilon)
        rows[n : n + 32] = (total * r * gain[...]).astype(bf16)
    own = pl.ds(pl.multiple_of(place[2] * 16, 16), 16)
    stream[...] = residual[own].astype(f32) + (half[own] + other[own].astype(f32))
    for n, part in enumerate(multiplied(rows, weights, buffer, sems, 0)):
        part = part.astype(bf16)
        gated[:, 256 * n : 256 * n + 256] = part
        edge[:, 256 * n : 256 * n + 256] = part[112:128]


def lift_kernel(core, rows, weights, lifted, buffer, sems):
    fetched(core[0], weights, buffer, sems, 192)
    for n, part in enumerate(multiplied(rows, weights, buffer, sems, 192)):
        lifted[:, 256 * n : 256 * n + part.shape[1]] = part.astype(bf16)


def own_rows(place, i):
    return pl.ds(pl.multiple_of(32 * i + 16 * place[0], 16), 16)


def other_rows(place, i):
    return pl.ds(pl.multiple_of(32 * i + 16 - 16 * place[0], 16), 16)


def down_kernel(place, gated, lifted, prior, taps, weight, keep, give, whole):
    at = lax.broadcasted_iota(jnp.int32, (128, 1), 0)

    def activated(lo, hi):
        g = gated[:, lo:hi].astype(f32)
        p = prior[:, lo:hi].astype(f32)
        one = jnp.where(at == 0, p[15:16], pltpu.roll(g, 1, 0))
        two = jnp.where(at == 0, p[14:15], jnp.where(at == 1, p[15:16], pltpu.roll(g, 2, 0)))
        conv = taps[0:1, lo:hi] * two + taps[1:2, lo:hi] * one + taps[2:3, lo:hi] * g
        return g, conv * jax.nn.sigmoid(conv)

    acc = None
    for n in range(0, MAIN, 128):
        _, a = activated(n, n + 128)
        h = (a * lifted[:, n : n + 128].astype(f32)).astype(bf16)
        d = jnp.dot(h, weight[n : n + 128, :], preferred_element_type=f32)
        acc = d if acc is None else acc + d
    g, a = activated(MAIN, MAIN + 128)
    h = (pltpu.roll(a, 64, 1) * g).astype(bf16)
    whole[...] = acc + jnp.dot(h[:, 0:64], weight[MAIN:, :], preferred_element_type=f32)
    for i in range(4):
        keep[16 * i : 16 * i + 16] = whole[own_rows(place, i)]
        give[16 * i : 16 * i + 16] = whole[other_rows(place, i)].astype(bf16)


def pair_kernel(keep, other, out):
    for i in range(4):
        rows = slice(16 * i, 16 * i + 16)
        out[i] = (keep[rows] + other[rows].astype(f32)).astype(bf16)


def last_kernel(parts, stream, out):
    mixer = parts[0].astype(f32)
    for i in range(1, 4):
        mixer = mixer + parts[i].astype(f32)
    out[...] = (stream[...] + mixer).astype(bf16)


def swapped(a, axis, groups=None):
    return lax.all_to_all(a, axis, 0, 0, axis_index_groups=groups, tiled=True)


def gathered(a, axis, groups=None):
    return lax.all_gather(a, axis, axis_index_groups=groups, axis=0, tiled=True)


def in_hbm(a):
    return pltpu.with_memory_space_constraint(a, pltpu.HBM)


SMALL = pltpu.CompilerParams(vmem_limit_bytes=20 << 20)
LARGE = pltpu.CompilerParams(vmem_limit_bytes=30 << 20)


def on_device(
    query_one,
    key_one,
    query_two,
    key_two,
    values,
    mix_weight,
    head_gain,
    residual,
    out_weight,
    norm_gain,
    lift_weight,
    gate_weight,
    conv_taps,
    down_weight,
):
    tokens = query_one.shape[0]
    own = residual.shape[0]
    width = residual.shape[1]
    z = lax.axis_index("z")
    y = lax.axis_index("y")
    core = lax.axis_index("core")
    along_y = jnp.stack([z * SIDE, 1 + 0 * z, y, SIDE + 0 * z])
    along_z = jnp.stack([y, SIDE + 0 * z, z * SIDE, 1 + 0 * z])
    plan = jnp.where(core == 0, along_y, along_z).astype(jnp.int32)
    smem = pl.BlockSpec(memory_space=pltpu.SMEM)
    hbm = pl.BlockSpec(memory_space=pltpu.HBM)
    x = lax.axis_index("x")
    place = jnp.stack([core, x, 2 * x + core]).astype(jnp.int32)
    above = lax.ppermute(out_weight, "x", [(i, (i + 1) % 4) for i in range(4)])
    below = lax.ppermute(out_weight, "x", [(i, (i + 3) % 4) for i in range(4)])
    qsend, ksend = pl.pallas_call(
        pack_kernel,
        out_shape=[
            jax.ShapeDtypeStruct((256, 128), bf16),
            jax.ShapeDtypeStruct((SIDE, SENT, 128), bf16),
        ],
        in_specs=[hbm] * 7,
        out_specs=[vmem(), hbm],
        scratch_shapes=[
            pltpu.VMEM((128, 256), bf16),
            pltpu.VMEM((32, 704), bf16),
            pltpu.VMEM((32, 704), bf16),
            pltpu.VMEM((SENT, 128), bf16),
            pltpu.SemaphoreType.DMA((7,)),
            pltpu.SemaphoreType.DMA((SIDE,)),
        ],
        compiler_params=SMALL,
        name="pack",
    )(*(in_hbm(a) for a in (query_one, query_two, key_one, key_two, values, lift_weight, gate_weight)))
    kpool = swapped(ksend, ALL, K_GROUPS)
    qpool = gathered(qsend, ALL, Q_GROUPS).reshape(SIDE, 256, 128)
    part = kpool[:, 512:, :].reshape(SIDE * 352, 128)
    weights = in_hbm(gathered(part, ALL, Q_GROUPS).reshape(SIDE, SIDE, 352, 128))
    out = pl.pallas_call(
        attend_kernel,
        grid=(1,),
        out_shape=jax.ShapeDtypeStruct((SIDE, PACK, 128), bf16),
        in_specs=[
            pl.BlockSpec(memory_space=pltpu.SMEM),
            vmem(),
            pl.BlockSpec((SIDE, 512, 128), lambda i: (0, 0, 0)),
        ],
        out_specs=vmem(),
        compiler_params=LARGE,
        name="attend",
    )(plan, qpool, kpool)
    back = swapped(out, ALL, Q_GROUPS)
    before = gathered(residual, TP)
    above, below, before = lax.optimization_barrier((above, below, before))
    across = (
        lax.ppermute(above[0:128], "x", [(i, (i + 1) % 4) for i in range(4)]),
        lax.ppermute(below[128:256], "x", [(i, (i + 3) % 4) for i in range(4)]),
    )
    heads = pl.pallas_call(
        join_kernel,
        out_shape=jax.ShapeDtypeStruct((4, tokens, VD), bf16),
        in_specs=[pl.BlockSpec(memory_space=pltpu.SMEM)] + [vmem()] * 2,
        out_specs=vmem(),
        compiler_params=SMALL,
        name="join",
    )(mix_weight, back, head_gain.reshape(1, VD))
    heads = swapped(heads, "x")
    half, sent = pl.pallas_call(
        project_kernel,
        out_shape=[
            jax.ShapeDtypeStruct((tokens, width), f32),
            jax.ShapeDtypeStruct((tokens, width), bf16),
        ],
        in_specs=[smem, vmem()] + [pl.BlockSpec(memory_space=pl.ANY)] * 5,
        out_specs=[vmem()] * 2,
        scratch_shapes=[pltpu.VMEM((4, VD, 2048), bf16), pltpu.SemaphoreType.DMA((5,))],
        compiler_params=SMALL,
        name="project",
    )(place, heads, in_hbm(out_weight), above, below, *across)
    other = lax.ppermute(sent, "core", [(0, 1), (1, 0)])
    gated, edge, rows, stream = pl.pallas_call(
        gate_kernel,
        out_shape=[
            jax.ShapeDtypeStruct((tokens, MAIN + 128), bf16),
            jax.ShapeDtypeStruct((16, MAIN + 128), bf16),
            jax.ShapeDtypeStruct((tokens, width), bf16),
            jax.ShapeDtypeStruct((own, width), f32),
        ],
        in_specs=[smem] + [vmem()] * 4 + [hbm],
        out_specs=[vmem()] * 4,
        scratch_shapes=[
            pltpu.VMEM((SIDE, SIDE, 192, 128), bf16),
            pltpu.SemaphoreType.DMA((SIDE,)),
        ],
        compiler_params=SMALL,
        name="gate",
    )(place, half, other, before, norm_gain.reshape(1, width), weights)
    route = [(i, i + 1) for i in range(SIDE * SIDE - 1)]
    prior = lax.ppermute(edge, ("z", "y"), route)
    lifted = pl.pallas_call(
        lift_kernel,
        out_shape=jax.ShapeDtypeStruct((tokens, MAIN), bf16),
        in_specs=[smem, vmem(), hbm],
        out_specs=vmem(),
        scratch_shapes=[
            pltpu.VMEM((SIDE, SIDE, 160, 128), bf16),
            pltpu.SemaphoreType.DMA((SIDE,)),
        ],
        compiler_params=SMALL,
        cost_estimate=pl.CostEstimate(
            flops=2 * 128 * 2048 * 640, bytes_accessed=3 << 20, transcendentals=0
        ),
        name="lift",
    )(place, rows, weights)
    gap = jnp.zeros((WIDTH, 64), f32)
    taps = jnp.concatenate([conv_taps[:, :MAIN], gap, conv_taps[:, MAIN:]], axis=1)
    keep, give = pl.pallas_call(
        down_kernel,
        out_shape=[
            jax.ShapeDtypeStruct((tokens // 2, width), f32),
            jax.ShapeDtypeStruct((tokens // 2, width), bf16),
        ],
        in_specs=[smem] + [vmem()] * 5,
        out_specs=[vmem()] * 2,
        scratch_shapes=[pltpu.VMEM((128, 2048), f32)],
        compiler_params=SMALL,
        name="down",
    )(place, gated, lifted, prior, taps, down_weight)
    taken = lax.ppermute(give, "core", [(0, 1), (1, 0)])
    pair = pl.pallas_call(
        pair_kernel,
        out_shape=jax.ShapeDtypeStruct((4, own, width), bf16),
        in_specs=[vmem()] * 2,
        out_specs=vmem(),
        compiler_params=SMALL,
        name="pair",
    )(keep, taken)
    mixer = swapped(pair, "x")
    return pl.pallas_call(
        last_kernel,
        out_shape=jax.ShapeDtypeStruct((own, width), bf16),
        in_specs=[vmem()] * 2,
        out_specs=vmem(),
        compiler_params=SMALL,
        name="last",
    )(mixer, stream)


def solution(mesh):
    fine = Mesh(mesh.devices.reshape(SIDE, SIDE, 4, 2), ("z", "y", "x", "core"))
    sp = ("z", "y")

    return jax.shard_map(
        on_device,
        mesh=fine,
        in_specs=(
            P(sp, TP),
            P(sp, TP),
            P(sp, TP),
            P(sp, TP),
            P(sp, TP),
            P(TP),
            P(),
            P(("z", "y", "x", "core"), None),
            P(TP, None),
            P(),
            P(sp, TP),
            P(sp, TP),
            P(None, TP),
            P(TP, None),
        ),
        out_specs=P(("z", "y", "x", "core"), None),
        check_vma=False,
    )
```

```python
import jax
import jax.numpy as jnp
import numpy as np
from jax import lax
from jax.experimental import pallas as pl
from jax.experimental.pallas import tpu as pltpu
from jax.sharding import Mesh, PartitionSpec as P

HD = 128
VD = 256
STRETCH = 64
WIDTH = 3
SIDE = 8
BLOCK = 128
PACK = 4 * BLOCK + 16
TILES = 5
MAIN = 128 * TILES
SENT = 512 + 352
SHIFTS = (0, 1, -1, 2)
epsilon = 1e-06
masked_score = -1e30
LOG2E = 1.4426950408889634
EXP2_SCALE = LOG2E * HD**-0.5
f32 = jnp.float32
bf16 = jnp.bfloat16
TP = ("x", "core")
ALL = ("z", "y", "x", "core")
PLACES = np.arange(SIDE * SIDE * 8).reshape(SIDE, SIDE, 4, 2)
ROWS = [[PLACES[i, :, x, c].tolist() for i in range(SIDE) for x in range(4)] for c in range(2)]
COLS = [[PLACES[:, i, x, c].tolist() for i in range(SIDE) for x in range(4)] for c in range(2)]
Q_GROUPS = ROWS[0] + COLS[1]
K_GROUPS = COLS[0] + ROWS[1]


def vmem():
    return pl.BlockSpec(memory_space=pltpu.VMEM)


def pack_kernel(q1, q2, k1, k2, v, lift, gate, qsend, ksend, vv, ll, gg, rows, sems, sent):
    moves = [
        pltpu.make_async_copy(src, dst, sems.at[i])
        for i, (src, dst) in enumerate(
            (
                (k1, rows.at[0:128]),
                (k2, rows.at[128:256]),
                (v, vv),
                (lift, ll),
                (gate, gg),
                (q1, qsend.at[0:128]),
                (q2, qsend.at[128:256]),
            )
        )
    ]
    for move in moves:
        move.start()
    for move in moves:
        move.wait()
    rows[256:384, :] = vv[:, 0:128]
    rows[384:512, :] = vv[:, 128:256]
    for n in range(TILES):
        rows[512 + 32 * n : 544 + 32 * n, :] = gg[:, 128 * n : 128 * n + 128]
        rows[704 + 32 * n : 736 + 32 * n, :] = ll[:, 128 * n : 128 * n + 128]
    rows[672:704, :] = jnp.concatenate([ll[:, MAIN:], gg[:, MAIN:]], axis=1)
    copies = [pltpu.make_async_copy(rows, ksend.at[i], sent.at[i]) for i in range(SIDE)]
    for copy in copies:
        copy.start()
    for copy in copies:
        copy.wait()


def attend_kernel(plan, qpool, kpool, out):
    q_base, q_step, k_base, k_step = (plan[i] for i in range(4))
    at = lax.broadcasted_iota(jnp.int32, (16, 128), 0)
    row = lax.broadcasted_iota(jnp.int32, (256, 1), 0)
    col = lax.broadcasted_iota(jnp.int32, (1, 1024), 1)
    k_at = 2 * (k_base + k_step * (col // 128)) + (col % 128) // STRETCH
    vals = jnp.concatenate(
        [kpool[:, 256:384, :].reshape(1024, 128), kpool[:, 384:512, :].reshape(1024, 128)], axis=1
    )
    for c in range(SIDE // 2):
        q_at = 2 * (q_base + q_step * (2 * c + row // 128)) + (row % 128) // STRETCH
        seen = k_at <= q_at
        levels = []
        for m in range(2):
            lo = slice(128 * m, 128 * m + 128)
            q = jnp.concatenate([qpool[2 * c, lo, :], qpool[2 * c + 1, lo, :]], axis=0)
            k = kpool[:, lo, :].reshape(1024, 128)
            s = lax.dot_general(q, k, (((1,), (1,)), ((), ())), preferred_element_type=f32)
            s = jnp.where(seen, s, masked_score)
            top = jnp.max(s, axis=-1, keepdims=True)
            w = jnp.exp2((s - top) * EXP2_SCALE)
            total = jnp.sum(w, axis=-1, keepdims=True)
            o = (jnp.dot(w.astype(bf16), vals, preferred_element_type=f32) / total).astype(bf16)
            level = top * EXP2_SCALE + jnp.log2(total)
            levels.append(jnp.where(top > 0.5 * masked_score, level, masked_score))
            for h in range(2):
                for e in range(2):
                    out[2 * c + h, 256 * m + 128 * e : 256 * m + 128 * e + 128, :] = o[
                        128 * h : 128 * h + 128, 128 * e : 128 * e + 128
                    ]
        for h in range(2):
            rows = jnp.zeros((16, 128), f32)
            for m in range(2):
                wide = jnp.transpose(
                    jnp.broadcast_to(levels[m][128 * h : 128 * h + 128], (128, 128))
                )[0:16]
                a = wide.astype(bf16).astype(f32)
                b = (wide - a).astype(bf16).astype(f32)
                d = wide - a - b
                for n, piece in enumerate((a, b, d)):
                    rows = jnp.where(at == 3 * m + n, piece, rows)
            out[2 * c + h, 512:528, :] = rows.astype(bf16)


def join_kernel(mix, parts, gain, residual, out):
    tails = [parts[i, 512:528, :].astype(f32) for i in range(SIDE)]

    def joined(m):
        levels = jnp.concatenate(
            [jnp.sum(tail[3 * m : 3 * m + 3], axis=0, keepdims=True) for tail in tails], axis=0
        )
        top = jnp.max(levels, axis=0, keepdims=True)
        w = jnp.exp2(levels - top)
        w = w / jnp.sum(w, axis=0, keepdims=True)
        w = jnp.transpose(jnp.concatenate([w, jnp.zeros((120, 128), f32)], axis=0))
        acc = [jnp.zeros((128, 128), f32), jnp.zeros((128, 128), f32)]
        for i in range(SIDE):
            wi = w[:, i : i + 1]
            for e in range(2):
                at = 256 * m + 128 * e
                acc[e] = acc[e] + wi * parts[i, at : at + 128, :].astype(f32)
        return jnp.concatenate(acc, axis=1)

    mixed = joined(0) - mix[0] * joined(1)
    r = lax.rsqrt(jnp.mean(mixed * mixed, axis=-1, keepdims=True) + epsilon)
    head = (mixed * r * gain[...]).astype(bf16)
    for i in range(4):
        out[i, 0:128] = head
        for j in range(8):
            out[i, 128 + 16 * j : 144 + 16 * j, :] = residual[:, 256 * j : 256 * j + 256]


def own_rows(place, i):
    return pl.ds(pl.multiple_of(32 * i + 16 * place[0], 16), 16)


def other_rows(place, i):
    return pl.ds(pl.multiple_of(32 * i + 16 - 16 * place[0], 16), 16)


def project_kernel(place, heads, *refs):
    weights, (half, sent, buffer, sems) = refs[:4], refs[4:]
    x = place[1]
    moves = [
        pltpu.make_async_copy(weight, buffer.at[i], sems.at[i]) for i, weight in enumerate(weights)
    ]
    for move in moves:
        move.start()
    for i, shift in enumerate(SHIFTS):
        moves[i].wait()
        head = heads[lax.rem(x + 4 - shift, 4), 0:128]
        for n in range(0, 2048, 256):
            d = jnp.dot(head, buffer[i, :, n : n + 256], preferred_element_type=f32)
            if i > 0:
                d = d + half[:, n : n + 256]
            half[:, n : n + 256] = d
    for i in range(4):
        rows = own_rows(place, i)
        for j in range(8):
            r = heads[i, 128 + 16 * j : 144 + 16 * j, :].astype(f32)
            half[rows, 256 * j : 256 * j + 256] = half[rows, 256 * j : 256 * j + 256] + r
    sent[...] = half[...].astype(bf16)


def fetched(core, weights, buffer, sems, first):
    height = buffer.shape[2]
    for g in range(SIDE):
        rows = pl.ds(first, height)

        @pl.when(core == 0)
        def _():
            pltpu.make_async_copy(weights.at[:, g, rows, :], buffer.at[g], sems.at[g]).start()

        @pl.when(core != 0)
        def _():
            pltpu.make_async_copy(weights.at[g, :, rows, :], buffer.at[g], sems.at[g]).start()


def multiplied(rows, weights, buffer, sems, first):
    height = buffer.shape[2]
    count = height // 32
    acc = [None] * ((count + 1) // 2)
    for g in range(SIDE):
        pltpu.make_async_copy(
            weights.at[0, :, pl.ds(first, height), :], buffer.at[g], sems.at[g]
        ).wait()
        lhs = rows[:, 256 * g : 256 * g + 256]
        for n in range(0, count, 2):
            tiles = [
                buffer[g, :, 32 * m : 32 * m + 32, :].reshape(256, 128)
                for m in range(n, min(n + 2, count))
            ]
            rhs = jnp.concatenate(tiles, axis=1) if len(tiles) > 1 else tiles[0]
            d = jnp.dot(lhs, rhs, preferred_element_type=f32)
            acc[n // 2] = d if acc[n // 2] is None else acc[n // 2] + d
    return acc


def gate_kernel(place, half, other, gain, weights, gated, edge, rows, stream, buffer, sems):
    fetched(place[0], weights, buffer, sems, 0)
    for n in range(0, 128, 32):
        total = half[n : n + 32] + other[n : n + 32].astype(f32)
        r = lax.rsqrt(jnp.mean(total * total, axis=-1, keepdims=True) + epsilon)
        rows[n : n + 32] = (total * r * gain[...]).astype(bf16)
    own = pl.ds(pl.multiple_of(place[2] * 16, 16), 16)
    stream[...] = half[own] + other[own].astype(f32)
    for n, part in enumerate(multiplied(rows, weights, buffer, sems, 0)):
        part = part.astype(bf16)
        gated[:, 256 * n : 256 * n + 256] = part
        edge[:, 256 * n : 256 * n + 256] = part[112:128]


def lift_kernel(core, rows, weights, lifted, buffer, sems):
    fetched(core[0], weights, buffer, sems, 192)
    for n, part in enumerate(multiplied(rows, weights, buffer, sems, 192)):
        lifted[:, 256 * n : 256 * n + part.shape[1]] = part.astype(bf16)


def down_kernel(place, gated, lifted, prior, taps, weight, keep, give, whole):
    at = lax.broadcasted_iota(jnp.int32, (128, 1), 0)

    def activated(lo, hi):
        g = gated[:, lo:hi].astype(f32)
        p = prior[:, lo:hi].astype(f32)
        one = jnp.where(at == 0, p[15:16], pltpu.roll(g, 1, 0))
        two = jnp.where(at == 0, p[14:15], jnp.where(at == 1, p[15:16], pltpu.roll(g, 2, 0)))
        conv = taps[0:1, lo:hi] * two + taps[1:2, lo:hi] * one + taps[2:3, lo:hi] * g
        return g, conv * jax.nn.sigmoid(conv)

    acc = None
    for n in range(0, MAIN, 128):
        _, a = activated(n, n + 128)
        h = (a * lifted[:, n : n + 128].astype(f32)).astype(bf16)
        d = jnp.dot(h, weight[n : n + 128, :], preferred_element_type=f32)
        acc = d if acc is None else acc + d
    g, a = activated(MAIN, MAIN + 128)
    h = (pltpu.roll(a, 64, 1) * g).astype(bf16)
    whole[...] = acc + jnp.dot(h[:, 0:64], weight[MAIN:, :], preferred_element_type=f32)
    for i in range(4):
        keep[16 * i : 16 * i + 16] = whole[own_rows(place, i)]
        give[16 * i : 16 * i + 16] = whole[other_rows(place, i)].astype(bf16)


def pair_kernel(keep, other, out):
    for i in range(4):
        rows = slice(16 * i, 16 * i + 16)
        out[i] = (keep[rows] + other[rows].astype(f32)).astype(bf16)


def last_kernel(parts, stream, out):
    mixer = parts[0].astype(f32)
    for i in range(1, 4):
        mixer = mixer + parts[i].astype(f32)
    out[...] = (stream[...] + mixer).astype(bf16)


def swapped(a, axis, groups=None):
    return lax.all_to_all(a, axis, 0, 0, axis_index_groups=groups, tiled=True)


def gathered(a, axis, groups=None):
    return lax.all_gather(a, axis, axis_index_groups=groups, axis=0, tiled=True)


def in_hbm(a):
    return pltpu.with_memory_space_constraint(a, pltpu.HBM)


SMALL = pltpu.CompilerParams(vmem_limit_bytes=20 << 20)
LARGE = pltpu.CompilerParams(vmem_limit_bytes=30 << 20)


def on_device(
    query_one,
    key_one,
    query_two,
    key_two,
    values,
    mix_weight,
    head_gain,
    residual,
    out_weight,
    norm_gain,
    lift_weight,
    gate_weight,
    conv_taps,
    down_weight,
):
    tokens = query_one.shape[0]
    own = residual.shape[0]
    width = residual.shape[1]
    z = lax.axis_index("z")
    y = lax.axis_index("y")
    core = lax.axis_index("core")
    along_y = jnp.stack([z * SIDE, 1 + 0 * z, y, SIDE + 0 * z])
    along_z = jnp.stack([y, SIDE + 0 * z, z * SIDE, 1 + 0 * z])
    plan = jnp.where(core == 0, along_y, along_z).astype(jnp.int32)
    smem = pl.BlockSpec(memory_space=pltpu.SMEM)
    hbm = pl.BlockSpec(memory_space=pltpu.HBM)
    x = lax.axis_index("x")
    place = jnp.stack([core, x, 2 * x + core]).astype(jnp.int32)
    qsend, ksend = pl.pallas_call(
        pack_kernel,
        out_shape=[
            jax.ShapeDtypeStruct((256, 128), bf16),
            jax.ShapeDtypeStruct((SIDE, SENT, 128), bf16),
        ],
        in_specs=[hbm] * 7,
        out_specs=[vmem(), hbm],
        scratch_shapes=[
            pltpu.VMEM((128, 256), bf16),
            pltpu.VMEM((32, 704), bf16),
            pltpu.VMEM((32, 704), bf16),
            pltpu.VMEM((SENT, 128), bf16),
            pltpu.SemaphoreType.DMA((7,)),
            pltpu.SemaphoreType.DMA((SIDE,)),
        ],
        compiler_params=SMALL,
        name="pack",
    )(*(in_hbm(a) for a in (query_one, query_two, key_one, key_two, values, lift_weight, gate_weight)))
    kpool = swapped(ksend, ALL, K_GROUPS)
    qpool = gathered(qsend, ALL, Q_GROUPS).reshape(SIDE, 256, 128)
    part = kpool[:, 512:, :].reshape(SIDE * 352, 128)
    weights = in_hbm(gathered(part, ALL, Q_GROUPS).reshape(SIDE, SIDE, 352, 128))
    ring = [(i, (i + 1) % 4) for i in range(4)]
    above = lax.ppermute(out_weight, "x", ring)
    out = pl.pallas_call(
        attend_kernel,
        grid=(1,),
        out_shape=jax.ShapeDtypeStruct((SIDE, PACK, 128), bf16),
        in_specs=[
            pl.BlockSpec(memory_space=pltpu.SMEM),
            vmem(),
            pl.BlockSpec((SIDE, 512, 128), lambda i: (0, 0, 0)),
        ],
        out_specs=vmem(),
        compiler_params=LARGE,
        name="attend",
    )(plan, qpool, kpool)
    back = swapped(out, ALL, Q_GROUPS)
    across = lax.ppermute(above, "x", ring)
    below = lax.ppermute(out_weight, "x", [(j, i) for i, j in ring])
    heads = pl.pallas_call(
        join_kernel,
        out_shape=jax.ShapeDtypeStruct((4, 2 * tokens, VD), bf16),
        in_specs=[pl.BlockSpec(memory_space=pltpu.SMEM)] + [vmem()] * 3,
        out_specs=vmem(),
        compiler_params=SMALL,
        name="join",
    )(mix_weight, back, head_gain.reshape(1, VD), residual)
    heads = swapped(heads, "x")
    half, sent = pl.pallas_call(
        project_kernel,
        out_shape=[
            jax.ShapeDtypeStruct((tokens, width), f32),
            jax.ShapeDtypeStruct((tokens, width), bf16),
        ],
        in_specs=[smem, vmem()] + [pl.BlockSpec(memory_space=pl.ANY)] * 4,
        out_specs=[vmem()] * 2,
        scratch_shapes=[pltpu.VMEM((4, VD, 2048), bf16), pltpu.SemaphoreType.DMA((4,))],
        compiler_params=SMALL,
        name="project",
    )(place, heads, *(in_hbm(a) for a in (out_weight, above, below, across)))
    other = lax.ppermute(sent, "core", [(0, 1), (1, 0)])
    gated, edge, rows, stream = pl.pallas_call(
        gate_kernel,
        out_shape=[
            jax.ShapeDtypeStruct((tokens, MAIN + 128), bf16),
            jax.ShapeDtypeStruct((16, MAIN + 128), bf16),
            jax.ShapeDtypeStruct((tokens, width), bf16),
            jax.ShapeDtypeStruct((own, width), f32),
        ],
        in_specs=[smem] + [vmem()] * 3 + [hbm],
        out_specs=[vmem()] * 4,
        scratch_shapes=[
            pltpu.VMEM((SIDE, SIDE, 192, 128), bf16),
            pltpu.SemaphoreType.DMA((SIDE,)),
        ],
        compiler_params=SMALL,
        name="gate",
    )(place, half, other, norm_gain.reshape(1, width), weights)
    route = [(i, i + 1) for i in range(SIDE * SIDE - 1)]
    prior = lax.ppermute(edge, ("z", "y"), route)
    lifted = pl.pallas_call(
        lift_kernel,
        out_shape=jax.ShapeDtypeStruct((tokens, MAIN), bf16),
        in_specs=[smem, vmem(), hbm],
        out_specs=vmem(),
        scratch_shapes=[
            pltpu.VMEM((SIDE, SIDE, 160, 128), bf16),
            pltpu.SemaphoreType.DMA((SIDE,)),
        ],
        compiler_params=SMALL,
        cost_estimate=pl.CostEstimate(
            flops=2 * 128 * 2048 * 640, bytes_accessed=3 << 20, transcendentals=0
        ),
        name="lift",
    )(place, rows, weights)
    gap = jnp.zeros((WIDTH, 64), f32)
    taps = jnp.concatenate([conv_taps[:, :MAIN], gap, conv_taps[:, MAIN:]], axis=1)
    keep, give = pl.pallas_call(
        down_kernel,
        out_shape=[
            jax.ShapeDtypeStruct((tokens // 2, width), f32),
            jax.ShapeDtypeStruct((tokens // 2, width), bf16),
        ],
        in_specs=[smem] + [vmem()] * 5,
        out_specs=[vmem()] * 2,
        scratch_shapes=[pltpu.VMEM((128, 2048), f32)],
        compiler_params=SMALL,
        name="down",
    )(place, gated, lifted, prior, taps, down_weight)
    taken = lax.ppermute(give, "core", [(0, 1), (1, 0)])
    pair = pl.pallas_call(
        pair_kernel,
        out_shape=jax.ShapeDtypeStruct((4, own, width), bf16),
        in_specs=[vmem()] * 2,
        out_specs=vmem(),
        compiler_params=SMALL,
        name="pair",
    )(keep, taken)
    mixer = swapped(pair, "x")
    return pl.pallas_call(
        last_kernel,
        out_shape=jax.ShapeDtypeStruct((own, width), bf16),
        in_specs=[vmem()] * 2,
        out_specs=vmem(),
        compiler_params=SMALL,
        name="last",
    )(mixer, stream)


def solution(mesh):
    fine = Mesh(mesh.devices.reshape(SIDE, SIDE, 4, 2), ("z", "y", "x", "core"))
    sp = ("z", "y")

    return jax.shard_map(
        on_device,
        mesh=fine,
        in_specs=(
            P(sp, TP),
            P(sp, TP),
            P(sp, TP),
            P(sp, TP),
            P(sp, TP),
            P(TP),
            P(),
            P(("z", "y", "x", "core"), None),
            P(TP, None),
            P(),
            P(sp, TP),
            P(sp, TP),
            P(None, TP),
            P(TP, None),
        ),
        out_specs=P(("z", "y", "x", "core"), None),
        check_vma=False,
    )
```

```python
import jax
import jax.numpy as jnp
import numpy as np
from jax import lax
from jax.experimental import pallas as pl
from jax.experimental.pallas import tpu as pltpu
from jax.sharding import Mesh, PartitionSpec as P

HD = 128
VD = 256
STRETCH = 64
WIDTH = 3
SIDE = 8
BLOCK = 128
PACK = 4 * BLOCK + 16
TILES = 5
MAIN = 128 * TILES
SENT = 512 + 352
SHIFTS = (0, 1, -1, 2)
epsilon = 1e-06
masked_score = -1e30
LOG2E = 1.4426950408889634
EXP2_SCALE = LOG2E * HD**-0.5
f32 = jnp.float32
bf16 = jnp.bfloat16
TP = ("x", "core")
ALL = ("z", "y", "x", "core")
PLACES = np.arange(SIDE * SIDE * 8).reshape(SIDE, SIDE, 4, 2)
ROWS = [[PLACES[i, :, x, c].tolist() for i in range(SIDE) for x in range(4)] for c in range(2)]
COLS = [[PLACES[:, i, x, c].tolist() for i in range(SIDE) for x in range(4)] for c in range(2)]
Q_GROUPS = ROWS[0] + COLS[1]
K_GROUPS = COLS[0] + ROWS[1]


def vmem():
    return pl.BlockSpec(memory_space=pltpu.VMEM)


def pack_kernel(q1, q2, k1, k2, v, lift, gate, qsend, ksend, vv, ll, gg, rows, sems, sent):
    moves = [
        pltpu.make_async_copy(src, dst, sems.at[i])
        for i, (src, dst) in enumerate(
            (
                (k1, rows.at[0:128]),
                (k2, rows.at[128:256]),
                (v, vv),
                (lift, ll),
                (gate, gg),
                (q1, qsend.at[0:128]),
                (q2, qsend.at[128:256]),
            )
        )
    ]
    for move in moves:
        move.start()
    for move in moves:
        move.wait()
    rows[256:384, :] = vv[:, 0:128]
    rows[384:512, :] = vv[:, 128:256]
    for n in range(TILES):
        rows[512 + 32 * n : 544 + 32 * n, :] = gg[:, 128 * n : 128 * n + 128]
        rows[704 + 32 * n : 736 + 32 * n, :] = ll[:, 128 * n : 128 * n + 128]
    rows[672:704, :] = jnp.concatenate([ll[:, MAIN:], gg[:, MAIN:]], axis=1)
    copies = [pltpu.make_async_copy(rows, ksend.at[i], sent.at[i]) for i in range(SIDE)]
    for copy in copies:
        copy.start()
    for copy in copies:
        copy.wait()


def attend_kernel(plan, qpool, kpool, result, out, sems):
    q_base, q_step, k_base, k_step = (plan[i] for i in range(4))
    at = lax.broadcasted_iota(jnp.int32, (16, 128), 0)
    row = lax.broadcasted_iota(jnp.int32, (256, 1), 0)
    col = lax.broadcasted_iota(jnp.int32, (1, 1024), 1)
    k_at = 2 * (k_base + k_step * (col // 128)) + (col % 128) // STRETCH
    vals = jnp.concatenate(
        [kpool[:, 256:384, :].reshape(1024, 128), kpool[:, 384:512, :].reshape(1024, 128)], axis=1
    )
    for c in range(SIDE // 2):
        q_at = 2 * (q_base + q_step * (2 * c + row // 128)) + (row % 128) // STRETCH
        seen = k_at <= q_at
        levels = []
        for m in range(2):
            lo = slice(128 * m, 128 * m + 128)
            q = jnp.concatenate([qpool[2 * c, lo, :], qpool[2 * c + 1, lo, :]], axis=0)
            k = kpool[:, lo, :].reshape(1024, 128)
            s = lax.dot_general(q, k, (((1,), (1,)), ((), ())), preferred_element_type=f32)
            s = jnp.where(seen, s, masked_score)
            top = jnp.max(s, axis=-1, keepdims=True)
            w = jnp.exp2((s - top) * EXP2_SCALE)
            total = jnp.sum(w, axis=-1, keepdims=True)
            o = (jnp.dot(w.astype(bf16), vals, preferred_element_type=f32) / total).astype(bf16)
            level = top * EXP2_SCALE + jnp.log2(total)
            levels.append(jnp.where(top > 0.5 * masked_score, level, masked_score))
            for h in range(2):
                for e in range(2):
                    out[2 * c + h, 256 * m + 128 * e : 256 * m + 128 * e + 128, :] = o[
                        128 * h : 128 * h + 128, 128 * e : 128 * e + 128
                    ]
        for h in range(2):
            rows = jnp.zeros((16, 128), f32)
            for m in range(2):
                wide = jnp.transpose(
                    jnp.broadcast_to(levels[m][128 * h : 128 * h + 128], (128, 128))
                )[0:16]
                a = wide.astype(bf16).astype(f32)
                b = (wide - a).astype(bf16).astype(f32)
                d = wide - a - b
                for n, piece in enumerate((a, b, d)):
                    rows = jnp.where(at == 3 * m + n, piece, rows)
            out[2 * c + h, 512:528, :] = rows.astype(bf16)
        pair = pl.ds(2 * c, 2)
        pltpu.make_async_copy(out.at[pair], result.at[pair], sems.at[c]).start()
    for c in range(SIDE // 2):
        pair = pl.ds(2 * c, 2)
        pltpu.make_async_copy(out.at[pair], result.at[pair], sems.at[c]).wait()


def join_kernel(mix, parts, gain, residual, out):
    tails = [parts[i, 512:528, :].astype(f32) for i in range(SIDE)]

    def joined(m):
        levels = jnp.concatenate(
            [jnp.sum(tail[3 * m : 3 * m + 3], axis=0, keepdims=True) for tail in tails], axis=0
        )
        top = jnp.max(levels, axis=0, keepdims=True)
        w = jnp.exp2(levels - top)
        w = w / jnp.sum(w, axis=0, keepdims=True)
        w = jnp.transpose(jnp.concatenate([w, jnp.zeros((120, 128), f32)], axis=0))
        acc = [jnp.zeros((128, 128), f32), jnp.zeros((128, 128), f32)]
        for i in range(SIDE):
            wi = w[:, i : i + 1]
            for e in range(2):
                at = 256 * m + 128 * e
                acc[e] = acc[e] + wi * parts[i, at : at + 128, :].astype(f32)
        return jnp.concatenate(acc, axis=1)

    mixed = joined(0) - mix[0] * joined(1)
    r = lax.rsqrt(jnp.mean(mixed * mixed, axis=-1, keepdims=True) + epsilon)
    head = (mixed * r * gain[...]).astype(bf16)
    for i in range(4):
        out[i, 0:128] = head
        for j in range(8):
            out[i, 128 + 16 * j : 144 + 16 * j, :] = residual[:, 256 * j : 256 * j + 256]


def own_rows(place, i):
    return pl.ds(pl.multiple_of(32 * i + 16 * place[0], 16), 16)


def other_rows(place, i):
    return pl.ds(pl.multiple_of(32 * i + 16 - 16 * place[0], 16), 16)


def project_kernel(place, heads, *refs):
    weights, (half, sent, buffer, sems) = refs[:4], refs[4:]
    x = place[1]
    moves = [
        pltpu.make_async_copy(weight, buffer.at[i], sems.at[i]) for i, weight in enumerate(weights)
    ]
    for move in moves:
        move.start()
    for i, shift in enumerate(SHIFTS):
        moves[i].wait()
        head = heads[lax.rem(x + 4 - shift, 4), 0:128]
        for n in range(0, 2048, 256):
            d = jnp.dot(head, buffer[i, :, n : n + 256], preferred_element_type=f32)
            if i > 0:
                d = d + half[:, n : n + 256]
            half[:, n : n + 256] = d
    for i in range(4):
        rows = own_rows(place, i)
        for j in range(8):
            r = heads[i, 128 + 16 * j : 144 + 16 * j, :].astype(f32)
            half[rows, 256 * j : 256 * j + 256] = half[rows, 256 * j : 256 * j + 256] + r
    sent[...] = half[...].astype(bf16)


def fetched(core, weights, buffer, sems, first):
    height = buffer.shape[2]
    for g in range(SIDE):
        rows = pl.ds(first, height)

        @pl.when(core == 0)
        def _():
            pltpu.make_async_copy(weights.at[:, g, rows, :], buffer.at[g], sems.at[g]).start()

        @pl.when(core != 0)
        def _():
            pltpu.make_async_copy(weights.at[g, :, rows, :], buffer.at[g], sems.at[g]).start()


def multiplied(rows, buffer, ready):
    count = buffer.shape[2] // 32
    acc = [None] * ((count + 1) // 2)
    for g in range(SIDE):
        ready(g)
        lhs = rows[:, 256 * g : 256 * g + 256]
        for n in range(0, count, 2):
            tiles = [
                buffer[g, :, 32 * m : 32 * m + 32, :].reshape(256, 128)
                for m in range(n, min(n + 2, count))
            ]
            rhs = jnp.concatenate(tiles, axis=1) if len(tiles) > 1 else tiles[0]
            d = jnp.dot(lhs, rhs, preferred_element_type=f32)
            acc[n // 2] = d if acc[n // 2] is None else acc[n // 2] + d
    return acc


def gate_kernel(place, half, other, gain, weights, gated, edge, rows, stream, later, buffer, sems, more):
    fetched(place[0], weights, buffer, sems, 0)
    fetched(place[0], weights, later, more, 192)
    for n in range(0, 128, 32):
        total = half[n : n + 32] + other[n : n + 32].astype(f32)
        r = lax.rsqrt(jnp.mean(total * total, axis=-1, keepdims=True) + epsilon)
        rows[n : n + 32] = (total * r * gain[...]).astype(bf16)
    own = pl.ds(pl.multiple_of(place[2] * 16, 16), 16)
    stream[...] = half[own] + other[own].astype(f32)

    def ready(g):
        pltpu.make_async_copy(
            weights.at[0, :, pl.ds(0, 192), :], buffer.at[g], sems.at[g]
        ).wait()

    for n, part in enumerate(multiplied(rows, buffer, ready)):
        part = part.astype(bf16)
        gated[:, 256 * n : 256 * n + 256] = part
        edge[:, 256 * n : 256 * n + 256] = part[112:128]
    for g in range(SIDE):
        pltpu.make_async_copy(
            weights.at[0, :, pl.ds(192, 160), :], later.at[g], more.at[g]
        ).wait()


def lift_kernel(rows, weights, lifted):
    for n, part in enumerate(multiplied(rows, weights, lambda g: None)):
        lifted[:, 256 * n : 256 * n + part.shape[1]] = part.astype(bf16)


def down_kernel(place, gated, lifted, prior, taps, weight, keep, give, whole):
    at = lax.broadcasted_iota(jnp.int32, (128, 1), 0)

    def activated(lo, hi):
        g = gated[:, lo:hi].astype(f32)
        p = prior[:, lo:hi].astype(f32)
        one = jnp.where(at == 0, p[15:16], pltpu.roll(g, 1, 0))
        two = jnp.where(at == 0, p[14:15], jnp.where(at == 1, p[15:16], pltpu.roll(g, 2, 0)))
        conv = taps[0:1, lo:hi] * two + taps[1:2, lo:hi] * one + taps[2:3, lo:hi] * g
        return g, conv * jax.nn.sigmoid(conv)

    acc = None
    for n in range(0, MAIN, 128):
        _, a = activated(n, n + 128)
        h = (a * lifted[:, n : n + 128].astype(f32)).astype(bf16)
        d = jnp.dot(h, weight[n : n + 128, :], preferred_element_type=f32)
        acc = d if acc is None else acc + d
    g, a = activated(MAIN, MAIN + 128)
    h = (pltpu.roll(a, 64, 1) * g).astype(bf16)
    whole[...] = acc + jnp.dot(h[:, 0:64], weight[MAIN:, :], preferred_element_type=f32)
    for i in range(4):
        keep[16 * i : 16 * i + 16] = whole[own_rows(place, i)]
        give[16 * i : 16 * i + 16] = whole[other_rows(place, i)].astype(bf16)


def pair_kernel(keep, other, out):
    for i in range(4):
        rows = slice(16 * i, 16 * i + 16)
        out[i] = (keep[rows] + other[rows].astype(f32)).astype(bf16)


def last_kernel(parts, stream, out):
    mixer = parts[0].astype(f32)
    for i in range(1, 4):
        mixer = mixer + parts[i].astype(f32)
    out[...] = (stream[...] + mixer).astype(bf16)


def swapped(a, axis, groups=None):
    return lax.all_to_all(a, axis, 0, 0, axis_index_groups=groups, tiled=True)


def gathered(a, axis, groups=None):
    return lax.all_gather(a, axis, axis_index_groups=groups, axis=0, tiled=True)


def in_hbm(a):
    return pltpu.with_memory_space_constraint(a, pltpu.HBM)


SMALL = pltpu.CompilerParams(vmem_limit_bytes=20 << 20)
LARGE = pltpu.CompilerParams(vmem_limit_bytes=30 << 20)


def on_device(
    query_one,
    key_one,
    query_two,
    key_two,
    values,
    mix_weight,
    head_gain,
    residual,
    out_weight,
    norm_gain,
    lift_weight,
    gate_weight,
    conv_taps,
    down_weight,
):
    tokens = query_one.shape[0]
    own = residual.shape[0]
    width = residual.shape[1]
    z = lax.axis_index("z")
    y = lax.axis_index("y")
    core = lax.axis_index("core")
    along_y = jnp.stack([z * SIDE, 1 + 0 * z, y, SIDE + 0 * z])
    along_z = jnp.stack([y, SIDE + 0 * z, z * SIDE, 1 + 0 * z])
    plan = jnp.where(core == 0, along_y, along_z).astype(jnp.int32)
    smem = pl.BlockSpec(memory_space=pltpu.SMEM)
    hbm = pl.BlockSpec(memory_space=pltpu.HBM)
    x = lax.axis_index("x")
    place = jnp.stack([core, x, 2 * x + core]).astype(jnp.int32)
    qsend, ksend = pl.pallas_call(
        pack_kernel,
        out_shape=[
            jax.ShapeDtypeStruct((256, 128), bf16),
            jax.ShapeDtypeStruct((SIDE, SENT, 128), bf16),
        ],
        in_specs=[hbm] * 7,
        out_specs=[vmem(), hbm],
        scratch_shapes=[
            pltpu.VMEM((128, 256), bf16),
            pltpu.VMEM((32, 704), bf16),
            pltpu.VMEM((32, 704), bf16),
            pltpu.VMEM((SENT, 128), bf16),
            pltpu.SemaphoreType.DMA((7,)),
            pltpu.SemaphoreType.DMA((SIDE,)),
        ],
        compiler_params=SMALL,
        name="pack",
    )(*(in_hbm(a) for a in (query_one, query_two, key_one, key_two, values, lift_weight, gate_weight)))
    kpool = swapped(ksend, ALL, K_GROUPS)
    qpool = gathered(qsend, ALL, Q_GROUPS).reshape(SIDE, 256, 128)
    part = kpool[:, 512:, :].reshape(SIDE * 352, 128)
    weights = in_hbm(gathered(part, ALL, Q_GROUPS).reshape(SIDE, SIDE, 352, 128))
    ring = [(i, (i + 1) % 4) for i in range(4)]
    above = lax.ppermute(out_weight, "x", ring)
    out = pl.pallas_call(
        attend_kernel,
        out_shape=pltpu.HBM((SIDE, PACK, 128), bf16),
        in_specs=[pl.BlockSpec(memory_space=pltpu.SMEM), vmem(), vmem()],
        out_specs=hbm,
        scratch_shapes=[
            pltpu.VMEM((SIDE, PACK, 128), bf16),
            pltpu.SemaphoreType.DMA((SIDE // 2,)),
        ],
        compiler_params=LARGE,
        name="attend",
    )(plan, qpool, kpool)
    back = swapped(out, ALL, Q_GROUPS)
    across = lax.ppermute(above, "x", ring)
    below = lax.ppermute(out_weight, "x", [(j, i) for i, j in ring])
    heads = pl.pallas_call(
        join_kernel,
        out_shape=jax.ShapeDtypeStruct((4, 2 * tokens, VD), bf16),
        in_specs=[pl.BlockSpec(memory_space=pltpu.SMEM)] + [vmem()] * 3,
        out_specs=vmem(),
        compiler_params=SMALL,
        name="join",
    )(mix_weight, back, head_gain.reshape(1, VD), residual)
    heads = swapped(heads, "x")
    half, sent = pl.pallas_call(
        project_kernel,
        out_shape=[
            jax.ShapeDtypeStruct((tokens, width), f32),
            jax.ShapeDtypeStruct((tokens, width), bf16),
        ],
        in_specs=[smem, vmem()] + [pl.BlockSpec(memory_space=pl.ANY)] * 4,
        out_specs=[vmem()] * 2,
        scratch_shapes=[pltpu.VMEM((4, VD, 2048), bf16), pltpu.SemaphoreType.DMA((4,))],
        compiler_params=SMALL,
        name="project",
    )(place, heads, *(in_hbm(a) for a in (out_weight, above, below, across)))
    other = lax.ppermute(sent, "core", [(0, 1), (1, 0)])
    gated, edge, rows, stream, later = pl.pallas_call(
        gate_kernel,
        out_shape=[
            jax.ShapeDtypeStruct((tokens, MAIN + 128), bf16),
            jax.ShapeDtypeStruct((16, MAIN + 128), bf16),
            jax.ShapeDtypeStruct((tokens, width), bf16),
            jax.ShapeDtypeStruct((own, width), f32),
            jax.ShapeDtypeStruct((SIDE, SIDE, 160, 128), bf16),
        ],
        in_specs=[smem] + [vmem()] * 3 + [hbm],
        out_specs=[vmem()] * 5,
        scratch_shapes=[
            pltpu.VMEM((SIDE, SIDE, 192, 128), bf16),
            pltpu.SemaphoreType.DMA((SIDE,)),
            pltpu.SemaphoreType.DMA((SIDE,)),
        ],
        compiler_params=SMALL,
        name="gate",
    )(place, half, other, norm_gain.reshape(1, width), weights)
    route = [(i, i + 1) for i in range(SIDE * SIDE - 1)]
    prior = lax.ppermute(edge, ("z", "y"), route)
    lifted = pl.pallas_call(
        lift_kernel,
        out_shape=jax.ShapeDtypeStruct((tokens, MAIN), bf16),
        in_specs=[vmem()] * 2,
        out_specs=vmem(),
        compiler_params=SMALL,
        cost_estimate=pl.CostEstimate(
            flops=2 * 128 * 2048 * 640, bytes_accessed=3 << 20, transcendentals=0
        ),
        name="lift",
    )(rows, later)
    gap = jnp.zeros((WIDTH, 64), f32)
    taps = jnp.concatenate([conv_taps[:, :MAIN], gap, conv_taps[:, MAIN:]], axis=1)
    keep, give = pl.pallas_call(
        down_kernel,
        out_shape=[
            jax.ShapeDtypeStruct((tokens // 2, width), f32),
            jax.ShapeDtypeStruct((tokens // 2, width), bf16),
        ],
        in_specs=[smem] + [vmem()] * 5,
        out_specs=[vmem()] * 2,
        scratch_shapes=[pltpu.VMEM((128, 2048), f32)],
        compiler_params=SMALL,
        name="down",
    )(place, gated, lifted, prior, taps, down_weight)
    taken = lax.ppermute(give, "core", [(0, 1), (1, 0)])
    pair = pl.pallas_call(
        pair_kernel,
        out_shape=jax.ShapeDtypeStruct((4, own, width), bf16),
        in_specs=[vmem()] * 2,
        out_specs=vmem(),
        compiler_params=SMALL,
        name="pair",
    )(keep, taken)
    mixer = swapped(pair, "x")
    return pl.pallas_call(
        last_kernel,
        out_shape=jax.ShapeDtypeStruct((own, width), bf16),
        in_specs=[vmem()] * 2,
        out_specs=vmem(),
        compiler_params=SMALL,
        name="last",
    )(mixer, stream)


def solution(mesh):
    fine = Mesh(mesh.devices.reshape(SIDE, SIDE, 4, 2), ("z", "y", "x", "core"))
    sp = ("z", "y")

    return jax.shard_map(
        on_device,
        mesh=fine,
        in_specs=(
            P(sp, TP),
            P(sp, TP),
            P(sp, TP),
            P(sp, TP),
            P(sp, TP),
            P(TP),
            P(),
            P(("z", "y", "x", "core"), None),
            P(TP, None),
            P(),
            P(sp, TP),
            P(sp, TP),
            P(None, TP),
            P(TP, None),
        ),
        out_specs=P(("z", "y", "x", "core"), None),
        check_vma=False,
    )
```

```python
import jax
import jax.numpy as jnp
import numpy as np
from jax import lax
from jax.experimental import pallas as pl
from jax.experimental.pallas import tpu as pltpu
from jax.sharding import Mesh, PartitionSpec as P

HD = 128
VD = 256
STRETCH = 64
WIDTH = 3
SIDE = 8
BLOCK = 128
PACK = 4 * BLOCK + 16
TILES = 5
MAIN = 128 * TILES
SENT = 512
SHIFTS = (0, 1, -1, 2)
epsilon = 1e-06
masked_score = -1e30
LOG2E = 1.4426950408889634
EXP2_SCALE = LOG2E * HD**-0.5
f32 = jnp.float32
bf16 = jnp.bfloat16
TP = ("x", "core")
ALL = ("z", "y", "x", "core")
PLACES = np.arange(SIDE * SIDE * 8).reshape(SIDE, SIDE, 4, 2)
ROWS = [[PLACES[i, :, x, c].tolist() for i in range(SIDE) for x in range(4)] for c in range(2)]
COLS = [[PLACES[:, i, x, c].tolist() for i in range(SIDE) for x in range(4)] for c in range(2)]
Q_GROUPS = ROWS[0] + COLS[1]
K_GROUPS = COLS[0] + ROWS[1]


def vmem():
    return pl.BlockSpec(memory_space=pltpu.VMEM)


def pack_kernel(q1, q2, k1, k2, v, lift, gate, qsend, ksend, wsend, vv, ll, gg, rows, sems, sent):
    moves = [
        pltpu.make_async_copy(src, dst, sems.at[i])
        for i, (src, dst) in enumerate(
            (
                (k1, rows.at[0:128]),
                (k2, rows.at[128:256]),
                (v, vv),
                (lift, ll),
                (gate, gg),
                (q1, qsend.at[0:128]),
                (q2, qsend.at[128:256]),
            )
        )
    ]
    for move in moves:
        move.start()
    for move in moves:
        move.wait()
    rows[256:384, :] = vv[:, 0:128]
    rows[384:512, :] = vv[:, 128:256]
    for n in range(TILES):
        wsend[32 * n : 32 * n + 32, :] = gg[:, 128 * n : 128 * n + 128]
        wsend[192 + 32 * n : 224 + 32 * n, :] = ll[:, 128 * n : 128 * n + 128]
    wsend[160:192, :] = jnp.concatenate([ll[:, MAIN:], gg[:, MAIN:]], axis=1)
    copies = [pltpu.make_async_copy(rows, ksend.at[i], sent.at[i]) for i in range(SIDE)]
    for copy in copies:
        copy.start()
    for copy in copies:
        copy.wait()


def attend_kernel(plan, qpool, kpool, result, out, sems):
    q_base, q_step, k_base, k_step = (plan[i] for i in range(4))
    at = lax.broadcasted_iota(jnp.int32, (16, 128), 0)
    row = lax.broadcasted_iota(jnp.int32, (256, 1), 0)
    col = lax.broadcasted_iota(jnp.int32, (1, 1024), 1)
    k_at = 2 * (k_base + k_step * (col // 128)) + (col % 128) // STRETCH
    vals = jnp.concatenate(
        [kpool[:, 256:384, :].reshape(1024, 128), kpool[:, 384:512, :].reshape(1024, 128)], axis=1
    )
    for c in range(SIDE // 2):
        q_at = 2 * (q_base + q_step * (2 * c + row // 128)) + (row % 128) // STRETCH
        seen = k_at <= q_at
        levels = []
        for m in range(2):
            lo = slice(128 * m, 128 * m + 128)
            q = jnp.concatenate([qpool[2 * c, lo, :], qpool[2 * c + 1, lo, :]], axis=0)
            k = kpool[:, lo, :].reshape(1024, 128)
            s = lax.dot_general(q, k, (((1,), (1,)), ((), ())), preferred_element_type=f32)
            s = jnp.where(seen, s, masked_score)
            top = jnp.max(s, axis=-1, keepdims=True)
            w = jnp.exp2((s - top) * EXP2_SCALE)
            total = jnp.sum(w, axis=-1, keepdims=True)
            o = (jnp.dot(w.astype(bf16), vals, preferred_element_type=f32) / total).astype(bf16)
            level = top * EXP2_SCALE + jnp.log2(total)
            levels.append(jnp.where(top > 0.5 * masked_score, level, masked_score))
            for h in range(2):
                for e in range(2):
                    out[2 * c + h, 256 * m + 128 * e : 256 * m + 128 * e + 128, :] = o[
                        128 * h : 128 * h + 128, 128 * e : 128 * e + 128
                    ]
        for h in range(2):
            rows = jnp.zeros((16, 128), f32)
            for m in range(2):
                wide = jnp.transpose(
                    jnp.broadcast_to(levels[m][128 * h : 128 * h + 128], (128, 128))
                )[0:16]
                a = wide.astype(bf16).astype(f32)
                b = (wide - a).astype(bf16).astype(f32)
                d = wide - a - b
                for n, piece in enumerate((a, b, d)):
                    rows = jnp.where(at == 3 * m + n, piece, rows)
            out[2 * c + h, 512:528, :] = rows.astype(bf16)
        pair = pl.ds(2 * c, 2)
        pltpu.make_async_copy(out.at[pair], result.at[pair], sems.at[c]).start()
    for c in range(SIDE // 2):
        pair = pl.ds(2 * c, 2)
        pltpu.make_async_copy(out.at[pair], result.at[pair], sems.at[c]).wait()


def join_kernel(mix, parts, gain, residual, out):
    tails = [parts[i, 512:528, :].astype(f32) for i in range(SIDE)]

    def joined(m):
        levels = jnp.concatenate(
            [jnp.sum(tail[3 * m : 3 * m + 3], axis=0, keepdims=True) for tail in tails], axis=0
        )
        top = jnp.max(levels, axis=0, keepdims=True)
        w = jnp.exp2(levels - top)
        w = w / jnp.sum(w, axis=0, keepdims=True)
        w = jnp.transpose(jnp.concatenate([w, jnp.zeros((120, 128), f32)], axis=0))
        acc = [jnp.zeros((128, 128), f32), jnp.zeros((128, 128), f32)]
        for i in range(SIDE):
            wi = w[:, i : i + 1]
            for e in range(2):
                at = 256 * m + 128 * e
                acc[e] = acc[e] + wi * parts[i, at : at + 128, :].astype(f32)
        return jnp.concatenate(acc, axis=1)

    mixed = joined(0) - mix[0] * joined(1)
    r = lax.rsqrt(jnp.mean(mixed * mixed, axis=-1, keepdims=True) + epsilon)
    head = (mixed * r * gain[...]).astype(bf16)
    for i in range(4):
        out[i, 0:128] = head
        for j in range(8):
            out[i, 128 + 16 * j : 144 + 16 * j, :] = residual[:, 256 * j : 256 * j + 256]


def own_rows(place, i):
    return pl.ds(pl.multiple_of(32 * i + 16 * place[0], 16), 16)


def other_rows(place, i):
    return pl.ds(pl.multiple_of(32 * i + 16 - 16 * place[0], 16), 16)


def project_kernel(place, heads, *refs):
    weights, (half, sent, buffer, sems) = refs[:4], refs[4:]
    x = place[1]
    moves = [
        pltpu.make_async_copy(weight, buffer.at[i], sems.at[i]) for i, weight in enumerate(weights)
    ]
    for move in moves:
        move.start()
    for i, shift in enumerate(SHIFTS):
        moves[i].wait()
        head = heads[lax.rem(x + 4 - shift, 4), 0:128]
        for n in range(0, 2048, 256):
            d = jnp.dot(head, buffer[i, :, n : n + 256], preferred_element_type=f32)
            if i > 0:
                d = d + half[:, n : n + 256]
            half[:, n : n + 256] = d
    for i in range(4):
        rows = own_rows(place, i)
        for j in range(8):
            r = heads[i, 128 + 16 * j : 144 + 16 * j, :].astype(f32)
            half[rows, 256 * j : 256 * j + 256] = half[rows, 256 * j : 256 * j + 256] + r
    sent[...] = half[...].astype(bf16)


def fetched(weights, buffer, sems, first):
    rows = pl.ds(first, buffer.shape[2])
    for g in range(SIDE):
        pltpu.make_async_copy(weights.at[g, :, rows, :], buffer.at[g], sems.at[g]).start()


def multiplied(rows, buffer, ready):
    count = buffer.shape[2] // 32
    acc = [None] * ((count + 1) // 2)
    for g in range(SIDE):
        ready(g)
        lhs = rows[:, 256 * g : 256 * g + 256]
        for n in range(0, count, 2):
            tiles = [
                buffer[g, :, 32 * m : 32 * m + 32, :].reshape(256, 128)
                for m in range(n, min(n + 2, count))
            ]
            rhs = jnp.concatenate(tiles, axis=1) if len(tiles) > 1 else tiles[0]
            d = jnp.dot(lhs, rhs, preferred_element_type=f32)
            acc[n // 2] = d if acc[n // 2] is None else acc[n // 2] + d
    return acc


def gate_kernel(place, half, other, gain, weights, gated, edge, rows, stream, later, buffer, sems, more):
    fetched(weights, buffer, sems, 0)
    fetched(weights, later, more, 192)
    for n in range(0, 128, 32):
        total = half[n : n + 32] + other[n : n + 32].astype(f32)
        r = lax.rsqrt(jnp.mean(total * total, axis=-1, keepdims=True) + epsilon)
        rows[n : n + 32] = (total * r * gain[...]).astype(bf16)
    own = pl.ds(pl.multiple_of(place[2] * 16, 16), 16)
    stream[...] = half[own] + other[own].astype(f32)

    def ready(g):
        pltpu.make_async_copy(
            weights.at[0, :, pl.ds(0, 192), :], buffer.at[g], sems.at[g]
        ).wait()

    for n, part in enumerate(multiplied(rows, buffer, ready)):
        part = part.astype(bf16)
        gated[:, 256 * n : 256 * n + 256] = part
        edge[:, 256 * n : 256 * n + 256] = part[112:128]
    for g in range(SIDE):
        pltpu.make_async_copy(
            weights.at[0, :, pl.ds(192, 160), :], later.at[g], more.at[g]
        ).wait()


def lift_kernel(rows, weights, lifted):
    for n, part in enumerate(multiplied(rows, weights, lambda g: None)):
        lifted[:, 256 * n : 256 * n + part.shape[1]] = part.astype(bf16)


def down_kernel(place, gated, lifted, prior, taps, weight, keep, give, whole):
    at = lax.broadcasted_iota(jnp.int32, (128, 1), 0)

    def activated(lo, hi):
        g = gated[:, lo:hi].astype(f32)
        p = prior[:, lo:hi].astype(f32)
        one = jnp.where(at == 0, p[15:16], pltpu.roll(g, 1, 0))
        two = jnp.where(at == 0, p[14:15], jnp.where(at == 1, p[15:16], pltpu.roll(g, 2, 0)))
        conv = taps[0:1, lo:hi] * two + taps[1:2, lo:hi] * one + taps[2:3, lo:hi] * g
        return g, conv * jax.nn.sigmoid(conv)

    acc = None
    for n in range(0, MAIN, 128):
        _, a = activated(n, n + 128)
        h = (a * lifted[:, n : n + 128].astype(f32)).astype(bf16)
        d = jnp.dot(h, weight[n : n + 128, :], preferred_element_type=f32)
        acc = d if acc is None else acc + d
    g, a = activated(MAIN, MAIN + 128)
    h = (pltpu.roll(a, 64, 1) * g).astype(bf16)
    whole[...] = acc + jnp.dot(h[:, 0:64], weight[MAIN:, :], preferred_element_type=f32)
    for i in range(4):
        keep[16 * i : 16 * i + 16] = whole[own_rows(place, i)]
        give[16 * i : 16 * i + 16] = whole[other_rows(place, i)].astype(bf16)


def pair_kernel(keep, other, out):
    for i in range(4):
        rows = slice(16 * i, 16 * i + 16)
        out[i] = (keep[rows] + other[rows].astype(f32)).astype(bf16)


def last_kernel(parts, stream, out):
    mixer = parts[0].astype(f32)
    for i in range(1, 4):
        mixer = mixer + parts[i].astype(f32)
    out[...] = (stream[...] + mixer).astype(bf16)


def swapped(a, axis, groups=None):
    return lax.all_to_all(a, axis, 0, 0, axis_index_groups=groups, tiled=True)


def gathered(a, axis, groups=None):
    return lax.all_gather(a, axis, axis_index_groups=groups, axis=0, tiled=True)


def in_hbm(a):
    return pltpu.with_memory_space_constraint(a, pltpu.HBM)


SMALL = pltpu.CompilerParams(vmem_limit_bytes=20 << 20)
LARGE = pltpu.CompilerParams(vmem_limit_bytes=30 << 20)


def on_device(
    query_one,
    key_one,
    query_two,
    key_two,
    values,
    mix_weight,
    head_gain,
    residual,
    out_weight,
    norm_gain,
    lift_weight,
    gate_weight,
    conv_taps,
    down_weight,
):
    tokens = query_one.shape[0]
    own = residual.shape[0]
    width = residual.shape[1]
    z = lax.axis_index("z")
    y = lax.axis_index("y")
    core = lax.axis_index("core")
    along_y = jnp.stack([z * SIDE, 1 + 0 * z, y, SIDE + 0 * z])
    along_z = jnp.stack([y, SIDE + 0 * z, z * SIDE, 1 + 0 * z])
    plan = jnp.where(core == 0, along_y, along_z).astype(jnp.int32)
    smem = pl.BlockSpec(memory_space=pltpu.SMEM)
    hbm = pl.BlockSpec(memory_space=pltpu.HBM)
    x = lax.axis_index("x")
    place = jnp.stack([core, x, 2 * x + core]).astype(jnp.int32)
    qsend, ksend, wsend = pl.pallas_call(
        pack_kernel,
        out_shape=[
            jax.ShapeDtypeStruct((256, 128), bf16),
            jax.ShapeDtypeStruct((SIDE, SENT, 128), bf16),
            pltpu.HBM((352, 128), bf16),
        ],
        in_specs=[hbm] * 7,
        out_specs=[vmem(), hbm, vmem()],
        scratch_shapes=[
            pltpu.VMEM((128, 256), bf16),
            pltpu.VMEM((32, 704), bf16),
            pltpu.VMEM((32, 704), bf16),
            pltpu.VMEM((SENT, 128), bf16),
            pltpu.SemaphoreType.DMA((7,)),
            pltpu.SemaphoreType.DMA((SIDE,)),
        ],
        compiler_params=SMALL,
        name="pack",
    )(*(in_hbm(a) for a in (query_one, query_two, key_one, key_two, values, lift_weight, gate_weight)))
    kpool = swapped(ksend, ALL, K_GROUPS)
    qpool = gathered(qsend, ALL, Q_GROUPS).reshape(SIDE, 256, 128)
    weights = in_hbm(gathered(wsend, ("z", "y")).reshape(SIDE, SIDE, 352, 128))
    ring = [(i, (i + 1) % 4) for i in range(4)]
    above = lax.ppermute(out_weight, "x", ring)
    out = pl.pallas_call(
        attend_kernel,
        out_shape=pltpu.HBM((SIDE, PACK, 128), bf16),
        in_specs=[pl.BlockSpec(memory_space=pltpu.SMEM), vmem(), vmem()],
        out_specs=hbm,
        scratch_shapes=[
            pltpu.VMEM((SIDE, PACK, 128), bf16),
            pltpu.SemaphoreType.DMA((SIDE // 2,)),
        ],
        compiler_params=LARGE,
        name="attend",
    )(plan, qpool, kpool)
    back = swapped(out, ALL, Q_GROUPS)
    across = lax.ppermute(above, "x", ring)
    below = lax.ppermute(out_weight, "x", [(j, i) for i, j in ring])
    heads = pl.pallas_call(
        join_kernel,
        out_shape=jax.ShapeDtypeStruct((4, 2 * tokens, VD), bf16),
        in_specs=[pl.BlockSpec(memory_space=pltpu.SMEM)] + [vmem()] * 3,
        out_specs=vmem(),
        compiler_params=SMALL,
        name="join",
    )(mix_weight, back, head_gain.reshape(1, VD), residual)
    heads = swapped(heads, "x")
    half, sent = pl.pallas_call(
        project_kernel,
        out_shape=[
            jax.ShapeDtypeStruct((tokens, width), f32),
            jax.ShapeDtypeStruct((tokens, width), bf16),
        ],
        in_specs=[smem, vmem()] + [pl.BlockSpec(memory_space=pl.ANY)] * 4,
        out_specs=[vmem()] * 2,
        scratch_shapes=[pltpu.VMEM((4, VD, 2048), bf16), pltpu.SemaphoreType.DMA((4,))],
        compiler_params=SMALL,
        name="project",
    )(place, heads, *(in_hbm(a) for a in (out_weight, above, below, across)))
    other = lax.ppermute(sent, "core", [(0, 1), (1, 0)])
    gated, edge, rows, stream, later = pl.pallas_call(
        gate_kernel,
        out_shape=[
            jax.ShapeDtypeStruct((tokens, MAIN + 128), bf16),
            jax.ShapeDtypeStruct((16, MAIN + 128), bf16),
            jax.ShapeDtypeStruct((tokens, width), bf16),
            jax.ShapeDtypeStruct((own, width), f32),
            jax.ShapeDtypeStruct((SIDE, SIDE, 160, 128), bf16),
        ],
        in_specs=[smem] + [vmem()] * 3 + [hbm],
        out_specs=[vmem()] * 5,
        scratch_shapes=[
            pltpu.VMEM((SIDE, SIDE, 192, 128), bf16),
            pltpu.SemaphoreType.DMA((SIDE,)),
            pltpu.SemaphoreType.DMA((SIDE,)),
        ],
        compiler_params=SMALL,
        name="gate",
    )(place, half, other, norm_gain.reshape(1, width), weights)
    route = [(i, i + 1) for i in range(SIDE * SIDE - 1)]
    prior = lax.ppermute(edge, ("z", "y"), route)
    lifted = pl.pallas_call(
        lift_kernel,
        out_shape=jax.ShapeDtypeStruct((tokens, MAIN), bf16),
        in_specs=[vmem()] * 2,
        out_specs=vmem(),
        compiler_params=SMALL,
        cost_estimate=pl.CostEstimate(
            flops=2 * 128 * 2048 * 640, bytes_accessed=3 << 20, transcendentals=0
        ),
        name="lift",
    )(rows, later)
    gap = jnp.zeros((WIDTH, 64), f32)
    taps = jnp.concatenate([conv_taps[:, :MAIN], gap, conv_taps[:, MAIN:]], axis=1)
    keep, give = pl.pallas_call(
        down_kernel,
        out_shape=[
            jax.ShapeDtypeStruct((tokens // 2, width), f32),
            jax.ShapeDtypeStruct((tokens // 2, width), bf16),
        ],
        in_specs=[smem] + [vmem()] * 5,
        out_specs=[vmem()] * 2,
        scratch_shapes=[pltpu.VMEM((128, 2048), f32)],
        compiler_params=SMALL,
        name="down",
    )(place, gated, lifted, prior, taps, down_weight)
    taken = lax.ppermute(give, "core", [(0, 1), (1, 0)])
    pair = pl.pallas_call(
        pair_kernel,
        out_shape=jax.ShapeDtypeStruct((4, own, width), bf16),
        in_specs=[vmem()] * 2,
        out_specs=vmem(),
        compiler_params=SMALL,
        name="pair",
    )(keep, taken)
    mixer = swapped(pair, "x")
    return pl.pallas_call(
        last_kernel,
        out_shape=jax.ShapeDtypeStruct((own, width), bf16),
        in_specs=[vmem()] * 2,
        out_specs=vmem(),
        compiler_params=SMALL,
        name="last",
    )(mixer, stream)


def solution(mesh):
    fine = Mesh(mesh.devices.reshape(SIDE, SIDE, 4, 2), ("z", "y", "x", "core"))
    sp = ("z", "y")

    return jax.shard_map(
        on_device,
        mesh=fine,
        in_specs=(
            P(sp, TP),
            P(sp, TP),
            P(sp, TP),
            P(sp, TP),
            P(sp, TP),
            P(TP),
            P(),
            P(("z", "y", "x", "core"), None),
            P(TP, None),
            P(),
            P(sp, TP),
            P(sp, TP),
            P(None, TP),
            P(TP, None),
        ),
        out_specs=P(("z", "y", "x", "core"), None),
        check_vma=False,
    )
```

```python
import jax
import jax.numpy as jnp
import numpy as np
from jax import lax
from jax.experimental import pallas as pl
from jax.experimental.pallas import tpu as pltpu
from jax.sharding import Mesh, PartitionSpec as P

HD = 128
VD = 256
STRETCH = 64
WIDTH = 3
SIDE = 8
BLOCK = 128
PACK = 4 * BLOCK + 16
TILES = 5
MAIN = 128 * TILES
SENT = 512
SHIFTS = (0, 1, -1, 2)
epsilon = 1e-06
masked_score = -1e30
LOG2E = 1.4426950408889634
EXP2_SCALE = LOG2E * HD**-0.5
f32 = jnp.float32
bf16 = jnp.bfloat16
TP = ("x", "core")
ALL = ("z", "y", "x", "core")
PLACES = np.arange(SIDE * SIDE * 8).reshape(SIDE, SIDE, 4, 2)
ROWS = [[PLACES[i, :, x, c].tolist() for i in range(SIDE) for x in range(4)] for c in range(2)]
COLS = [[PLACES[:, i, x, c].tolist() for i in range(SIDE) for x in range(4)] for c in range(2)]
Q_GROUPS = ROWS[0] + COLS[1]
K_GROUPS = COLS[0] + ROWS[1]


def vmem():
    return pl.BlockSpec(memory_space=pltpu.VMEM)


def rows_kernel(lift, gate, wsend, ll, gg, sems):
    moves = [
        pltpu.make_async_copy(gate, gg, sems.at[0]),
        pltpu.make_async_copy(lift, ll, sems.at[1]),
    ]
    for move in moves:
        move.start()
    for move in moves:
        move.wait()
    for n in range(TILES):
        wsend[32 * n : 32 * n + 32, :] = gg[:, 128 * n : 128 * n + 128]
        wsend[192 + 32 * n : 224 + 32 * n, :] = ll[:, 128 * n : 128 * n + 128]
    wsend[160:192, :] = jnp.concatenate([ll[:, MAIN:], gg[:, MAIN:]], axis=1)


def pack_kernel(q1, q2, k1, k2, v, qsend, ksend, vv, rows, sems, sent):
    sources = (k1, k2, v, q1, q2)
    targets = (rows.at[0:128], rows.at[128:256], vv, qsend.at[0:128], qsend.at[128:256])
    moves = [
        pltpu.make_async_copy(src, dst, sems.at[i])
        for i, (src, dst) in enumerate(zip(sources, targets))
    ]
    for move in moves:
        move.start()
    for move in moves:
        move.wait()
    rows[256:384, :] = vv[:, 0:128]
    rows[384:512, :] = vv[:, 128:256]
    copies = [pltpu.make_async_copy(rows, ksend.at[i], sent.at[i]) for i in range(SIDE)]
    for copy in copies:
        copy.start()
    for copy in copies:
        copy.wait()


def attend_kernel(plan, qpool, kpool, result, out, sems):
    q_base, q_step, k_base, k_step = (plan[i] for i in range(4))
    at = lax.broadcasted_iota(jnp.int32, (16, 128), 0)
    row = lax.broadcasted_iota(jnp.int32, (256, 1), 0)
    col = lax.broadcasted_iota(jnp.int32, (1, 1024), 1)
    k_at = 2 * (k_base + k_step * (col // 128)) + (col % 128) // STRETCH
    vals = jnp.concatenate(
        [kpool[:, 256:384, :].reshape(1024, 128), kpool[:, 384:512, :].reshape(1024, 128)], axis=1
    )
    for c in range(SIDE // 2):
        q_at = 2 * (q_base + q_step * (2 * c + row // 128)) + (row % 128) // STRETCH
        seen = k_at <= q_at
        levels = []
        for m in range(2):
            lo = slice(128 * m, 128 * m + 128)
            q = jnp.concatenate([qpool[2 * c, lo, :], qpool[2 * c + 1, lo, :]], axis=0)
            k = kpool[:, lo, :].reshape(1024, 128)
            s = lax.dot_general(q, k, (((1,), (1,)), ((), ())), preferred_element_type=f32)
            s = jnp.where(seen, s, masked_score)
            top = jnp.max(s, axis=-1, keepdims=True)
            w = jnp.exp2((s - top) * EXP2_SCALE)
            total = jnp.sum(w, axis=-1, keepdims=True)
            o = (jnp.dot(w.astype(bf16), vals, preferred_element_type=f32) / total).astype(bf16)
            level = top * EXP2_SCALE + jnp.log2(total)
            levels.append(jnp.where(top > 0.5 * masked_score, level, masked_score))
            for h in range(2):
                for e in range(2):
                    out[2 * c + h, 256 * m + 128 * e : 256 * m + 128 * e + 128, :] = o[
                        128 * h : 128 * h + 128, 128 * e : 128 * e + 128
                    ]
        for h in range(2):
            rows = jnp.zeros((16, 128), f32)
            for m in range(2):
                wide = jnp.transpose(
                    jnp.broadcast_to(levels[m][128 * h : 128 * h + 128], (128, 128))
                )[0:16]
                a = wide.astype(bf16).astype(f32)
                b = (wide - a).astype(bf16).astype(f32)
                d = wide - a - b
                for n, piece in enumerate((a, b, d)):
                    rows = jnp.where(at == 3 * m + n, piece, rows)
            out[2 * c + h, 512:528, :] = rows.astype(bf16)
        pair = pl.ds(2 * c, 2)
        pltpu.make_async_copy(out.at[pair], result.at[pair], sems.at[c]).start()
    for c in range(SIDE // 2):
        pair = pl.ds(2 * c, 2)
        pltpu.make_async_copy(out.at[pair], result.at[pair], sems.at[c]).wait()


def join_kernel(mix, parts, gain, residual, out):
    tails = [parts[i, 512:528, :].astype(f32) for i in range(SIDE)]

    def joined(m):
        levels = jnp.concatenate(
            [jnp.sum(tail[3 * m : 3 * m + 3], axis=0, keepdims=True) for tail in tails], axis=0
        )
        top = jnp.max(levels, axis=0, keepdims=True)
        w = jnp.exp2(levels - top)
        w = w / jnp.sum(w, axis=0, keepdims=True)
        w = jnp.transpose(jnp.concatenate([w, jnp.zeros((120, 128), f32)], axis=0))
        acc = [jnp.zeros((128, 128), f32), jnp.zeros((128, 128), f32)]
        for i in range(SIDE):
            wi = w[:, i : i + 1]
            for e in range(2):
                at = 256 * m + 128 * e
                acc[e] = acc[e] + wi * parts[i, at : at + 128, :].astype(f32)
        return jnp.concatenate(acc, axis=1)

    mixed = joined(0) - mix[0] * joined(1)
    r = lax.rsqrt(jnp.mean(mixed * mixed, axis=-1, keepdims=True) + epsilon)
    head = (mixed * r * gain[...]).astype(bf16)
    for i in range(4):
        out[i, 0:128] = head
        for j in range(8):
            out[i, 128 + 16 * j : 144 + 16 * j, :] = residual[:, 256 * j : 256 * j + 256]


def own_rows(place, i):
    return pl.ds(pl.multiple_of(32 * i + 16 * place[0], 16), 16)


def other_rows(place, i):
    return pl.ds(pl.multiple_of(32 * i + 16 - 16 * place[0], 16), 16)


def project_kernel(place, heads, *refs):
    weights, (half, sent, buffer, sems) = refs[:4], refs[4:]
    x = place[1]
    moves = [
        pltpu.make_async_copy(weight, buffer.at[i], sems.at[i]) for i, weight in enumerate(weights)
    ]
    for move in moves:
        move.start()
    for i, shift in enumerate(SHIFTS):
        moves[i].wait()
        head = heads[lax.rem(x + 4 - shift, 4), 0:128]
        for n in range(0, 2048, 256):
            d = jnp.dot(head, buffer[i, :, n : n + 256], preferred_element_type=f32)
            if i > 0:
                d = d + half[:, n : n + 256]
            half[:, n : n + 256] = d
    for i in range(4):
        rows = own_rows(place, i)
        for j in range(8):
            r = heads[i, 128 + 16 * j : 144 + 16 * j, :].astype(f32)
            half[rows, 256 * j : 256 * j + 256] = half[rows, 256 * j : 256 * j + 256] + r
    sent[...] = half[...].astype(bf16)


def fetched(weights, buffer, sems, first):
    rows = pl.ds(first, buffer.shape[2])
    for g in range(SIDE):
        pltpu.make_async_copy(weights.at[g, :, rows, :], buffer.at[g], sems.at[g]).start()


def multiplied(rows, buffer, ready):
    count = buffer.shape[2] // 32
    acc = [None] * ((count + 1) // 2)
    for g in range(SIDE):
        ready(g)
        lhs = rows[:, 256 * g : 256 * g + 256]
        for n in range(0, count, 2):
            tiles = [
                buffer[g, :, 32 * m : 32 * m + 32, :].reshape(256, 128)
                for m in range(n, min(n + 2, count))
            ]
            rhs = jnp.concatenate(tiles, axis=1) if len(tiles) > 1 else tiles[0]
            d = jnp.dot(lhs, rhs, preferred_element_type=f32)
            acc[n // 2] = d if acc[n // 2] is None else acc[n // 2] + d
    return acc


def gate_kernel(place, half, other, gain, weights, gated, edge, rows, stream, later, buffer, sems, more):
    fetched(weights, buffer, sems, 0)
    fetched(weights, later, more, 192)
    for n in range(0, 128, 32):
        total = half[n : n + 32] + other[n : n + 32].astype(f32)
        r = lax.rsqrt(jnp.mean(total * total, axis=-1, keepdims=True) + epsilon)
        rows[n : n + 32] = (total * r * gain[...]).astype(bf16)
    own = pl.ds(pl.multiple_of(place[2] * 16, 16), 16)
    stream[...] = half[own] + other[own].astype(f32)

    def ready(g):
        pltpu.make_async_copy(
            weights.at[0, :, pl.ds(0, 192), :], buffer.at[g], sems.at[g]
        ).wait()

    for n, part in enumerate(multiplied(rows, buffer, ready)):
        part = part.astype(bf16)
        gated[:, 256 * n : 256 * n + 256] = part
        edge[:, 256 * n : 256 * n + 256] = part[112:128]
    for g in range(SIDE):
        pltpu.make_async_copy(
            weights.at[0, :, pl.ds(192, 160), :], later.at[g], more.at[g]
        ).wait()


def lift_kernel(rows, weights, lifted):
    for n, part in enumerate(multiplied(rows, weights, lambda g: None)):
        lifted[:, 256 * n : 256 * n + part.shape[1]] = part.astype(bf16)


def down_kernel(place, gated, lifted, prior, taps, weight, keep, give, whole):
    at = lax.broadcasted_iota(jnp.int32, (128, 1), 0)

    def activated(lo, hi):
        g = gated[:, lo:hi].astype(f32)
        p = prior[:, lo:hi].astype(f32)
        one = jnp.where(at == 0, p[15:16], pltpu.roll(g, 1, 0))
        two = jnp.where(at == 0, p[14:15], jnp.where(at == 1, p[15:16], pltpu.roll(g, 2, 0)))
        conv = taps[0:1, lo:hi] * two + taps[1:2, lo:hi] * one + taps[2:3, lo:hi] * g
        return g, conv * jax.nn.sigmoid(conv)

    acc = None
    for n in range(0, MAIN, 128):
        _, a = activated(n, n + 128)
        h = (a * lifted[:, n : n + 128].astype(f32)).astype(bf16)
        d = jnp.dot(h, weight[n : n + 128, :], preferred_element_type=f32)
        acc = d if acc is None else acc + d
    g, a = activated(MAIN, MAIN + 128)
    h = (pltpu.roll(a, 64, 1) * g).astype(bf16)
    whole[...] = acc + jnp.dot(h[:, 0:64], weight[MAIN:, :], preferred_element_type=f32)
    for i in range(4):
        keep[16 * i : 16 * i + 16] = whole[own_rows(place, i)]
        give[16 * i : 16 * i + 16] = whole[other_rows(place, i)].astype(bf16)


def pair_kernel(keep, other, out):
    for i in range(4):
        rows = slice(16 * i, 16 * i + 16)
        out[i] = (keep[rows] + other[rows].astype(f32)).astype(bf16)


def last_kernel(parts, stream, out):
    mixer = parts[0].astype(f32)
    for i in range(1, 4):
        mixer = mixer + parts[i].astype(f32)
    out[...] = (stream[...] + mixer).astype(bf16)


def swapped(a, axis, groups=None):
    return lax.all_to_all(a, axis, 0, 0, axis_index_groups=groups, tiled=True)


def gathered(a, axis, groups=None):
    return lax.all_gather(a, axis, axis_index_groups=groups, axis=0, tiled=True)


def in_hbm(a):
    return pltpu.with_memory_space_constraint(a, pltpu.HBM)


SMALL = pltpu.CompilerParams(vmem_limit_bytes=20 << 20)
LARGE = pltpu.CompilerParams(vmem_limit_bytes=30 << 20)


def on_device(
    query_one,
    key_one,
    query_two,
    key_two,
    values,
    mix_weight,
    head_gain,
    residual,
    out_weight,
    norm_gain,
    lift_weight,
    gate_weight,
    conv_taps,
    down_weight,
):
    tokens = query_one.shape[0]
    own = residual.shape[0]
    width = residual.shape[1]
    z = lax.axis_index("z")
    y = lax.axis_index("y")
    core = lax.axis_index("core")
    along_y = jnp.stack([z * SIDE, 1 + 0 * z, y, SIDE + 0 * z])
    along_z = jnp.stack([y, SIDE + 0 * z, z * SIDE, 1 + 0 * z])
    plan = jnp.where(core == 0, along_y, along_z).astype(jnp.int32)
    smem = pl.BlockSpec(memory_space=pltpu.SMEM)
    hbm = pl.BlockSpec(memory_space=pltpu.HBM)
    x = lax.axis_index("x")
    place = jnp.stack([core, x, 2 * x + core]).astype(jnp.int32)
    wsend = pl.pallas_call(
        rows_kernel,
        out_shape=pltpu.HBM((352, 128), bf16),
        in_specs=[hbm] * 2,
        out_specs=vmem(),
        scratch_shapes=[
            pltpu.VMEM((32, 704), bf16),
            pltpu.VMEM((32, 704), bf16),
            pltpu.SemaphoreType.DMA((2,)),
        ],
        compiler_params=SMALL,
        name="rows",
    )(in_hbm(lift_weight), in_hbm(gate_weight))
    wsend, *sources = lax.optimization_barrier(
        (wsend, query_one, query_two, key_one, key_two, values)
    )
    qsend, ksend = pl.pallas_call(
        pack_kernel,
        out_shape=[
            jax.ShapeDtypeStruct((256, 128), bf16),
            jax.ShapeDtypeStruct((SIDE, SENT, 128), bf16),
        ],
        in_specs=[hbm] * 5,
        out_specs=[vmem(), hbm],
        scratch_shapes=[
            pltpu.VMEM((128, 256), bf16),
            pltpu.VMEM((SENT, 128), bf16),
            pltpu.SemaphoreType.DMA((5,)),
            pltpu.SemaphoreType.DMA((SIDE,)),
        ],
        compiler_params=SMALL,
        name="pack",
    )(*(in_hbm(a) for a in sources))
    kpool = swapped(ksend, ALL, K_GROUPS)
    qpool = gathered(qsend, ALL, Q_GROUPS).reshape(SIDE, 256, 128)
    weights = in_hbm(gathered(wsend, ("z", "y")).reshape(SIDE, SIDE, 352, 128))
    ring = [(i, (i + 1) % 4) for i in range(4)]
    above = lax.ppermute(out_weight, "x", ring)
    out = pl.pallas_call(
        attend_kernel,
        out_shape=pltpu.HBM((SIDE, PACK, 128), bf16),
        in_specs=[pl.BlockSpec(memory_space=pltpu.SMEM), vmem(), vmem()],
        out_specs=hbm,
        scratch_shapes=[
            pltpu.VMEM((SIDE, PACK, 128), bf16),
            pltpu.SemaphoreType.DMA((SIDE // 2,)),
        ],
        compiler_params=LARGE,
        name="attend",
    )(plan, qpool, kpool)
    back = swapped(out, ALL, Q_GROUPS)
    across = lax.ppermute(above, "x", ring)
    below = lax.ppermute(out_weight, "x", [(j, i) for i, j in ring])
    heads = pl.pallas_call(
        join_kernel,
        out_shape=jax.ShapeDtypeStruct((4, 2 * tokens, VD), bf16),
        in_specs=[pl.BlockSpec(memory_space=pltpu.SMEM)] + [vmem()] * 3,
        out_specs=vmem(),
        compiler_params=SMALL,
        name="join",
    )(mix_weight, back, head_gain.reshape(1, VD), residual)
    heads = swapped(heads, "x")
    half, sent = pl.pallas_call(
        project_kernel,
        out_shape=[
            jax.ShapeDtypeStruct((tokens, width), f32),
            jax.ShapeDtypeStruct((tokens, width), bf16),
        ],
        in_specs=[smem, vmem()] + [pl.BlockSpec(memory_space=pl.ANY)] * 4,
        out_specs=[vmem()] * 2,
        scratch_shapes=[pltpu.VMEM((4, VD, 2048), bf16), pltpu.SemaphoreType.DMA((4,))],
        compiler_params=SMALL,
        name="project",
    )(place, heads, *(in_hbm(a) for a in (out_weight, above, below, across)))
    other = lax.ppermute(sent, "core", [(0, 1), (1, 0)])
    gated, edge, rows, stream, later = pl.pallas_call(
        gate_kernel,
        out_shape=[
            jax.ShapeDtypeStruct((tokens, MAIN + 128), bf16),
            jax.ShapeDtypeStruct((16, MAIN + 128), bf16),
            jax.ShapeDtypeStruct((tokens, width), bf16),
            jax.ShapeDtypeStruct((own, width), f32),
            jax.ShapeDtypeStruct((SIDE, SIDE, 160, 128), bf16),
        ],
        in_specs=[smem] + [vmem()] * 3 + [hbm],
        out_specs=[vmem()] * 5,
        scratch_shapes=[
            pltpu.VMEM((SIDE, SIDE, 192, 128), bf16),
            pltpu.SemaphoreType.DMA((SIDE,)),
            pltpu.SemaphoreType.DMA((SIDE,)),
        ],
        compiler_params=SMALL,
        name="gate",
    )(place, half, other, norm_gain.reshape(1, width), weights)
    route = [(i, i + 1) for i in range(SIDE * SIDE - 1)]
    prior = lax.ppermute(edge, ("z", "y"), route)
    lifted = pl.pallas_call(
        lift_kernel,
        out_shape=jax.ShapeDtypeStruct((tokens, MAIN), bf16),
        in_specs=[vmem()] * 2,
        out_specs=vmem(),
        compiler_params=SMALL,
        cost_estimate=pl.CostEstimate(
            flops=2 * 128 * 2048 * 640, bytes_accessed=3 << 20, transcendentals=0
        ),
        name="lift",
    )(rows, later)
    gap = jnp.zeros((WIDTH, 64), f32)
    taps = jnp.concatenate([conv_taps[:, :MAIN], gap, conv_taps[:, MAIN:]], axis=1)
    keep, give = pl.pallas_call(
        down_kernel,
        out_shape=[
            jax.ShapeDtypeStruct((tokens // 2, width), f32),
            jax.ShapeDtypeStruct((tokens // 2, width), bf16),
        ],
        in_specs=[smem] + [vmem()] * 5,
        out_specs=[vmem()] * 2,
        scratch_shapes=[pltpu.VMEM((128, 2048), f32)],
        compiler_params=SMALL,
        name="down",
    )(place, gated, lifted, prior, taps, down_weight)
    taken = lax.ppermute(give, "core", [(0, 1), (1, 0)])
    pair = pl.pallas_call(
        pair_kernel,
        out_shape=jax.ShapeDtypeStruct((4, own, width), bf16),
        in_specs=[vmem()] * 2,
        out_specs=vmem(),
        compiler_params=SMALL,
        name="pair",
    )(keep, taken)
    mixer = swapped(pair, "x")
    return pl.pallas_call(
        last_kernel,
        out_shape=jax.ShapeDtypeStruct((own, width), bf16),
        in_specs=[vmem()] * 2,
        out_specs=vmem(),
        compiler_params=SMALL,
        name="last",
    )(mixer, stream)


def solution(mesh):
    fine = Mesh(mesh.devices.reshape(SIDE, SIDE, 4, 2), ("z", "y", "x", "core"))
    sp = ("z", "y")

    return jax.shard_map(
        on_device,
        mesh=fine,
        in_specs=(
            P(sp, TP),
            P(sp, TP),
            P(sp, TP),
            P(sp, TP),
            P(sp, TP),
            P(TP),
            P(),
            P(("z", "y", "x", "core"), None),
            P(TP, None),
            P(),
            P(sp, TP),
            P(sp, TP),
            P(None, TP),
            P(TP, None),
        ),
        out_specs=P(("z", "y", "x", "core"), None),
        check_vma=False,
    )
```
